256 devices in a mesh: sp: 64 (over z, y, core), tp: 4 (over x).
Axes of the slice: x: 4, y: 4, z: 8, core: 2. Of those that a mesh axis runs over, the one named last changes fastest.
Arguments:
- residual: bfloat16 [16384, 2048], P(('sp', 'tp')), may hold values from -6 to 6
- output_gate_projected: bfloat16 [16384, 4096], P('sp', 'tp'), may hold values from -6 to 6
- value_projected_input: bfloat16 [16384, 4096], P('sp', 'tp'), may hold values from -6 to 6
- state_projected_input: bfloat16 [16384, 2048], P('sp', 'tp'), may hold values from -6 to 6
- readout_projected_input: bfloat16 [16384, 2048], P('sp', 'tp'), may hold values from -6 to 6
- step_preactivation: float32 [16384, 64], P('sp', 'tp'), may hold values from -5 to 5
- position_decay_extra: float32 [16384, 64], P('sp', 'tp')
- value_conv_kernel: bfloat16 [4, 4096], P(None, 'tp'), may hold values from -0.29882812 to 0.29882812
- state_conv_kernel: bfloat16 [4, 2048], P(None, 'tp'), may hold values from -0.8984375 to 0.8984375
- readout_conv_kernel: bfloat16 [4, 2048], P(None, 'tp'), may hold values from -0.8984375 to 0.8984375
- head_log_decay_rates: float32 [64], P('tp')
- head_direct_weight: float32 [64], P('tp'), may hold values from 0.5 to 4
- head_norm_gain: float32 [4096], P('tp'), may hold values from 0.1 to 1.9
- mixer_output_weight: bfloat16 [4096, 2048], P('tp'), may hold values from -0.09375 to 0.09375
- expert_norm_gain: float32 [2048], replicated, may hold values from 0.1 to 1.9
- routed_expert_index: int32 [16384, 4], P(('sp', 'tp')), may hold values from 0 to 63, all different within a row; in each aligned block of 64 rows (0 to 63, 64 to 127, ...) at most 8 rows name the same one
- routed_expert_weight: float32 [16384, 4], P(('sp', 'tp')), may hold values from 0.2 to 1
- routed_gate_weight: bfloat16 [64, 2048, 256], P('sp'), may hold values from -0.125 to 0.125
- routed_up_weight: bfloat16 [64, 2048, 256], P('sp'), may hold values from -0.125 to 0.125
- routed_down_weight: bfloat16 [64, 256, 2048], P('sp'), may hold values from -0.375 to 0.375
- common_gate_weight: bfloat16 [2048, 512], P(None, 'tp'), may hold values from -0.125 to 0.125
- common_up_weight: bfloat16 [2048, 512], P(None, 'tp'), may hold values from -0.125 to 0.125
- common_down_weight: bfloat16 [2048, 512], P(None, 'tp'), may hold values from -0.25 to 0.25
Outputs:
- layer_out: bfloat16 [16384, 2048], P(('sp', 'tp'))
The draws below stay inside these ranges and needn't reach their ends.
Inputs may be any that keep to these rules, and one draw needn't show every extreme that they name: `routed_expert_index`: among the 64 rows of one device, no expert is named by more than 8 rows.
All inputs are finite; a program needn't handle non-finite values.
Results may differ from the reference program's by a relative error of at most 0.02.
Values may be sent and summed in bfloat16 or wider, within the bound.
A program may use at most 128 MiB of HBM per device.

```python
import math
import jax
import jax.numpy as jnp
import numpy as np
from jax import lax

D = 2048
HEAD_DIM = 64
HEADS = 64
HEAD_GROUPS = 16
STATE = 128
CONV = 4
BLOCK_POSITIONS = 128
FE = 256
FS = 512
TOPK = 4
TOK_DEV = 256
INNER = 4096
SEQ = 16384
ROWS = 64
EXPERTS = 64
CAP = 8
N_TP = 4


def draw_step_preactivation(key, part):
    base_key, shift_key = jax.random.split(jax.random.fold_in(key, 11))
    block_list = SEQ // TOK_DEV
    jitter = jnp.clip(jax.random.normal(base_key, (SEQ, HEADS), jnp.float32), -4.0, 4.0)
    offsets = jax.random.uniform(shift_key, (block_list, 1, HEADS), jnp.float32, -1.0, 1.0)
    return (jitter.reshape(block_list, TOK_DEV, HEADS) + offsets).reshape(SEQ, HEADS)


def draw_head_log_decay_rates(key, part):
    pick_key, fast_key, slow_key = jax.random.split(jax.random.fold_in(key, 23), 3)
    ranking = jax.random.permutation(pick_key, HEADS)
    fast = ranking < HEADS // 2
    fast_rate = jax.random.uniform(fast_key, (HEADS,), jnp.float32, math.log(2.0 / BLOCK_POSITIONS), math.log(6.0 / BLOCK_POSITIONS))
    slow_rate = jax.random.uniform(slow_key, (HEADS,), jnp.float32, math.log(0.1 / SEQ), math.log(0.6 / SEQ))
    return jnp.where(fast, fast_rate, slow_rate)


def draw_position_decay_extra(key, part):
    place_key, depth_key = jax.random.split(jax.random.fold_in(key, 37))
    places = jax.random.randint(place_key, (3,), 0, SEQ)
    depths = jax.random.uniform(depth_key, (3, HEADS), jnp.float32, math.log(0.6), math.log(0.8))
    return jnp.zeros((SEQ, HEADS), jnp.float32).at[places].add(depths)


def steps_of(rng, dims, pieces, least, high):
    def one(position, parts):
        heights = jax.random.uniform(jax.random.fold_in(jax.random.fold_in(rng, 6), position), (parts,), jnp.float32, least / len(pieces), high / len(pieces))
        return jnp.repeat(jnp.exp(heights), dims[position] // parts).reshape((-1,) + (1,) * (len(dims) - position - 1))

    loudness = one(*pieces[0])
    for cut in pieces[1:]:
        loudness = loudness * one(*cut)
    return loudness


def assign_block(own_key, own, number, rows, count, top, bound, slope):
    sequence = jax.random.permutation(own_key, count)
    packed, common = load_shares(count, rows * top, bound, slope, True), load_shares(count, rows * top, bound, slope, False)
    places = jnp.arange(count)

    def named(tallies, turn):
        used = int((tallies > 0).sum())
        fixed = max(1, used // 4)
        moved = fixed + (places - fixed + turn * (used - fixed)) % max(1, count - fixed)
        return jnp.zeros((count,), jnp.int32).at[sequence[jnp.where(places < fixed, places, moved)]].set(jnp.asarray(tallies, jnp.int32))

    tallies = jnp.where(number % 4 == 0, named(packed, number // 4), named(common, number - number // 4 - 1))
    mixed = jax.random.permutation(jax.random.fold_in(own, 3), count)
    source_of, sink = mixed[0:count // 2 * 2:2], mixed[1:count // 2 * 2:2]
    slack = jnp.minimum(tallies[source_of] - 1, bound - tallies[sink]) // 2
    slack = jnp.where((source_of == sequence[0]) | (sink == sequence[0]) | (tallies[sink] == 0), 0, jnp.maximum(slack, 0))
    moved = jax.random.randint(jax.random.fold_in(own, 4), (count // 2,), 0, 1 << 20) % (slack + 1)
    tallies = tallies.at[source_of].add(-moved).at[sink].add(moved)
    members = jnp.searchsorted(jnp.cumsum(tallies), jnp.arange(rows * top), side="right").astype(jnp.int32)
    table = members.reshape(top, rows).T
    table = table[jax.random.permutation(jax.random.fold_in(own, 1), rows)]
    turn = jax.random.randint(jax.random.fold_in(own, 2), (rows, 1), 0, top)
    return jnp.take_along_axis(table, (jnp.arange(top)[None, :] + turn) % top, axis=1)


def load_shares(number_of, total, reach, lean, full):
    portions = [(1 << 20) // math.isqrt(grade ** lean) + 1 for grade in range(1, number_of + 1)]
    largest = reach if full else min(reach, max(-(-total // number_of), total * portions[0] // sum(portions)))
    least = 1 if total - largest >= number_of - 1 else 0
    holding, surplus = [largest] + [least] * (number_of - 1), total - largest - least * (number_of - 1)
    while surplus > 0:
        candidates = [i for i in range(1, number_of) if holding[i] < largest] or [i for i in range(1, number_of) if holding[i] < reach]
        mass, remaining = sum([portions[i] for i in candidates]), surplus
        for i in candidates:
            more = min(reach - holding[i], max(1, remaining * portions[i] // mass), surplus)
            holding[i] = holding[i] + more
            surplus = surplus - more
    return np.array(holding)


def scatter_about(rng, dims, deviation, most, pieces=(), held_as=jnp.bfloat16):
    values = deviation * jax.random.normal(rng, dims, jnp.float32)
    if pieces:
        values = values * steps_of(rng, dims, pieces, -0.22, 0.18)
    return jnp.clip(values, -most, most).astype(held_as)


def setup_inputs(seed: int = 0) -> dict:
    arg_keys = jax.random.split(jax.random.key(seed), 24)
    residual = scatter_about(arg_keys[0], (SEQ, D), 1.0, 6.0, ((0, 256),))
    output_gate_projected = scatter_about(arg_keys[1], (SEQ, INNER), 1.0, 6.0, ((0, 64), (1, 4)))
    value_projected_input = scatter_about(arg_keys[2], (SEQ, INNER), 1.0, 6.0, ((0, 64), (1, 4)))
    state_projected_input = scatter_about(arg_keys[3], (SEQ, HEAD_GROUPS * STATE), 1.0, 6.0, ((0, 64), (1, 4)))
    readout_projected_input = scatter_about(arg_keys[4], (SEQ, HEAD_GROUPS * STATE), 1.0, 6.0, ((0, 64), (1, 4)))
    step_preactivation = draw_step_preactivation(jax.random.fold_in(arg_keys[23], 71), 0)
    position_decay_extra = draw_position_decay_extra(jax.random.fold_in(arg_keys[23], 71), 0)
    value_conv_kernel = scatter_about(arg_keys[7], (CONV, INNER), 0.05, 0.29882812, ((1, 4),))
    state_conv_kernel = scatter_about(arg_keys[8], (CONV, HEAD_GROUPS * STATE), 0.15, 0.8984375, ((1, 4),))
    readout_conv_kernel = scatter_about(arg_keys[9], (CONV, HEAD_GROUPS * STATE), 0.15, 0.8984375, ((1, 4),))
    head_log_decay_rates = draw_head_log_decay_rates(jax.random.fold_in(arg_keys[23], 71), 0)
    head_direct_weight = jnp.clip(jnp.exp(math.log(4.0) - 2.0794415 * jax.random.uniform(arg_keys[11], (HEADS,), jnp.float32) ** steps_of(arg_keys[11], (HEADS,), ((0, 4),), -0.2, 0.2)), 0.5, 4.0)
    head_norm_gain = jnp.clip(1.0 + 0.18 * jax.random.normal(arg_keys[12], (INNER,), jnp.float32), 0.1, 1.9)
    mixer_output_weight = scatter_about(arg_keys[13], (INNER, D), INNER ** -0.5, 0.09375, ((0, 4),))
    expert_norm_gain = jnp.clip(1.0 + 0.18 * jax.random.normal(arg_keys[14], (D,), jnp.float32), 0.1, 1.9)
    routed_expert_index_keys = jax.random.split(jax.random.fold_in(arg_keys[15], 1), SEQ // ROWS)
    routed_expert_index_turns = jax.random.permutation(jax.random.fold_in(arg_keys[15], 3), SEQ // ROWS)
    routed_expert_index = jax.vmap(lambda own, number: assign_block(jax.random.fold_in(arg_keys[15], 2), own, number, ROWS, EXPERTS, TOPK, CAP, 2))(routed_expert_index_keys, routed_expert_index_turns).reshape((SEQ, TOPK))
    routed_expert_weight = jnp.clip(0.2 + 0.8 * jax.random.uniform(arg_keys[16], (SEQ, TOPK), jnp.float32) ** steps_of(arg_keys[16], (SEQ, TOPK), ((0, 256),), -0.2, 0.2), 0.2, 1.0)
    routed_gate_weight = scatter_about(arg_keys[17], (EXPERTS, D, FE), D ** -0.5, 0.125, ((0, 64),))
    routed_up_weight = scatter_about(arg_keys[18], (EXPERTS, D, FE), D ** -0.5, 0.125, ((0, 64),))
    routed_down_weight = scatter_about(arg_keys[19], (EXPERTS, FE, D), FE ** -0.5, 0.375, ((0, 64),))
    common_gate_weight = scatter_about(arg_keys[20], (D, FS), D ** -0.5, 0.125, ((1, 4),))
    common_up_weight = scatter_about(arg_keys[21], (D, FS), D ** -0.5, 0.125, ((1, 4),))
    common_down_weight = scatter_about(arg_keys[22], (D, FS), FS ** -0.5, 0.25, ((1, 4),))
    return dict(residual=residual, output_gate_projected=output_gate_projected, value_projected_input=value_projected_input, state_projected_input=state_projected_input, readout_projected_input=readout_projected_input, step_preactivation=step_preactivation, position_decay_extra=position_decay_extra, value_conv_kernel=value_conv_kernel, state_conv_kernel=state_conv_kernel, readout_conv_kernel=readout_conv_kernel, head_log_decay_rates=head_log_decay_rates, head_direct_weight=head_direct_weight, head_norm_gain=head_norm_gain, mixer_output_weight=mixer_output_weight, expert_norm_gain=expert_norm_gain, routed_expert_index=routed_expert_index, routed_expert_weight=routed_expert_weight, routed_gate_weight=routed_gate_weight, routed_up_weight=routed_up_weight, routed_down_weight=routed_down_weight, common_gate_weight=common_gate_weight, common_up_weight=common_up_weight, common_down_weight=common_down_weight)


EPSILON = 1e-06
HIGHEST_PRECISION = lax.Precision.HIGHEST

def short_conv(inputs, weights):
    length = inputs.shape[0]
    padded = jnp.pad(inputs.astype(jnp.float32), ((CONV - 1, 0), (0, 0)))
    totals = jnp.zeros((length, inputs.shape[1]), jnp.float32)
    for tap_index in range(CONV):
        totals = totals + padded[tap_index:tap_index + length] * weights[tap_index].astype(jnp.float32)
    return jax.nn.silu(totals)

def swiglu_rows(rows, gate_weight, up_weight, down_weight):
    gate_part = jnp.dot(rows, gate_weight, preferred_element_type=jnp.float32)
    lifted = jnp.dot(rows, up_weight, preferred_element_type=jnp.float32)
    hidden = (jax.nn.silu(gate_part) * lifted).astype(jnp.bfloat16)
    return jnp.dot(hidden, down_weight, preferred_element_type=jnp.float32)

def reference(residual, output_gate_projected, value_projected_input, state_projected_input, readout_projected_input, step_preactivation, position_decay_extra, value_conv_kernel, state_conv_kernel, readout_conv_kernel, head_log_decay_rates, head_direct_weight, head_norm_gain, mixer_output_weight, expert_norm_gain, routed_expert_index, routed_expert_weight, routed_gate_weight, routed_up_weight, routed_down_weight, common_gate_weight, common_up_weight, common_down_weight):
    heads_per_group = HEADS // HEAD_GROUPS
    block_list = SEQ // BLOCK_POSITIONS
    values = short_conv(value_projected_input, value_conv_kernel).reshape(block_list, BLOCK_POSITIONS, HEAD_GROUPS, heads_per_group, HEAD_DIM)
    state_in = short_conv(state_projected_input, state_conv_kernel).reshape(block_list, BLOCK_POSITIONS, HEAD_GROUPS, STATE)
    readout = short_conv(readout_projected_input, readout_conv_kernel).reshape(block_list, BLOCK_POSITIONS, HEAD_GROUPS, STATE)
    head_step_lengths = jax.nn.softplus(step_preactivation)
    decay_logarithm = (head_step_lengths * (-jnp.exp(head_log_decay_rates))[None, :] + position_decay_extra).reshape(block_list, BLOCK_POSITIONS, HEAD_GROUPS, heads_per_group)
    head_step_lengths = head_step_lengths.reshape(block_list, BLOCK_POSITIONS, HEAD_GROUPS, heads_per_group)
    gates = output_gate_projected.reshape(block_list, BLOCK_POSITIONS, HEADS, HEAD_DIM)
    streams = residual.reshape(block_list, BLOCK_POSITIONS, D)
    skips = head_direct_weight.reshape(HEAD_GROUPS, heads_per_group)
    gains = head_norm_gain.reshape(HEADS, HEAD_DIM)
    out_parts = mixer_output_weight.astype(jnp.float32).reshape(N_TP, INNER // N_TP, D)
    causal = jnp.arange(BLOCK_POSITIONS)[:, None] >= jnp.arange(BLOCK_POSITIONS)[None, :]

    def block_step(carried, block_inputs):
        value_blk, input_blk, readout_blk, decay_blk, sizes_blk, gate_blk, stream_blk = block_inputs
        cumulative = jnp.cumsum(decay_blk, axis=0)
        weighted_output = value_blk * sizes_blk[..., None]
        by_head = jnp.transpose(cumulative, (1, 2, 0))
        span_logs = by_head[:, :, :, None] - by_head[:, :, None, :]
        decay_factors = jnp.exp(jnp.where(causal, span_logs, -jnp.inf))
        attention_scores = jnp.einsum('tgn,sgn->gts', readout_blk, input_blk, precision=HIGHEST_PRECISION)
        within_block_output = jnp.einsum('wkij,jwke->iwke', attention_scores[:, None] * decay_factors, weighted_output, precision=HIGHEST_PRECISION)
        carried_out = jnp.einsum('tgn,grpn->tgrp', readout_blk, carried, precision=HIGHEST_PRECISION) * jnp.exp(cumulative)[..., None]
        mixed_heads = within_block_output + carried_out + skips[None, :, :, None] * value_blk
        to_end = jnp.exp(cumulative[-1:] - cumulative)
        fresh_state = jnp.einsum('sgn,sgrp->grpn', input_blk, weighted_output * to_end[..., None], precision=HIGHEST_PRECISION)
        carried = jnp.exp(cumulative[-1])[..., None, None] * carried + fresh_state
        mixed_heads = mixed_heads.reshape(BLOCK_POSITIONS, HEADS, HEAD_DIM) * jax.nn.silu(gate_blk.astype(jnp.float32))
        normed = mixed_heads * lax.rsqrt(lax.optimization_barrier(jnp.mean(mixed_heads * mixed_heads, axis=-1, keepdims=True)) + EPSILON) * gains
        heads_out = lax.optimization_barrier(normed.astype(jnp.bfloat16)).astype(jnp.float32)
        heads_out = heads_out.reshape(BLOCK_POSITIONS, N_TP, INNER // N_TP)
        partials = jnp.einsum('tqi,qid->qtd', heads_out, out_parts).astype(jnp.bfloat16)
        partials = lax.optimization_barrier(partials).astype(jnp.float32)
        stream = stream_blk.astype(jnp.float32) + lax.optimization_barrier(jnp.sum(partials, axis=0))
        return (carried, stream.astype(jnp.bfloat16))
    start_state = jnp.zeros((HEAD_GROUPS, heads_per_group, HEAD_DIM, STATE), jnp.float32)
    _, stream = lax.scan(block_step, start_state, (values, state_in, readout, decay_logarithm, head_step_lengths, gates, streams))
    stream = stream.reshape(SEQ, D).astype(jnp.float32)
    normed_rows = (stream * lax.rsqrt(lax.optimization_barrier(jnp.mean(stream * stream, axis=-1, keepdims=True)) + EPSILON) * expert_norm_gain).astype(jnp.bfloat16)
    shared = swiglu_rows(normed_rows, common_gate_weight, common_up_weight, common_down_weight.T)
    group_rows = 128
    tokens = SEQ
    assignments = tokens * TOPK
    flat_ids = routed_expert_index.reshape(-1).astype(jnp.int32)
    sort_order = jnp.argsort(flat_ids).astype(jnp.int32)
    sorted_ids = flat_ids[sort_order]
    counts = lax.optimization_barrier(jnp.sum((flat_ids[:, None] == jnp.arange(EXPERTS, dtype=jnp.int32)[None, :]).astype(jnp.int32), axis=0)).astype(jnp.int32)
    padded = ((counts + group_rows - 1) // group_rows * group_rows).astype(jnp.int32)
    starts = (jnp.cumsum(counts) - counts).astype(jnp.int32)
    pad_end = jnp.cumsum(padded).astype(jnp.int32)
    pad_start = (pad_end - padded).astype(jnp.int32)
    destination = (pad_start[sorted_ids] + jnp.arange(assignments, dtype=jnp.int32) - starts[sorted_ids]).astype(jnp.int32)
    nblocks = -(-assignments // group_rows) + EXPERTS
    rows_total = nblocks * group_rows
    row_token = jnp.full((rows_total,), tokens, jnp.int32).at[destination].set((sort_order // TOPK).astype(jnp.int32))
    row_weight = jnp.zeros((rows_total,), jnp.float32).at[destination].set(routed_expert_weight.reshape(-1)[sort_order])
    block_expert = jnp.minimum(jnp.searchsorted(pad_end, jnp.arange(nblocks, dtype=jnp.int32) * group_rows, side='right'), EXPERTS - 1).astype(jnp.int32)
    padded_rows = jnp.concatenate([normed_rows, jnp.zeros((1, D), jnp.bfloat16)], axis=0)

    def expert_block(block_args):
        token_ids, expert_id = block_args
        chosen = padded_rows[token_ids]
        return swiglu_rows(chosen, routed_gate_weight[expert_id], routed_up_weight[expert_id], routed_down_weight[expert_id]).astype(jnp.bfloat16)
    outputs = lax.map(expert_block, (row_token.reshape(nblocks, group_rows), block_expert))
    contrib = outputs.reshape(rows_total, D).astype(jnp.float32) * row_weight[:, None]
    routed = jnp.zeros((tokens + 1, D), jnp.float32).at[row_token].add(contrib)[:tokens]
    return (stream + shared + routed).astype(jnp.bfloat16)
```

```python
import jax
import jax.numpy as jnp
from jax import lax
from jax.experimental import pallas as pl
from jax.experimental.pallas import tpu as pltpu
from jax.sharding import Mesh
from jax.sharding import PartitionSpec as P

D = 2048
HEAD_DIM = 64
STATE = 128
CONV = 4
BLOCK_POSITIONS = 128
SP = ("sp_0", "sp_1", "sp_2")
SP_TP = ("sp_0", "sp_1", "sp_2", "tp")


EPSILON = 1e-06


def shifted(value, axis, steps):
    count = lax.axis_size(axis)
    first, last = (max(0, -steps), min(count, count - steps))
    return lax.ppermute(value, axis, [(source, source + steps) for source in range(first, last)])


def filled_with(array, identity):
    return jax.tree.map(
        lambda part, zero: jnp.zeros_like(part) + jnp.asarray(zero, part.dtype), array, identity
    )


def carried_in(array, axes, combine, identity):
    before = start = filled_with(array, identity)
    total = array
    for axis in reversed(axes):
        size, index = (lax.axis_size(axis), lax.axis_index(axis))
        pieces = jax.tree.map(
            lambda part, kind: lax.all_gather(part.astype(kind), axis),
            total,
            (jnp.bfloat16, jnp.bfloat16),
        )
        inside, total = (start, start)
        for k in range(size):
            passed = k < index
            total = combine(
                total, jax.tree.map(lambda part, own: part[k].astype(own.dtype), pieces, array)
            )
            inside = jax.tree.map(lambda new, old: jnp.where(passed, new, old), total, inside)
        before = combine(inside, before)
    return before


def cut_along(array, dim, size):
    lengths = array.shape
    blocks = array.reshape(*lengths[:dim], size, lengths[dim] // size, *lengths[dim + 1 :])
    return jnp.moveaxis(blocks, dim, 0)


def sum_at_owner(array, axis, dim):
    size = lax.axis_size(axis)
    blocks = lax.all_to_all(cut_along(array, dim, size), axis, 0, 0, tiled=True)
    return jnp.sum(blocks.astype(jnp.float32), axis=0)


def sent_together(arrays, axis, dim, along):
    widths = [a.shape[along] for a in arrays]
    both = jnp.concatenate(arrays, axis=along)
    filled = lax.all_gather(both, axis, axis=dim, tiled=True)
    return tuple(jnp.split(filled, [sum(widths[:k]) for k in range(1, len(widths))], axis=along))


def short_conv(inputs, rim_rows, weights):
    length = inputs.shape[0]
    extended = jnp.concatenate([rim_rows, inputs], axis=0)
    totals = jnp.zeros(inputs.shape, jnp.float32)
    for tap_index in range(CONV):
        totals = totals + extended[tap_index : tap_index + length].astype(jnp.float32) * weights[
            tap_index
        ].astype(jnp.float32)
    return jax.nn.silu(totals)


def shared_part(rows, gate_piece, up_piece, down_piece):
    gate_part = jnp.dot(rows, gate_piece, preferred_element_type=jnp.float32)
    lifted = jnp.dot(rows, up_piece, preferred_element_type=jnp.float32)
    hidden = (jax.nn.silu(gate_part) * lifted).astype(jnp.bfloat16)
    return jnp.einsum("rc,dc->rd", hidden, down_piece, preferred_element_type=jnp.float32)


def join_states(earlier, later):
    return (earlier[0] * later[0], later[0][..., None, None] * earlier[1] + later[1])


MESH = pl.DeviceIdType.MESH
BF16 = jnp.bfloat16
F32 = jnp.float32
NZ, NY, NC, NX = 8, 4, 2, 4
PLANE = NY * NC
ROWS = 64
HALF = ROWS // 2
CAP = 8
FE = 256


def place():
    return tuple(lax.axis_index(name) for name in SP_TP)


def device(z, y, c, x):
    return {"sp_0": z, "sp_1": y, "sp_2": c, "tp": x}


def remote(src, dst, send_sem, recv_sem, target):
    return pltpu.make_async_remote_copy(
        src_ref=src,
        dst_ref=dst,
        send_sem=send_sem,
        recv_sem=recv_sem,
        device_id=target,
        device_id_type=MESH,
    )


def arrive(ref, sem):
    pltpu.make_async_copy(ref, ref, sem).wait()


def greet(targets):
    barrier = pltpu.get_barrier_semaphore()
    for target in targets:
        pl.semaphore_signal(barrier, inc=1, device_id=target, device_id_type=MESH)
    pl.semaphore_wait(barrier, len(targets))


def moe_kernel(
    rows,
    stream,
    meta,
    rg_hbm,
    ru_hbm,
    rd_hbm,
    cg_hbm,
    cu_hbm,
    cd_hbm,
    out,
    zall,
    metas,
    combine_w,
    send_rows,
    expert_rows,
    expert_out,
    back_rows,
    rs_send,
    rs_recv,
    xall,
    sh_send,
    sh_recv,
    rg,
    ru,
    rd,
    cg,
    cu,
    cd,
    w_sem,
    zs_sem,
    zr_sem,
    ms_sem,
    mr_sem,
    ds_sem,
    dr_sem,
    bs_sem,
    br_sem,
    rss_sem,
    rsr_sem,
    xs_sem,
    xr_sem,
    hs_sem,
    hr_sem,
):
    z, y, c, x = place()
    me = y * NC + c
    z_up, z_down = lax.rem(z + 1, NZ), lax.rem(z + NZ - 1, NZ)
    z_peers = [device(lax.rem(z + d, NZ), y, c, x) for d in range(1, NZ)]
    x_peers = [device(z, y, c, lax.rem(x + d, NX)) for d in range(1, NX)]
    plane_peers = []
    for dy in (1, 3, 2, 0):
        for dc in range(NC):
            if dy or dc:
                yy, cc = lax.rem(y + dy, NY), lax.rem(c + dc, NC)
                plane_peers.append((yy * NC + cc, device(z, yy, cc, x)))

    weights = [
        pltpu.make_async_copy(far, near, w_sem.at[k])
        for k, (far, near) in enumerate(
            ((cg_hbm, cg), (cu_hbm, cu), (cd_hbm, cd), (rg_hbm, rg), (ru_hbm, ru), (rd_hbm, rd))
        )
    ]
    for copy in weights:
        copy.start()
    greet(z_peers + x_peers + [peer for _, peer in plane_peers])

    ring = []

    def hop(step, up, half):
        lo = half * HALF
        here = ((NZ - step) % NZ) if up else step
        there = ((NZ - step - 1) % NZ) if up else step + 1
        source = rows if step == 0 else zall.at[here]
        k = 0 if up else 1
        copy = remote(
            source.at[pl.ds(lo, HALF)],
            zall.at[there, pl.ds(lo, HALF)],
            zs_sem.at[k, step, half],
            zr_sem.at[k, step, half],
            device(z_up if up else z_down, y, c, x),
        )
        copy.start()
        ring.append(copy)

    def ring_arrived(step, up, half):
        lo = half * HALF
        there = ((NZ - step - 1) % NZ) if up else step + 1
        arrive(zall.at[there, pl.ds(lo, HALF)], zr_sem.at[0 if up else 1, step, half])

    meta_copies = [
        remote(meta, metas.at[NZ - d], ms_sem.at[d - 1], mr_sem.at[NZ - d - 1], z_peers[d - 1])
        for d in range(1, NZ)
    ]
    for copy in meta_copies:
        copy.start()
    for half in range(2):
        hop(0, True, half)
        hop(0, False, half)
    x_copies = [
        remote(rows, xall.at[x], xs_sem.at[d - 1], xr_sem.at[NX - d - 1], x_peers[d - 1])
        for d in range(1, NX)
    ]
    for copy in x_copies:
        copy.start()

    token = lax.broadcasted_iota(jnp.int32, (ROWS, ROWS), 0)
    later = lax.broadcasted_iota(jnp.int32, (ROWS, ROWS), 1)
    before = jnp.where(token < later, 1.0, 0.0).astype(BF16)
    expert_row = lax.broadcasted_iota(jnp.int32, (PLANE, ROWS), 0) + z * PLANE
    expert_row = expert_row.astype(F32)
    slot = lax.broadcasted_iota(jnp.int32, (PLANE, CAP, ROWS), 1).astype(F32)
    sends = []

    def dispatch(o):
        table = meta[...] if o == 0 else metas[o]
        hits = jnp.zeros((PLANE, ROWS), F32)
        shares = jnp.zeros((PLANE, ROWS), F32)
        for k in range(4):
            hit = jnp.where(expert_row == table[k : k + 1, :ROWS], 1.0, 0.0)
            hits = hits + hit
            shares = shares + hit * table[4 + k : 5 + k, :ROWS]
        rank = jnp.dot(hits.astype(BF16), before, preferred_element_type=F32)
        chosen = jnp.where(
            (rank[:, None, :] == slot) & (hits[:, None, :] > 0.5),
            jnp.ones((PLANE, CAP, ROWS), F32),
            jnp.zeros((PLANE, CAP, ROWS), F32),
        )
        combine_w[o] = (chosen * shares[:, None, :]).reshape(ROWS, ROWS)
        block = rows[...] if o == 0 else zall[o]
        packed = jnp.dot(
            chosen.reshape(ROWS, ROWS).astype(BF16), block, preferred_element_type=F32
        )
        send_rows[o] = packed.reshape(PLANE, CAP, D).astype(BF16)
        for index, peer in plane_peers:
            copy = remote(
                send_rows.at[o, index], expert_rows.at[o, me], ds_sem.at[o], dr_sem.at[o], peer
            )
            copy.start()
        sends.append((send_rows.at[o], ds_sem.at[o]))
        expert_rows[o, me] = send_rows[o, me]

    def run_expert(blocks):
        for o in blocks:
            arrive(expert_rows.at[o, pl.ds(0, PLANE - 1)], dr_sem.at[o])
        inputs = jnp.concatenate(
            [expert_rows[o].astype(F32).reshape(ROWS, D) for o in blocks], axis=0
        ).astype(BF16)
        gate = jnp.dot(inputs, rg[...], preferred_element_type=F32)
        lifted = jnp.dot(inputs, ru[...], preferred_element_type=F32)
        hidden = (jax.nn.silu(gate) * lifted).astype(BF16)
        result = jnp.dot(hidden, rd[...], preferred_element_type=F32)
        for k, o in enumerate(blocks):
            expert_out[o] = (
                result[k * ROWS : (k + 1) * ROWS].reshape(PLANE, CAP, D).astype(BF16)
            )

    def give_back(o):
        for index, peer in plane_peers:
            copy = remote(
                expert_out.at[o, index], back_rows.at[o, me], bs_sem.at[o], br_sem.at[o], peer
            )
            copy.start()
        sends.append((expert_out.at[o], bs_sem.at[o]))
        back_rows[o, me] = expert_out[o, me]

    def combined(o):
        arrive(back_rows.at[o, pl.ds(0, PLANE - 1)], br_sem.at[o])
        returned = back_rows[o].astype(F32).reshape(ROWS, D).astype(BF16)
        return lax.dot_general(
            combine_w[o].astype(BF16),
            returned,
            (((0,), (0,)), ((), ())),
            preferred_element_type=F32,
        )

    dispatch(0)
    for d in range(1, NZ):
        arrive(metas.at[NZ - d], mr_sem.at[NZ - d - 1])
    for half in range(2):
        for up in (True, False):
            ring_arrived(0, up, half)
            hop(1, up, half)
    dispatch(7)
    dispatch(1)
    for copy in weights:
        copy.wait()
    run_expert((0,))
    for half in range(2):
        for up in (True, False):
            ring_arrived(1, up, half)
            hop(2, up, half)
    dispatch(6)
    dispatch(2)
    run_expert((7, 1))
    ring_arrived(2, True, 0)
    hop(3, True, 0)
    ring_arrived(2, False, 1)
    hop(3, False, 1)
    ring_arrived(2, True, 1)
    ring_arrived(2, False, 0)
    dispatch(5)
    dispatch(3)
    run_expert((6, 2))

    for d in range(1, NX):
        arrive(xall.at[0], xr_sem.at[d - 1])
    xall[x] = rows[...]
    share_copies = []
    hidden_rows = xall[...].reshape(NX * ROWS, D)
    gate = jnp.dot(hidden_rows, cg[...], preferred_element_type=F32)
    lifted = jnp.dot(hidden_rows, cu[...], preferred_element_type=F32)
    hidden = (jax.nn.silu(gate) * lifted).astype(BF16)
    shared = lax.dot_general(
        hidden, cd[...], (((1,), (1,)), ((), ())), preferred_element_type=F32
    )
    sh_send[...] = shared.reshape(NX, ROWS, D).astype(BF16)
    for d in range(1, NX):
        xx = lax.rem(x + d, NX)
        copy = remote(
            sh_send.at[xx],
            sh_recv.at[NX - d - 1],
            hs_sem.at[d - 1],
            hr_sem.at[NX - d - 1],
            x_peers[d - 1],
        )
        copy.start()
        share_copies.append(copy)

    ring_arrived(3, True, 0)
    ring_arrived(3, False, 1)
    dispatch(4)
    run_expert((5, 3))
    run_expert((4,))
    for o in (4, 3, 5, 2, 6, 1, 7, 0):
        give_back(o)

    def pass_on(step, up, half):
        k = 0 if up else 1
        lo = half * HALF
        copy = remote(
            rs_send.at[k, step, pl.ds(lo, HALF)],
            rs_recv.at[k, step, pl.ds(lo, HALF)],
            rss_sem.at[k, step, half],
            rsr_sem.at[k, step, half],
            device(z_up if up else z_down, y, c, x),
        )
        copy.start()
        ring.append(copy)

    def sum_arrived(step, up, half):
        k = 0 if up else 1
        part = rs_recv.at[k, step, pl.ds(half * HALF, HALF)]
        arrive(part, rsr_sem.at[k, step, half])
        return rs_recv[k, step, pl.ds(half * HALF, HALF)].astype(F32)

    first = combined(4).astype(BF16)
    rs_send[0, 0, :HALF] = first[:HALF]
    pass_on(0, True, 0)
    rs_send[1, 0, HALF:] = first[HALF:]
    pass_on(0, False, 1)
    for step in range(1, 4):
        parts = (combined(4 - step), combined(4 + step))
        for turn in range(2):
            for k, up in enumerate((True, False)):
                half = turn if up else 1 - turn
                piece = parts[k][half * HALF : (half + 1) * HALF]
                if step > 1 or turn == 0:
                    piece = piece + sum_arrived(step - 1, up, half)
                rs_send[k, step, pl.ds(half * HALF, HALF)] = piece.astype(BF16)
                pass_on(step, up, half)
    total = combined(0) + stream[...].astype(F32)
    total = total + sh_send[x].astype(F32)
    for d in range(1, NX):
        arrive(sh_recv.at[d - 1], hr_sem.at[d - 1])
        total = total + sh_recv[d - 1].astype(F32)
    for half in range(2):
        piece = total[half * HALF : (half + 1) * HALF]
        for up in (True, False):
            piece = piece + sum_arrived(3, up, half if up else half)
        out[half * HALF : (half + 1) * HALF] = piece.astype(BF16)

    for copy in ring + meta_copies + x_copies + share_copies:
        copy.wait_send()
    for ref, sem in sends:
        arrive(ref.at[pl.ds(0, PLANE - 1)], sem)


def moe(rows, stream, meta, rg, ru, rd, cg, cu, cd):
    vmem = pl.BlockSpec(memory_space=pltpu.VMEM)
    hbm = pl.BlockSpec(memory_space=pl.ANY)
    blocks = (NZ, PLANE, CAP, D)
    dma = pltpu.SemaphoreType.DMA
    return pl.pallas_call(
        moe_kernel,
        out_shape=jax.ShapeDtypeStruct((ROWS, D), BF16),
        in_specs=[vmem] * 3 + [hbm] * 6,
        out_specs=vmem,
        scratch_shapes=[
            pltpu.VMEM((NZ, ROWS, D), BF16),
            pltpu.VMEM((NZ, 8, 128), F32),
            pltpu.VMEM((NZ, ROWS, ROWS), F32),
            pltpu.VMEM(blocks, BF16),
            pltpu.VMEM(blocks, BF16),
            pltpu.VMEM(blocks, BF16),
            pltpu.VMEM(blocks, BF16),
            pltpu.VMEM((2, 4, ROWS, D), BF16),
            pltpu.VMEM((2, 4, ROWS, D), BF16),
            pltpu.VMEM((NX, ROWS, D), BF16),
            pltpu.VMEM((NX, ROWS, D), BF16),
            pltpu.VMEM((NX - 1, ROWS, D), BF16),
            pltpu.VMEM(rg.shape, BF16),
            pltpu.VMEM(ru.shape, BF16),
            pltpu.VMEM(rd.shape, BF16),
            pltpu.VMEM(cg.shape, BF16),
            pltpu.VMEM(cu.shape, BF16),
            pltpu.VMEM(cd.shape, BF16),
            dma((6,)),
            dma((2, 4, 2)),
            dma((2, 4, 2)),
            dma((NZ - 1,)),
            dma((NZ - 1,)),
            dma((NZ,)),
            dma((NZ,)),
            dma((NZ,)),
            dma((NZ,)),
            dma((2, 4, 2)),
            dma((2, 4, 2)),
            dma((NX - 1,)),
            dma((NX - 1,)),
            dma((NX - 1,)),
            dma((NX - 1,)),
        ],
        compiler_params=pltpu.CompilerParams(
            collective_id=1, has_side_effects=True, vmem_limit_bytes=56 * 1024 * 1024
        ),
    )(rows, stream, meta, rg, ru, rd, cg, cu, cd)


def shards(
    residual,
    output_gate_projected,
    value_projected_input,
    state_projected_input,
    readout_projected_input,
    step_preactivation,
    position_decay_extra,
    value_conv_kernel,
    state_conv_kernel,
    readout_conv_kernel,
    head_log_decay_rates,
    head_direct_weight,
    head_norm_gain,
    mixer_output_weight,
    expert_norm_gain,
    routed_expert_index,
    routed_expert_weight,
    routed_gate_weight,
    routed_up_weight,
    routed_down_weight,
    common_gate_weight,
    common_up_weight,
    common_down_weight,
):
    head_count = step_preactivation.shape[1]
    groups = state_projected_input.shape[1] // STATE
    heads_per_group = head_count // groups
    length = value_projected_input.shape[0]
    block_list = length // BLOCK_POSITIONS
    conv_tails = (
        value_projected_input[length - CONV + 1 :],
        state_projected_input[length - CONV + 1 :],
        readout_projected_input[length - CONV + 1 :],
    )
    value_rim, input_rim, readout_rim = shifted(
        (conv_tails[0], conv_tails[1], conv_tails[2]), SP, 1
    )
    values = short_conv(value_projected_input, value_rim, value_conv_kernel).reshape(
        block_list, BLOCK_POSITIONS, groups, heads_per_group, HEAD_DIM
    )
    state_in = short_conv(state_projected_input, input_rim, state_conv_kernel).reshape(
        block_list, BLOCK_POSITIONS, groups, STATE
    )
    readout = short_conv(readout_projected_input, readout_rim, readout_conv_kernel).reshape(
        block_list, BLOCK_POSITIONS, groups, STATE
    )
    head_step_lengths = jax.nn.softplus(step_preactivation)
    decay_logarithm = (
        head_step_lengths * (-jnp.exp(head_log_decay_rates))[None, :] + position_decay_extra
    ).reshape(block_list, BLOCK_POSITIONS, groups, heads_per_group)
    head_step_lengths = head_step_lengths.reshape(
        block_list, BLOCK_POSITIONS, groups, heads_per_group
    )
    causal = jnp.arange(BLOCK_POSITIONS)[:, None] >= jnp.arange(BLOCK_POSITIONS)[None, :]
    cumulative = jnp.cumsum(decay_logarithm, axis=1)
    weighted_output = values * head_step_lengths[..., None]
    by_head = jnp.transpose(cumulative, (0, 2, 3, 1))
    span_logs = by_head[..., :, None] - by_head[..., None, :]
    decay_factors = jnp.exp(jnp.where(causal, span_logs, -jnp.inf))
    attention_scores = jnp.einsum("ctgn,csgn->cgts", readout, state_in)
    within_block_output = jnp.einsum(
        "cgrts,csgrp->ctgrp", attention_scores[:, :, None] * decay_factors, weighted_output
    )
    to_end = jnp.exp(cumulative[:, -1:] - cumulative)
    fresh_state = jnp.einsum("csgn,csgrp->cgrpn", state_in, weighted_output * to_end[..., None])
    block_decay = jnp.exp(cumulative[:, -1])

    def block_chain(carried, block_item):
        state_now, factor = carried
        decay_blk, fresh_blk = block_item
        return (
            (decay_blk[..., None, None] * state_now + fresh_blk, decay_blk * factor),
            (state_now, factor),
        )

    empty_state = jnp.zeros((groups, heads_per_group, HEAD_DIM, STATE), jnp.float32)
    unit_decay = jnp.ones((groups, heads_per_group), jnp.float32)
    (own_state, own_decay), (local_start, local_factor) = lax.scan(
        block_chain, (empty_state, unit_decay), (block_decay, fresh_state)
    )
    incoming = carried_in((own_decay, own_state), SP, join_states, (unit_decay, empty_state))
    start_states = local_start + local_factor[..., None, None] * incoming[1][None]
    carried_out = (
        jnp.einsum("ctgn,cgrpn->ctgrp", readout, start_states) * jnp.exp(cumulative)[..., None]
    )
    mixed_heads = (
        within_block_output
        + carried_out
        + head_direct_weight.reshape(groups, heads_per_group)[None, None, :, :, None] * values
    )
    mixed_heads = mixed_heads.reshape(length, head_count, HEAD_DIM) * jax.nn.silu(
        output_gate_projected.reshape(length, head_count, HEAD_DIM).astype(jnp.float32)
    )
    normed = mixed_heads * lax.rsqrt(
        jnp.mean(mixed_heads * mixed_heads, axis=-1, keepdims=True) + EPSILON
    )
    heads_out = (
        (normed * head_norm_gain.reshape(head_count, HEAD_DIM))
        .astype(jnp.bfloat16)
        .reshape(length, head_count * HEAD_DIM)
    )
    row_count = residual.shape[0]
    mix_sum = sum_at_owner(
        jnp.dot(heads_out, mixer_output_weight, preferred_element_type=jnp.float32).astype(
            jnp.bfloat16
        ),
        "tp",
        0,
    )
    stream = (residual.astype(jnp.float32) + mix_sum).astype(jnp.bfloat16)
    stream_wide = stream.astype(jnp.float32)
    normed_rows = (
        stream_wide
        * lax.rsqrt(jnp.mean(stream_wide * stream_wide, axis=-1, keepdims=True) + EPSILON)
        * expert_norm_gain
    ).astype(jnp.bfloat16)
    meta = jnp.concatenate(
        [routed_expert_index.T.astype(F32), routed_expert_weight.T.astype(F32)], axis=0
    )
    meta = jnp.pad(meta, ((0, 0), (0, 128 - row_count)))
    return moe(
        normed_rows,
        stream,
        meta,
        routed_gate_weight[0],
        routed_up_weight[0],
        routed_down_weight[0],
        common_gate_weight,
        common_up_weight,
        common_down_weight,
    )


def solution(mesh):
    torus = Mesh(mesh.devices.reshape(8, 4, 2, mesh.shape["tp"]), ("sp_0", "sp_1", "sp_2", "tp"))
    return jax.shard_map(
        shards,
        mesh=torus,
        in_specs=(
            P(SP_TP, None),
            P(SP, "tp"),
            P(SP, "tp"),
            P(SP, "tp"),
            P(SP, "tp"),
            P(SP, "tp"),
            P(SP, "tp"),
            P(None, "tp"),
            P(None, "tp"),
            P(None, "tp"),
            P("tp"),
            P("tp"),
            P("tp"),
            P("tp", None),
            P(),
            P(SP_TP, None),
            P(SP_TP, None),
            P(SP, None, None),
            P(SP, None, None),
            P(SP, None, None),
            P(None, "tp"),
            P(None, "tp"),
            P(None, "tp"),
        ),
        out_specs=P(SP_TP, None),
        check_vma=False,
    )
```

```python
import jax
import jax.numpy as jnp
from jax import lax
from jax.experimental import pallas as pl
from jax.experimental.pallas import tpu as pltpu
from jax.sharding import Mesh
from jax.sharding import PartitionSpec as P

D = 2048
HEAD_DIM = 64
STATE = 128
CONV = 4
SP = ("sp_0", "sp_1", "sp_2")
SP_TP = ("sp_0", "sp_1", "sp_2", "tp")


EPSILON = 1e-06


MESH = pl.DeviceIdType.MESH
BF16 = jnp.bfloat16
F32 = jnp.float32
NZ, NY, NC, NX = 8, 4, 2, 4
PLANE = NY * NC
ROWS = 64
HALF = ROWS // 2
CAP = 8
FE = 256


def place():
    return tuple(lax.axis_index(name) for name in SP_TP)


def device(z, y, c, x):
    return {"sp_0": z, "sp_1": y, "sp_2": c, "tp": x}


def remote(src, dst, send_sem, recv_sem, target):
    return pltpu.make_async_remote_copy(
        src_ref=src,
        dst_ref=dst,
        send_sem=send_sem,
        recv_sem=recv_sem,
        device_id=target,
        device_id_type=MESH,
    )


def arrive(ref, sem):
    pltpu.make_async_copy(ref, ref, sem).wait()


def greet(targets):
    barrier = pltpu.get_barrier_semaphore()
    for target in targets:
        pl.semaphore_signal(barrier, inc=1, device_id=target, device_id_type=MESH)
    pl.semaphore_wait(barrier, len(targets))


def moe_kernel(
    rows,
    stream,
    meta,
    rg_hbm,
    ru_hbm,
    rd_hbm,
    cg_hbm,
    cu_hbm,
    cd_hbm,
    out,
    zall,
    metas,
    combine_w,
    send_rows,
    expert_rows,
    expert_out,
    back_rows,
    rs_send,
    rs_recv,
    xall,
    sh_send,
    sh_recv,
    rg,
    ru,
    rd,
    cg,
    cu,
    cd,
    w_sem,
    zs_sem,
    zr_sem,
    ms_sem,
    mr_sem,
    ds_sem,
    dr_sem,
    bs_sem,
    br_sem,
    rss_sem,
    rsr_sem,
    xs_sem,
    xr_sem,
    hs_sem,
    hr_sem,
):
    z, y, c, x = place()
    me = y * NC + c
    z_up, z_down = lax.rem(z + 1, NZ), lax.rem(z + NZ - 1, NZ)
    z_peers = [device(lax.rem(z + d, NZ), y, c, x) for d in range(1, NZ)]
    x_peers = [device(z, y, c, lax.rem(x + d, NX)) for d in range(1, NX)]
    plane_peers = []
    for dy in (1, 3, 2, 0):
        for dc in range(NC):
            if dy or dc:
                yy, cc = lax.rem(y + dy, NY), lax.rem(c + dc, NC)
                plane_peers.append((yy * NC + cc, device(z, yy, cc, x)))

    weights = [
        pltpu.make_async_copy(far, near, w_sem.at[k])
        for k, (far, near) in enumerate(
            ((cg_hbm, cg), (cu_hbm, cu), (cd_hbm, cd), (rg_hbm, rg), (ru_hbm, ru), (rd_hbm, rd))
        )
    ]
    for copy in weights:
        copy.start()
    greet(z_peers + x_peers + [peer for _, peer in plane_peers])

    ring = []

    def hop(step, up, half):
        lo = half * HALF
        here = ((NZ - step) % NZ) if up else step
        there = ((NZ - step - 1) % NZ) if up else step + 1
        source = rows if step == 0 else zall.at[here]
        k = 0 if up else 1
        copy = remote(
            source.at[pl.ds(lo, HALF)],
            zall.at[there, pl.ds(lo, HALF)],
            zs_sem.at[k, step, half],
            zr_sem.at[k, step, half],
            device(z_up if up else z_down, y, c, x),
        )
        copy.start()
        ring.append(copy)

    def ring_arrived(step, up, half):
        lo = half * HALF
        there = ((NZ - step - 1) % NZ) if up else step + 1
        arrive(zall.at[there, pl.ds(lo, HALF)], zr_sem.at[0 if up else 1, step, half])

    meta_copies = [
        remote(meta, metas.at[NZ - d], ms_sem.at[d - 1], mr_sem.at[NZ - d - 1], z_peers[d - 1])
        for d in range(1, NZ)
    ]
    for copy in meta_copies:
        copy.start()
    for half in range(2):
        hop(0, True, half)
        hop(0, False, half)
    x_copies = [
        remote(rows, xall.at[x], xs_sem.at[d - 1], xr_sem.at[NX - d - 1], x_peers[d - 1])
        for d in range(1, NX)
    ]
    for copy in x_copies:
        copy.start()

    token = lax.broadcasted_iota(jnp.int32, (ROWS, ROWS), 0)
    later = lax.broadcasted_iota(jnp.int32, (ROWS, ROWS), 1)
    before = jnp.where(token < later, 1.0, 0.0).astype(BF16)
    expert_row = lax.broadcasted_iota(jnp.int32, (PLANE, ROWS), 0) + z * PLANE
    expert_row = expert_row.astype(F32)
    slot = lax.broadcasted_iota(jnp.int32, (PLANE, CAP, ROWS), 1).astype(F32)
    sends = []

    def dispatch(o):
        table = meta[...] if o == 0 else metas[o]
        hits = jnp.zeros((PLANE, ROWS), F32)
        shares = jnp.zeros((PLANE, ROWS), F32)
        for k in range(4):
            hit = jnp.where(expert_row == table[k : k + 1, :ROWS], 1.0, 0.0)
            hits = hits + hit
            shares = shares + hit * table[4 + k : 5 + k, :ROWS]
        rank = jnp.dot(hits.astype(BF16), before, preferred_element_type=F32)
        chosen = jnp.where(
            (rank[:, None, :] == slot) & (hits[:, None, :] > 0.5),
            jnp.ones((PLANE, CAP, ROWS), F32),
            jnp.zeros((PLANE, CAP, ROWS), F32),
        )
        combine_w[o] = (chosen * shares[:, None, :]).reshape(ROWS, ROWS)
        block = rows[...] if o == 0 else zall[o]
        packed = jnp.dot(
            chosen.reshape(ROWS, ROWS).astype(BF16), block, preferred_element_type=F32
        )
        send_rows[o] = packed.reshape(PLANE, CAP, D).astype(BF16)
        for index, peer in plane_peers:
            copy = remote(
                send_rows.at[o, index], expert_rows.at[o, me], ds_sem.at[o], dr_sem.at[o], peer
            )
            copy.start()
        sends.append((send_rows.at[o], ds_sem.at[o]))
        expert_rows[o, me] = send_rows[o, me]

    def run_expert(blocks):
        for o in blocks:
            arrive(expert_rows.at[o, pl.ds(0, PLANE - 1)], dr_sem.at[o])
        inputs = jnp.concatenate(
            [expert_rows[o].astype(F32).reshape(ROWS, D) for o in blocks], axis=0
        ).astype(BF16)
        gate = jnp.dot(inputs, rg[...], preferred_element_type=F32)
        lifted = jnp.dot(inputs, ru[...], preferred_element_type=F32)
        hidden = (jax.nn.silu(gate) * lifted).astype(BF16)
        result = jnp.dot(hidden, rd[...], preferred_element_type=F32)
        for k, o in enumerate(blocks):
            expert_out[o] = (
                result[k * ROWS : (k + 1) * ROWS].reshape(PLANE, CAP, D).astype(BF16)
            )

    def give_back(o):
        for index, peer in plane_peers:
            copy = remote(
                expert_out.at[o, index], back_rows.at[o, me], bs_sem.at[o], br_sem.at[o], peer
            )
            copy.start()
        sends.append((expert_out.at[o], bs_sem.at[o]))
        back_rows[o, me] = expert_out[o, me]

    def combined(o):
        arrive(back_rows.at[o, pl.ds(0, PLANE - 1)], br_sem.at[o])
        returned = back_rows[o].astype(F32).reshape(ROWS, D).astype(BF16)
        return lax.dot_general(
            combine_w[o].astype(BF16),
            returned,
            (((0,), (0,)), ((), ())),
            preferred_element_type=F32,
        )

    dispatch(0)
    for d in range(1, NZ):
        arrive(metas.at[NZ - d], mr_sem.at[NZ - d - 1])
    for half in range(2):
        for up in (True, False):
            ring_arrived(0, up, half)
            hop(1, up, half)
    dispatch(7)
    dispatch(1)
    for copy in weights:
        copy.wait()
    run_expert((0,))
    for half in range(2):
        for up in (True, False):
            ring_arrived(1, up, half)
            hop(2, up, half)
    dispatch(6)
    dispatch(2)
    run_expert((7, 1))
    ring_arrived(2, True, 0)
    hop(3, True, 0)
    ring_arrived(2, False, 1)
    hop(3, False, 1)
    ring_arrived(2, True, 1)
    ring_arrived(2, False, 0)
    dispatch(5)
    dispatch(3)
    run_expert((6, 2))

    for d in range(1, NX):
        arrive(xall.at[0], xr_sem.at[d - 1])
    xall[x] = rows[...]
    share_copies = []
    hidden_rows = xall[...].reshape(NX * ROWS, D)
    gate = jnp.dot(hidden_rows, cg[...], preferred_element_type=F32)
    lifted = jnp.dot(hidden_rows, cu[...], preferred_element_type=F32)
    hidden = (jax.nn.silu(gate) * lifted).astype(BF16)
    shared = lax.dot_general(
        hidden, cd[...], (((1,), (1,)), ((), ())), preferred_element_type=F32
    )
    sh_send[...] = shared.reshape(NX, ROWS, D).astype(BF16)
    for d in range(1, NX):
        xx = lax.rem(x + d, NX)
        copy = remote(
            sh_send.at[xx],
            sh_recv.at[NX - d - 1],
            hs_sem.at[d - 1],
            hr_sem.at[NX - d - 1],
            x_peers[d - 1],
        )
        copy.start()
        share_copies.append(copy)

    ring_arrived(3, True, 0)
    ring_arrived(3, False, 1)
    dispatch(4)
    run_expert((5, 3))
    run_expert((4,))
    for o in (4, 3, 5, 2, 6, 1, 7, 0):
        give_back(o)

    def pass_on(step, up, half):
        k = 0 if up else 1
        lo = half * HALF
        copy = remote(
            rs_send.at[k, step, pl.ds(lo, HALF)],
            rs_recv.at[k, step, pl.ds(lo, HALF)],
            rss_sem.at[k, step, half],
            rsr_sem.at[k, step, half],
            device(z_up if up else z_down, y, c, x),
        )
        copy.start()
        ring.append(copy)

    def sum_arrived(step, up, half):
        k = 0 if up else 1
        part = rs_recv.at[k, step, pl.ds(half * HALF, HALF)]
        arrive(part, rsr_sem.at[k, step, half])
        return rs_recv[k, step, pl.ds(half * HALF, HALF)].astype(F32)

    first = combined(4).astype(BF16)
    rs_send[0, 0, :HALF] = first[:HALF]
    pass_on(0, True, 0)
    rs_send[1, 0, HALF:] = first[HALF:]
    pass_on(0, False, 1)
    for step in range(1, 4):
        parts = (combined(4 - step), combined(4 + step))
        for turn in range(2):
            for k, up in enumerate((True, False)):
                half = turn if up else 1 - turn
                piece = parts[k][half * HALF : (half + 1) * HALF]
                if step > 1 or turn == 0:
                    piece = piece + sum_arrived(step - 1, up, half)
                rs_send[k, step, pl.ds(half * HALF, HALF)] = piece.astype(BF16)
                pass_on(step, up, half)
    total = combined(0) + stream[...].astype(F32)
    total = total + sh_send[x].astype(F32)
    for d in range(1, NX):
        arrive(sh_recv.at[d - 1], hr_sem.at[d - 1])
        total = total + sh_recv[d - 1].astype(F32)
    for half in range(2):
        piece = total[half * HALF : (half + 1) * HALF]
        for up in (True, False):
            piece = piece + sum_arrived(3, up, half if up else half)
        out[half * HALF : (half + 1) * HALF] = piece.astype(BF16)

    for copy in ring + meta_copies + x_copies + share_copies:
        copy.wait_send()
    for ref, sem in sends:
        arrive(ref.at[pl.ds(0, PLANE - 1)], sem)


def moe(rows, stream, meta, rg, ru, rd, cg, cu, cd):
    vmem = pl.BlockSpec(memory_space=pltpu.VMEM)
    hbm = pl.BlockSpec(memory_space=pl.ANY)
    blocks = (NZ, PLANE, CAP, D)
    dma = pltpu.SemaphoreType.DMA
    return pl.pallas_call(
        moe_kernel,
        out_shape=jax.ShapeDtypeStruct((ROWS, D), BF16),
        in_specs=[vmem] * 3 + [hbm] * 6,
        out_specs=vmem,
        scratch_shapes=[
            pltpu.VMEM((NZ, ROWS, D), BF16),
            pltpu.VMEM((NZ, 8, 128), F32),
            pltpu.VMEM((NZ, ROWS, ROWS), F32),
            pltpu.VMEM(blocks, BF16),
            pltpu.VMEM(blocks, BF16),
            pltpu.VMEM(blocks, BF16),
            pltpu.VMEM(blocks, BF16),
            pltpu.VMEM((2, 4, ROWS, D), BF16),
            pltpu.VMEM((2, 4, ROWS, D), BF16),
            pltpu.VMEM((NX, ROWS, D), BF16),
            pltpu.VMEM((NX, ROWS, D), BF16),
            pltpu.VMEM((NX - 1, ROWS, D), BF16),
            pltpu.VMEM(rg.shape, BF16),
            pltpu.VMEM(ru.shape, BF16),
            pltpu.VMEM(rd.shape, BF16),
            pltpu.VMEM(cg.shape, BF16),
            pltpu.VMEM(cu.shape, BF16),
            pltpu.VMEM(cd.shape, BF16),
            dma((6,)),
            dma((2, 4, 2)),
            dma((2, 4, 2)),
            dma((NZ - 1,)),
            dma((NZ - 1,)),
            dma((NZ,)),
            dma((NZ,)),
            dma((NZ,)),
            dma((NZ,)),
            dma((2, 4, 2)),
            dma((2, 4, 2)),
            dma((NX - 1,)),
            dma((NX - 1,)),
            dma((NX - 1,)),
            dma((NX - 1,)),
        ],
        compiler_params=pltpu.CompilerParams(
            collective_id=1, has_side_effects=True, vmem_limit_bytes=56 * 1024 * 1024
        ),
    )(rows, stream, meta, rg, ru, rd, cg, cu, cd)


LENGTH = 256
HEADS_HERE = 16
GROUPS_HERE = 4
WIDE = 256
PAIRS = 8
RIM = 16
COLS = 512


def split_terms(value, count):
    terms = []
    for _ in range(count):
        term = value.astype(BF16)
        terms.append(term)
        value = value - term.astype(F32)
    return terms


def mixer_kernel(
    residual,
    gate_hbm,
    value_hbm,
    state_hbm,
    read_hbm,
    step_hbm,
    extra_hbm,
    value_taps,
    state_taps,
    read_taps,
    rates,
    direct,
    head_gain,
    w_hbm,
    expert_gain,
    stream_out,
    rows_out,
    gate_in,
    value_in,
    state_raw,
    read_raw,
    step_in,
    extra_in,
    w_out,
    value_rim,
    state_rim,
    read_rim,
    ext,
    values,
    weighted,
    state_in,
    readout,
    mixed,
    heads_out,
    own,
    own_send,
    other,
    chips,
    y_before,
    planes,
    z_before,
    logs,
    plane_logs,
    weights_ref,
    mix_send,
    mix_recv,
    load_sem,
    rim_s,
    rim_r,
    log_s,
    log_r,
    pair_s,
    pair_r,
    chip_s,
    chip_r,
    plog_s,
    plog_r,
    slice_s,
    slice_r,
    yo_s,
    yo_r,
    zb_s,
    zb_r,
    mix_s,
    mix_r,
):
    z, y, c, x = place()
    me = y * NC + c
    partner = device(z, y, 1 - c, x)
    y_peers = [device(z, lax.rem(y + d, NY), c, x) for d in range(1, NY)]
    z_peers = [device(lax.rem(z + d, NZ), y, c, x) for d in range(1, NZ)]
    x_peers = [device(z, y, c, lax.rem(x + d, NX)) for d in range(1, NX)]
    plane_peers = []
    for dy in (1, 3, 2, 0):
        for dc in range(NC):
            if dy or dc:
                away = dy * NC + dc
                back = ((NY - dy) % NY) * NC + dc
                target = device(z, lax.rem(y + dy, NY), lax.rem(c + dc, NC), x)
                plane_peers.append((away - 1, back - 1, target))

    def along(step):
        flat = lax.rem((z * NY + y) * NC + c + step + NZ * NY * NC, NZ * NY * NC)
        return device(flat // (NY * NC), lax.rem(flat // NC, NY), lax.rem(flat, NC), x)

    loads = [
        pltpu.make_async_copy(far, near, load_sem.at[k])
        for k, (far, near) in enumerate(
            (
                (value_hbm, value_in),
                (state_hbm, state_raw),
                (read_hbm, read_raw),
                (step_hbm, step_in),
                (extra_hbm, extra_in),
                (gate_hbm, gate_in),
                (w_hbm, w_out),
            )
        )
    ]
    for load in loads:
        load.start()
    greet(
        [target for _, _, target in plane_peers]
        + z_peers
        + x_peers
        + [along(1), along(-1)]
    )
    started = []

    def send(src, dst, send_sem, recv_sem, target):
        copy = remote(src, dst, send_sem, recv_sem, target)
        copy.start()
        started.append(copy)

    for k in range(3):
        loads[k].wait()
    for k, (near, rim) in enumerate(
        ((value_in, value_rim), (state_raw, state_rim), (read_raw, read_rim))
    ):
        send(near.at[pl.ds(LENGTH - RIM, RIM)], rim, rim_s.at[k], rim_r.at[k], along(1))

    loads[3].wait()
    loads[4].wait()
    sizes = jax.nn.softplus(step_in[...])
    log_decay = sizes * (-jnp.exp(rates[...])) + extra_in[...]
    early = lax.broadcasted_iota(jnp.int32, (LENGTH, LENGTH), 0)
    late = lax.broadcasted_iota(jnp.int32, (LENGTH, LENGTH), 1)
    causal = early >= late
    lower = jnp.where(causal, 1.0, 0.0).astype(BF16)
    upper = jnp.where(early <= late, 1.0, 0.0).astype(BF16)
    cumulative = jnp.zeros((LENGTH, HEADS_HERE), F32)
    by_head = jnp.zeros((HEADS_HERE, LENGTH), F32)
    for term in split_terms(log_decay, 3):
        cumulative = cumulative + jnp.dot(lower, term, preferred_element_type=F32)
        by_head = by_head + lax.dot_general(
            term, upper, (((0,), (0,)), ((), ())), preferred_element_type=F32
        )
    head_row = lax.broadcasted_iota(jnp.int32, (HEADS_HERE, WIDE), 0)
    lane_head = lax.broadcasted_iota(jnp.int32, (HEADS_HERE, WIDE), 1) // HEAD_DIM
    spreads = [
        jnp.where(head_row == lane_head + 4 * g, 1.0, 0.0).astype(BF16) for g in range(GROUPS_HERE)
    ]

    def spread(value, g, count):
        wide = jnp.zeros((value.shape[0], WIDE), F32)
        for term in split_terms(value, count):
            wide = wide + jnp.dot(term, spreads[g], preferred_element_type=F32)
        return wide

    total = cumulative[LENGTH - 1 :, :]
    total_rows = jnp.broadcast_to(total, (8, HEADS_HERE))
    for g in range(GROUPS_HERE):
        wide = spread(total_rows, g, 3)
        for k in range(2):
            logs[me, pl.ds(2 * g + k, 1)] = wide[:1, k * 128 : (k + 1) * 128]
    for away, back, target in plane_peers:
        send(logs.at[me], logs.at[me], log_s.at[away], log_r.at[back], target)

    first = jnp.where(z + y + c == 0, 0.0, 1.0)

    def convolved(near, rim, taps, lo):
        ext[:8] = rim[8:16, lo : lo + WIDE].astype(F32) * first
        ext[8:] = near[:, lo : lo + WIDE].astype(F32)
        weights = taps[:, lo : lo + WIDE].astype(F32)
        sums = ext[5 : 5 + LENGTH] * weights[0:1]
        for k in range(1, CONV):
            sums = sums + ext[5 + k : 5 + k + LENGTH] * weights[k : k + 1]
        return jax.nn.silu(sums)

    arrive(value_rim, rim_r.at[0])
    arrive(state_rim, rim_r.at[1])
    for lo in range(0, GROUPS_HERE * STATE, WIDE):
        state_in[:, lo : lo + WIDE] = convolved(state_raw, state_rim, state_taps, lo).astype(BF16)
    ends = jnp.exp(total - cumulative) * sizes
    for g in range(GROUPS_HERE):
        lo = g * WIDE
        value = convolved(value_in, value_rim, value_taps, lo)
        values[:, lo : lo + WIDE] = value
        weighted[:, lo : lo + WIDE] = (value * spread(sizes, g, 2)).astype(BF16)
        ending = (value * spread(ends, g, 2)).astype(BF16)
        fresh = lax.dot_general(
            state_in[:, g * STATE : (g + 1) * STATE],
            ending,
            (((0,), (0,)), ((), ())),
            preferred_element_type=F32,
        )
        for k in range(2):
            piece = fresh[:, k * 128 : (k + 1) * 128]
            own[2 * g + k] = piece
            own_send[2 * g + k] = piece.astype(BF16)
    theirs, mine = (1 - c) * 4, c * 4
    send(own_send.at[pl.ds(theirs, 4)], other.at[pl.ds(theirs, 4)], pair_s.at[0], pair_r.at[0], partner)
    send(own_send.at[pl.ds(mine, 4)], other.at[pl.ds(mine, 4)], pair_s.at[1], pair_r.at[1], partner)

    for away, back, target in plane_peers:
        arrive(logs.at[0], log_r.at[away])
    chip_logs = [logs[2 * k] + logs[2 * k + 1] for k in range(NY)]
    plane_log = chip_logs[0] + chip_logs[1] + chip_logs[2] + chip_logs[3]
    plane_logs[z] = plane_log
    for d in range(1, NZ):
        send(plane_logs.at[z], plane_logs.at[z], plog_s.at[d - 1], plog_r.at[NZ - d - 1], z_peers[d - 1])
    log_even, log_odd = logs[y * NC], logs[y * NC + 1]
    keep_odd = jnp.exp(log_odd)
    one = jnp.ones((PAIRS, 128), F32)
    weights_ref[0] = jnp.where(c == 0, keep_odd, one)
    weights_ref[1] = jnp.where(c == 0, one, keep_odd)
    for k in range(NY):
        weights_ref[2 + k] = jnp.exp(chip_logs[k])

    arrive(read_rim, rim_r.at[2])
    for lo in range(0, GROUPS_HERE * STATE, WIDE):
        readout[:, lo : lo + WIDE] = convolved(read_raw, read_rim, read_taps, lo).astype(BF16)

    arrive(other.at[pl.ds(0, 4)], pair_r.at[0])
    for j in range(4):
        pair = mine + j
        chips[y, j] = (
            own[pair] * weights_ref[0, pl.ds(pair, 1)]
            + other[pair].astype(F32) * weights_ref[1, pl.ds(pair, 1)]
        ).astype(BF16)
    for d in range(1, NY):
        send(chips.at[y], chips.at[y], chip_s.at[d - 1], chip_r.at[NY - d - 1], y_peers[d - 1])

    def within(g):
        scores = lax.dot_general(
            readout[:, g * STATE : (g + 1) * STATE],
            state_in[:, g * STATE : (g + 1) * STATE],
            (((1,), (1,)), ((), ())),
            preferred_element_type=F32,
        )
        scores = jnp.where(causal, scores, 0.0)
        group_values = weighted[:, g * WIDE : (g + 1) * WIDE]
        lane = lax.broadcasted_iota(jnp.int32, (LENGTH, WIDE), 1) // HEAD_DIM
        result = jnp.zeros((LENGTH, WIDE), F32)
        for r in range(4):
            h = 4 * g + r
            span = cumulative[:, h : h + 1] - by_head[h : h + 1, :]
            decay = jnp.exp(jnp.where(causal, span, -jnp.inf))
            chosen = jnp.where(lane == r, group_values, jnp.zeros_like(group_values))
            result = result + jnp.dot(
                (scores * decay).astype(BF16), chosen, preferred_element_type=F32
            )
        mixed[:, g * WIDE : (g + 1) * WIDE] = result

    within(0)
    within(1)

    for d in range(1, NY):
        arrive(chips.at[0], chip_r.at[d - 1])
    mine_pair = mine + y
    whole = jnp.zeros((STATE, 128), F32)
    for k in range(NY):
        whole = whole * weights_ref[2 + k, pl.ds(mine_pair, 1)] + chips[k, y].astype(F32)
    planes[z] = whole.astype(BF16)
    for d in range(1, NZ):
        send(planes.at[z], planes.at[z], slice_s.at[d - 1], slice_r.at[NZ - d - 1], z_peers[d - 1])
    for j in range(4):
        pair = mine + j
        carried = jnp.zeros((STATE, 128), F32)
        for k in range(NY - 1):
            joined = carried * weights_ref[2 + k, pl.ds(pair, 1)] + chips[k, j].astype(F32)
            carried = jnp.where(k < y, joined, carried)
        y_before[pair] = carried.astype(BF16)
    send(y_before.at[pl.ds(mine, 4)], y_before.at[pl.ds(mine, 4)], yo_s, yo_r, partner)

    within(2)
    within(3)

    for d in range(1, NZ):
        arrive(plane_logs.at[0], plog_r.at[d - 1])
    for k in range(NZ - 1):
        weights_ref[6 + k] = jnp.exp(plane_logs[k])
    for d in range(1, NZ):
        arrive(planes.at[0], slice_r.at[d - 1])
    carried = jnp.zeros((STATE, 128), F32)
    for k in range(NZ - 1):
        joined = carried * weights_ref[6 + k, pl.ds(mine_pair, 1)] + planes[k].astype(F32)
        carried = jnp.where(k < z, joined, carried)
    z_before[mine_pair] = carried.astype(BF16)
    for away, back, target in plane_peers:
        send(
            z_before.at[mine_pair], z_before.at[mine_pair], zb_s.at[away], zb_r.at[back], target
        )

    loads[5].wait()
    direct_rows = jnp.broadcast_to(direct[...], (8, HEADS_HERE))
    for g in range(GROUPS_HERE):
        at = slice(g * WIDE, (g + 1) * WIDE)
        mixed[:, at] = mixed[:, at] + values[:, at] * spread(direct_rows, g, 3)[:1]
        gate = gate_in[:, at].astype(F32)
        values[:, at] = jax.nn.silu(gate)
    from_start = jnp.exp(cumulative)
    since = jnp.zeros((PAIRS, 128), F32)
    for k in range(NY - 1):
        since = since + jnp.where(k < y, chip_logs[k], jnp.zeros_like(since))
    plane_keep = jnp.exp(since)
    core_keep = jnp.exp(log_even)
    lane_a = lax.broadcasted_iota(jnp.int32, (WIDE, WIDE), 0) // HEAD_DIM
    lane_b = lax.broadcasted_iota(jnp.int32, (WIDE, WIDE), 1) // HEAD_DIM
    same_head = jnp.where(lane_a == lane_b, 1.0, 0.0).astype(BF16)

    arrive(y_before.at[pl.ds(0, 4)], yo_r)
    arrive(other.at[pl.ds(0, 4)], pair_r.at[1])
    for away, back, target in plane_peers:
        arrive(z_before.at[0], zb_r.at[away])
    for g in range(GROUPS_HERE):
        at = slice(g * WIDE, (g + 1) * WIDE)
        halves = []
        for k in range(2):
            pair = 2 * g + k
            state = z_before[pair].astype(F32) * plane_keep[pair : pair + 1]
            state = state + y_before[pair].astype(F32)
            joined = state * core_keep[pair : pair + 1] + other[pair].astype(F32)
            halves.append(jnp.where(c == 1, joined, state).astype(BF16))
        carried_out = jnp.dot(
            readout[:, g * STATE : (g + 1) * STATE],
            jnp.concatenate(halves, axis=1),
            preferred_element_type=F32,
        )
        gated = (mixed[:, at] + carried_out * spread(from_start, g, 2)) * values[:, at]
        squares = jnp.zeros((LENGTH, WIDE), F32)
        for term in split_terms(gated * gated, 2):
            squares = squares + jnp.dot(term, same_head, preferred_element_type=F32)
        normed = gated * lax.rsqrt(squares * (1.0 / HEAD_DIM) + EPSILON) * head_gain[:, at]
        heads_out[:, at] = normed.astype(BF16)

    loads[6].wait()
    for n in range(D // COLS):
        partial = jnp.dot(
            heads_out[...], w_out[:, n * COLS : (n + 1) * COLS], preferred_element_type=F32
        )
        mix_send[n] = partial.astype(BF16)
        for d in range(1, NX):
            xx = lax.rem(x + d, NX)
            send(
                mix_send.at[n, pl.ds(pl.multiple_of(xx * ROWS, ROWS), ROWS)],
                mix_recv.at[NX - d - 1, n],
                mix_s.at[d - 1, n],
                mix_r.at[NX - d - 1, n],
                x_peers[d - 1],
            )
    squares = jnp.zeros((ROWS, 1), F32)
    for n in range(D // COLS):
        at = slice(n * COLS, (n + 1) * COLS)
        summed = mix_send[n, pl.ds(pl.multiple_of(x * ROWS, ROWS), ROWS)].astype(F32)
        for d in range(1, NX):
            arrive(mix_recv.at[d - 1, n], mix_r.at[d - 1, n])
            summed = summed + mix_recv[d - 1, n].astype(F32)
        stream = (residual[:, at].astype(F32) + summed).astype(BF16)
        stream_out[:, at] = stream
        wide = stream.astype(F32)
        squares = squares + jnp.sum(wide * wide, axis=-1, keepdims=True)
    scale = lax.rsqrt(squares * (1.0 / D) + EPSILON)
    for n in range(D // COLS):
        at = slice(n * COLS, (n + 1) * COLS)
        rows_out[:, at] = (stream_out[:, at].astype(F32) * scale * expert_gain[:, at]).astype(BF16)
    for copy in started:
        copy.wait_send()


def mixer(
    residual,
    gate,
    value,
    state,
    read,
    step,
    extra,
    value_taps,
    state_taps,
    read_taps,
    rates,
    direct,
    head_gain,
    weight,
    expert_gain,
):
    vmem = pl.BlockSpec(memory_space=pltpu.VMEM)
    hbm = pl.BlockSpec(memory_space=pl.ANY)
    dma = pltpu.SemaphoreType.DMA
    inner = HEADS_HERE * HEAD_DIM
    narrow = GROUPS_HERE * STATE
    pair_block = (PAIRS, STATE, 128)
    return pl.pallas_call(
        mixer_kernel,
        out_shape=[jax.ShapeDtypeStruct((ROWS, D), BF16)] * 2,
        in_specs=[vmem] + [hbm] * 6 + [vmem] * 6 + [hbm, vmem],
        out_specs=[vmem, vmem],
        scratch_shapes=[
            pltpu.VMEM((LENGTH, inner), BF16),
            pltpu.VMEM((LENGTH, inner), BF16),
            pltpu.VMEM((LENGTH, narrow), BF16),
            pltpu.VMEM((LENGTH, narrow), BF16),
            pltpu.VMEM((LENGTH, HEADS_HERE), F32),
            pltpu.VMEM((LENGTH, HEADS_HERE), F32),
            pltpu.VMEM((inner, D), BF16),
            pltpu.VMEM((RIM, inner), BF16),
            pltpu.VMEM((RIM, narrow), BF16),
            pltpu.VMEM((RIM, narrow), BF16),
            pltpu.VMEM((LENGTH + 8, WIDE), F32),
            pltpu.VMEM((LENGTH, inner), F32),
            pltpu.VMEM((LENGTH, inner), BF16),
            pltpu.VMEM((LENGTH, narrow), BF16),
            pltpu.VMEM((LENGTH, narrow), BF16),
            pltpu.VMEM((LENGTH, inner), F32),
            pltpu.VMEM((LENGTH, inner), BF16),
            pltpu.VMEM(pair_block, F32),
            pltpu.VMEM(pair_block, BF16),
            pltpu.VMEM(pair_block, BF16),
            pltpu.VMEM((NY, 4, STATE, 128), BF16),
            pltpu.VMEM(pair_block, BF16),
            pltpu.VMEM((NZ, STATE, 128), BF16),
            pltpu.VMEM(pair_block, BF16),
            pltpu.VMEM((PLANE, PAIRS, 128), F32),
            pltpu.VMEM((NZ, PAIRS, 128), F32),
            pltpu.VMEM((13, PAIRS, 128), F32),
            pltpu.VMEM((D // COLS, LENGTH, COLS), BF16),
            pltpu.VMEM((NX - 1, D // COLS, ROWS, COLS), BF16),
            dma((7,)),
            dma((3,)),
            dma((3,)),
            dma((PLANE - 1,)),
            dma((PLANE - 1,)),
            dma((2,)),
            dma((2,)),
            dma((NY - 1,)),
            dma((NY - 1,)),
            dma((NZ - 1,)),
            dma((NZ - 1,)),
            dma((NZ - 1,)),
            dma((NZ - 1,)),
            dma,
            dma,
            dma((PLANE - 1,)),
            dma((PLANE - 1,)),
            dma((NX - 1, D // COLS)),
            dma((NX - 1, D // COLS)),
        ],
        compiler_params=pltpu.CompilerParams(
            collective_id=2, has_side_effects=True, vmem_limit_bytes=56 * 1024 * 1024
        ),
    )(
        residual,
        gate,
        value,
        state,
        read,
        step,
        extra,
        value_taps,
        state_taps,
        read_taps,
        rates,
        direct,
        head_gain,
        weight,
        expert_gain,
    )


def shards(
    residual,
    output_gate_projected,
    value_projected_input,
    state_projected_input,
    readout_projected_input,
    step_preactivation,
    position_decay_extra,
    value_conv_kernel,
    state_conv_kernel,
    readout_conv_kernel,
    head_log_decay_rates,
    head_direct_weight,
    head_norm_gain,
    mixer_output_weight,
    expert_norm_gain,
    routed_expert_index,
    routed_expert_weight,
    routed_gate_weight,
    routed_up_weight,
    routed_down_weight,
    common_gate_weight,
    common_up_weight,
    common_down_weight,
):
    row_count = residual.shape[0]
    stream, normed_rows = mixer(
        residual,
        output_gate_projected,
        value_projected_input,
        state_projected_input,
        readout_projected_input,
        step_preactivation,
        position_decay_extra,
        value_conv_kernel,
        state_conv_kernel,
        readout_conv_kernel,
        head_log_decay_rates[None, :],
        head_direct_weight[None, :],
        head_norm_gain[None, :],
        mixer_output_weight,
        expert_norm_gain[None, :],
    )
    meta = jnp.concatenate(
        [routed_expert_index.T.astype(F32), routed_expert_weight.T.astype(F32)], axis=0
    )
    meta = jnp.pad(meta, ((0, 0), (0, 128 - row_count)))
    return moe(
        normed_rows,
        stream,
        meta,
        routed_gate_weight[0],
        routed_up_weight[0],
        routed_down_weight[0],
        common_gate_weight,
        common_up_weight,
        common_down_weight,
    )


def solution(mesh):
    torus = Mesh(mesh.devices.reshape(8, 4, 2, mesh.shape["tp"]), ("sp_0", "sp_1", "sp_2", "tp"))
    return jax.shard_map(
        shards,
        mesh=torus,
        in_specs=(
            P(SP_TP, None),
            P(SP, "tp"),
            P(SP, "tp"),
            P(SP, "tp"),
            P(SP, "tp"),
            P(SP, "tp"),
            P(SP, "tp"),
            P(None, "tp"),
            P(None, "tp"),
            P(None, "tp"),
            P("tp"),
            P("tp"),
            P("tp"),
            P("tp", None),
            P(),
            P(SP_TP, None),
            P(SP_TP, None),
            P(SP, None, None),
            P(SP, None, None),
            P(SP, None, None),
            P(None, "tp"),
            P(None, "tp"),
            P(None, "tp"),
        ),
        out_specs=P(SP_TP, None),
        check_vma=False,
    )
```

```python
import jax
import jax.numpy as jnp
from jax import lax
from jax.experimental import pallas as pl
from jax.experimental.pallas import tpu as pltpu
from jax.sharding import Mesh
from jax.sharding import PartitionSpec as P

D = 2048
HEAD_DIM = 64
STATE = 128
CONV = 4
SP = ("sp_0", "sp_1", "sp_2")
SP_TP = ("sp_0", "sp_1", "sp_2", "tp")
EPSILON = 1e-06
MESH = pl.DeviceIdType.MESH
BF16 = jnp.bfloat16
F32 = jnp.float32
NZ, NY, NC, NX = 8, 4, 2, 4
PLANE = NY * NC
ROWS = 64
HALF = ROWS // 2
CAP = 8
FE = 256
TOPK = 4
LENGTH = 256
HEADS_HERE = 16
GROUPS_HERE = 4
INNER = HEADS_HERE * HEAD_DIM
NARROW = GROUPS_HERE * STATE
WIDE = 256
PAIRS = 8
RIM = 16
COLS = 512


def device(z, y, c, x):
    return {"sp_0": z, "sp_1": y, "sp_2": c, "tp": x}


def arrive(ref, sem):
    pltpu.make_async_copy(ref, ref, sem).wait()


def split_terms(value, count):
    terms = []
    for _ in range(count):
        term = value.astype(BF16)
        terms.append(term)
        value = value - term.astype(F32)
    return terms


def over(a, b, dims):
    return lax.dot_general(a, b, (dims, ((), ())), preferred_element_type=F32)


def layer_kernel(
    residual,
    gate_hbm,
    value_hbm,
    state_hbm,
    read_hbm,
    step_raw,
    extra_raw,
    value_taps,
    state_taps,
    read_taps,
    rates,
    direct,
    head_gain,
    w_hbm,
    expert_gain,
    index_raw,
    share_raw,
    rg_hbm,
    ru_hbm,
    rd_hbm,
    cg_hbm,
    cu_hbm,
    cd_hbm,
    out,
    gate_in,
    value_in,
    state_raw,
    read_raw,
    w_out,
    value_rim,
    state_rim,
    read_rim,
    ext,
    top,
    values,
    weighted,
    state_in,
    readout,
    mixed,
    heads_out,
    own_send,
    gathered,
    before_me,
    planes,
    incoming_send,
    incoming,
    logs,
    plane_logs,
    factors,
    mix_send,
    mix_recv,
    stream,
    rows,
    meta,
    zall,
    metas,
    combine_w,
    send_rows,
    expert_rows,
    expert_out,
    back_rows,
    rs_send,
    rs_recv,
    xall,
    sh_send,
    sh_recv,
    rg,
    ru,
    rd,
    cg,
    cu,
    cd,
    load_sem,
    rim_s,
    rim_r,
    log_s,
    log_r,
    own_s,
    own_r,
    plog_s,
    plog_r,
    slice_s,
    slice_r,
    in_s,
    in_r,
    mix_s,
    mix_r,
    zs_sem,
    zr_sem,
    ms_sem,
    mr_sem,
    ds_sem,
    dr_sem,
    bs_sem,
    br_sem,
    rss_sem,
    rsr_sem,
    xs_sem,
    xr_sem,
    hs_sem,
    hr_sem,
):
    z, y, c, x = tuple(lax.axis_index(name) for name in SP_TP)
    me = y * NC + c
    turn = 1 - 2 * c

    def z_at(steps):
        return lax.rem(z + turn * steps + NZ, NZ)

    x_peers = [device(z, y, c, lax.rem(x + d, NX)) for d in range(1, NX)]
    z_peers = [device(z_at(d), y, c, x) for d in range(1, NZ)]
    plane_peers = []
    for dy in (1, 3, 2, 0):
        for dc in range(NC):
            if dy or dc:
                yy, cc = lax.rem(y + dy, NY), lax.rem(c + dc, NC)
                back = ((NY - dy) % NY) * NC + dc
                plane_peers.append((dy * NC + dc - 1, back - 1, yy * NC + cc, device(z, yy, cc, x)))

    def along(step):
        count = NZ * NY * NC
        flat = lax.rem((z * NY + y) * NC + c + step + count, count)
        return device(flat // (NY * NC), lax.rem(flat // NC, NY), lax.rem(flat, NC), x)

    loads = [
        pltpu.make_async_copy(far, near, load_sem.at[k])
        for k, (far, near) in enumerate(
            (
                (value_hbm, value_in),
                (state_hbm, state_raw),
                (read_hbm, read_raw),
                (gate_hbm, gate_in),
                (w_hbm, w_out),
                (rg_hbm, rg),
                (ru_hbm, ru),
                (rd_hbm, rd),
                (cg_hbm, cg),
                (cu_hbm, cu),
                (cd_hbm, cd),
            )
        )
    ]
    for load in loads:
        load.start()
    greeted = x_peers + z_peers + [peer[3] for peer in plane_peers] + [along(1), along(-1)]
    barrier = pltpu.get_barrier_semaphore()
    for target in greeted:
        pl.semaphore_signal(barrier, inc=1, device_id=target, device_id_type=MESH)
    started = []

    def send(src, dst, send_sem, recv_sem, target):
        copy = pltpu.make_async_remote_copy(
            src_ref=src,
            dst_ref=dst,
            send_sem=send_sem,
            recv_sem=recv_sem,
            device_id=target,
            device_id_type=MESH,
        )
        copy.start()
        started.append(copy)

    meta[...] = jnp.zeros((8, 128), F32)
    meta[:TOPK, :ROWS] = index_raw[...].astype(F32)
    meta[TOPK:, :ROWS] = share_raw[...]
    sizes = jax.nn.softplus(step_raw[...])
    head_a = lax.broadcasted_iota(jnp.int32, (HEADS_HERE, HEADS_HERE), 0)
    head_b = lax.broadcasted_iota(jnp.int32, (HEADS_HERE, HEADS_HERE), 1)

    def as_column(row):
        square = jnp.broadcast_to(row, (HEADS_HERE, HEADS_HERE))
        return jnp.sum(jnp.where(head_a == head_b, square, 0.0), axis=1, keepdims=True)

    log_decay = sizes * as_column(-jnp.exp(rates[...])) + extra_raw[...]
    early = lax.broadcasted_iota(jnp.int32, (LENGTH, LENGTH), 0)
    late = lax.broadcasted_iota(jnp.int32, (LENGTH, LENGTH), 1)
    causal = early >= late
    lower = jnp.where(causal, 1.0, 0.0).astype(BF16)
    cumulative = jnp.zeros((LENGTH, HEADS_HERE), F32)
    by_head = jnp.zeros((HEADS_HERE, LENGTH), F32)
    for term in split_terms(log_decay, 3):
        cumulative = cumulative + over(lower, term, ((1,), (1,)))
        by_head = by_head + over(term, lower, ((1,), (1,)))
    head_row = lax.broadcasted_iota(jnp.int32, (HEADS_HERE, WIDE), 0)
    lane_head = lax.broadcasted_iota(jnp.int32, (HEADS_HERE, WIDE), 1) // HEAD_DIM
    spreads = [
        jnp.where(head_row == lane_head + 4 * g, 1.0, 0.0).astype(BF16) for g in range(GROUPS_HERE)
    ]

    def spread(value, g, count):
        wide = jnp.zeros((value.shape[1], WIDE), F32)
        for term in split_terms(value, count):
            wide = wide + over(term, spreads[g], ((0,), (0,)))
        return wide

    total = by_head[:, LENGTH - 1 :]
    total_wide = jnp.broadcast_to(total, (HEADS_HERE, 128))
    for g in range(GROUPS_HERE):
        wide = spread(total_wide, g, 3)
        for k in range(2):
            logs[me, pl.ds(2 * g + k, 1)] = wide[:1, k * 128 : (k + 1) * 128]

    for k in range(3):
        loads[k].wait()
    pl.semaphore_wait(barrier, len(greeted))
    convs = (
        (value_in, value_rim, value_taps),
        (state_raw, state_rim, state_taps),
        (read_raw, read_rim, read_taps),
    )
    for k, (near, rim, _) in enumerate(convs):
        send(near.at[pl.ds(LENGTH - RIM, RIM)], rim, rim_s.at[k], rim_r.at[k], along(1))
    for away, back, _, target in plane_peers:
        send(logs.at[me], logs.at[me], log_s.at[away], log_r.at[back], target)
    for d in range(1, NZ):
        send(meta, metas.at[NZ - d], ms_sem.at[d - 1], mr_sem.at[NZ - d - 1], z_peers[d - 1])

    def late_rows(which, lo):
        near, _, taps = convs[which]
        ext[...] = near[:, lo : lo + WIDE].astype(F32)
        weights = taps[:, lo : lo + WIDE].astype(F32)
        sums = ext[RIM - 3 : LENGTH - 3] * weights[0:1]
        for k in range(1, CONV):
            sums = sums + ext[RIM - 3 + k : LENGTH - 3 + k] * weights[k : k + 1]
        return jax.nn.silu(sums)

    first = jnp.where(z + y + c == 0, 0.0, 1.0)

    def early_rows(which, lo):
        near, rim, taps = convs[which]
        top[:8] = rim[:, lo : lo + WIDE].astype(F32)[RIM - 8 :] * first
        top[8:] = near[:RIM, lo : lo + WIDE].astype(F32)
        weights = taps[:, lo : lo + WIDE].astype(F32)
        sums = top[5 : 5 + RIM] * weights[0:1]
        for k in range(1, CONV):
            sums = sums + top[5 + k : 5 + k + RIM] * weights[k : k + 1]
        return jax.nn.silu(sums)

    for lo in range(0, NARROW, WIDE):
        state_in[RIM:, lo : lo + WIDE] = late_rows(1, lo).astype(BF16)
    for lo in range(0, INNER, WIDE):
        values[RIM:, lo : lo + WIDE] = late_rows(0, lo)
    arrive(state_rim, rim_r.at[1])
    for lo in range(0, NARROW, WIDE):
        state_in[:RIM, lo : lo + WIDE] = early_rows(1, lo).astype(BF16)
    arrive(value_rim, rim_r.at[0])
    for lo in range(0, INNER, WIDE):
        values[:RIM, lo : lo + WIDE] = early_rows(0, lo)
    ends = jnp.exp(total - by_head) * sizes
    for g in range(GROUPS_HERE):
        at = slice(g * WIDE, (g + 1) * WIDE)
        ending = (values[:, at] * spread(ends, g, 2)).astype(BF16)
        fresh = over(state_in[:, g * STATE : (g + 1) * STATE], ending, ((0,), (0,)))
        for k in range(2):
            own_send[2 * g + k] = fresh[:, k * 128 : (k + 1) * 128].astype(BF16)
    for away, back, index, target in plane_peers:
        send(own_send.at[index], gathered.at[me], own_s.at[away], own_r.at[back], target)
    gathered[me] = own_send[me]

    for away, _, _, _ in plane_peers:
        arrive(logs.at[0], log_r.at[away])
    reach = jnp.zeros((PAIRS, 128), F32)
    for k in range(PLANE):
        factors[k] = jnp.exp(logs[k])
        factors[PLANE + k] = jnp.exp(reach)
        reach = reach + logs[k]
    plane_logs[z] = reach
    for d in range(1, NZ):
        send(plane_logs.at[z], plane_logs.at[z], plog_s.at[d - 1], plog_r.at[NZ - d - 1], z_peers[d - 1])

    for lo in range(0, NARROW, WIDE):
        readout[RIM:, lo : lo + WIDE] = late_rows(2, lo).astype(BF16)
    arrive(read_rim, rim_r.at[2])
    for lo in range(0, NARROW, WIDE):
        readout[:RIM, lo : lo + WIDE] = early_rows(2, lo).astype(BF16)
    for g in range(GROUPS_HERE):
        at = slice(g * WIDE, (g + 1) * WIDE)
        weighted[:, at] = (values[:, at] * spread(sizes, g, 2)).astype(BF16)

    def within(g):
        scores = over(
            readout[:, g * STATE : (g + 1) * STATE],
            state_in[:, g * STATE : (g + 1) * STATE],
            ((1,), (1,)),
        )
        scores = jnp.where(causal, scores, 0.0)
        group_values = weighted[:, g * WIDE : (g + 1) * WIDE]
        lane = lax.broadcasted_iota(jnp.int32, (LENGTH, WIDE), 1) // HEAD_DIM
        result = jnp.zeros((LENGTH, WIDE), F32)
        for r in range(4):
            h = 4 * g + r
            span = cumulative[:, h : h + 1] - by_head[h : h + 1, :]
            decay = jnp.exp(jnp.where(causal, span, -jnp.inf))
            chosen = jnp.where(lane == r, group_values, jnp.zeros_like(group_values))
            result = result + over((scores * decay).astype(BF16), chosen, ((1,), (0,)))
        mixed[:, g * WIDE : (g + 1) * WIDE] = result

    within(0)

    for away, _, _, _ in plane_peers:
        arrive(gathered.at[0], own_r.at[away])
    carried = jnp.zeros((STATE, 128), F32)
    for k in range(PLANE):
        before_me[k] = carried
        carried = carried * factors[k, pl.ds(me, 1)] + gathered[k].astype(F32)
    planes[z] = carried.astype(BF16)
    for d in range(1, NZ):
        send(planes.at[z], planes.at[z], slice_s.at[d - 1], slice_r.at[NZ - d - 1], z_peers[d - 1])

    within(1)
    within(2)
    within(3)
    loads[3].wait()
    direct_wide = jnp.broadcast_to(as_column(direct[...]), (HEADS_HERE, 128))
    for g in range(GROUPS_HERE):
        at = slice(g * WIDE, (g + 1) * WIDE)
        mixed[:, at] = mixed[:, at] + values[:, at] * spread(direct_wide, g, 3)[:1]
        values[:, at] = jax.nn.silu(gate_in[:, at].astype(F32))
    from_start = jnp.exp(by_head)
    lane_a = lax.broadcasted_iota(jnp.int32, (WIDE, WIDE), 0) // HEAD_DIM
    lane_b = lax.broadcasted_iota(jnp.int32, (WIDE, WIDE), 1) // HEAD_DIM
    same_head = jnp.where(lane_a == lane_b, 1.0, 0.0).astype(BF16)

    for d in range(1, NZ):
        arrive(plane_logs.at[0], plog_r.at[d - 1])
    for k in range(NZ - 1):
        factors[2 * PLANE + k] = jnp.exp(plane_logs[k])
    for d in range(1, NZ):
        arrive(planes.at[0], slice_r.at[d - 1])
    carried = jnp.zeros((STATE, 128), F32)
    for k in range(NZ - 1):
        joined = carried * factors[2 * PLANE + k, pl.ds(me, 1)] + planes[k].astype(F32)
        carried = jnp.where(k < z, joined, carried)
    for k in range(PLANE):
        incoming_send[k] = (carried * factors[PLANE + k, pl.ds(me, 1)] + before_me[k]).astype(BF16)
    for away, back, index, target in plane_peers:
        send(incoming_send.at[index], incoming.at[me], in_s.at[away], in_r.at[back], target)
    incoming[me] = incoming_send[me]
    loads[4].wait()
    for away, _, _, _ in plane_peers:
        arrive(incoming.at[0], in_r.at[away])
    for g in range(GROUPS_HERE):
        at = slice(g * WIDE, (g + 1) * WIDE)
        state = jnp.concatenate([incoming[2 * g], incoming[2 * g + 1]], axis=1)
        carried_out = over(readout[:, g * STATE : (g + 1) * STATE], state, ((1,), (0,)))
        gated = (mixed[:, at] + carried_out * spread(from_start, g, 2)) * values[:, at]
        squares = jnp.zeros((LENGTH, WIDE), F32)
        for term in split_terms(gated * gated, 2):
            squares = squares + over(term, same_head, ((1,), (0,)))
        normed = gated * lax.rsqrt(squares * (1.0 / HEAD_DIM) + EPSILON) * head_gain[:, at]
        heads_out[:, at] = normed.astype(BF16)

    for n in range(D // COLS):
        partial = over(heads_out[...], w_out[:, n * COLS : (n + 1) * COLS], ((1,), (0,)))
        mix_send[n] = partial.astype(BF16)
        for d in range(1, NX):
            xx = lax.rem(x + d, NX)
            send(
                mix_send.at[n, pl.ds(pl.multiple_of(xx * ROWS, ROWS), ROWS)],
                mix_recv.at[NX - d - 1, n],
                mix_s.at[d - 1, n],
                mix_r.at[NX - d - 1, n],
                x_peers[d - 1],
            )
    squares = jnp.zeros((ROWS, 1), F32)
    for n in range(D // COLS):
        at = slice(n * COLS, (n + 1) * COLS)
        summed = mix_send[n, pl.ds(pl.multiple_of(x * ROWS, ROWS), ROWS)].astype(F32)
        for d in range(1, NX):
            arrive(mix_recv.at[d - 1, n], mix_r.at[d - 1, n])
            summed = summed + mix_recv[d - 1, n].astype(F32)
        joined = (residual[:, at].astype(F32) + summed).astype(BF16)
        stream[:, at] = joined
        wide = joined.astype(F32)
        squares = squares + jnp.sum(wide * wide, axis=-1, keepdims=True)
    scale = lax.rsqrt(squares * (1.0 / D) + EPSILON)
    for n in range(D // COLS):
        at = slice(n * COLS, (n + 1) * COLS)
        rows[:, at] = (stream[:, at].astype(F32) * scale * expert_gain[:, at]).astype(BF16)

    def hop(step, up, half):
        lo = half * HALF
        here = ((NZ - step) % NZ) if up else step
        there = ((NZ - step - 1) % NZ) if up else step + 1
        source = rows if step == 0 else zall.at[here]
        k = 0 if up else 1
        send(
            source.at[pl.ds(lo, HALF)],
            zall.at[there, pl.ds(lo, HALF)],
            zs_sem.at[k, step, half],
            zr_sem.at[k, step, half],
            device(z_at(1 if up else -1), y, c, x),
        )

    def ring_arrived(step, up, half):
        lo = half * HALF
        there = ((NZ - step - 1) % NZ) if up else step + 1
        arrive(zall.at[there, pl.ds(lo, HALF)], zr_sem.at[0 if up else 1, step, half])

    for half in range(2):
        for up in (True, False):
            hop(0, up, half)

    token = lax.broadcasted_iota(jnp.int32, (ROWS, ROWS), 0)
    later = lax.broadcasted_iota(jnp.int32, (ROWS, ROWS), 1)
    before = jnp.where(token < later, 1.0, 0.0).astype(BF16)
    expert_row = lax.broadcasted_iota(jnp.int32, (PLANE, ROWS), 0) + z * PLANE
    expert_row = expert_row.astype(F32)
    slot = lax.broadcasted_iota(jnp.int32, (PLANE, CAP, ROWS), 1).astype(F32)
    sends = []

    def dispatch(o):
        table = meta[...] if o == 0 else metas[o]
        hits = jnp.zeros((PLANE, ROWS), F32)
        shares = jnp.zeros((PLANE, ROWS), F32)
        for k in range(TOPK):
            hit = jnp.where(expert_row == table[k : k + 1, :ROWS], 1.0, 0.0)
            hits = hits + hit
            shares = shares + hit * table[TOPK + k : TOPK + k + 1, :ROWS]
        rank = over(hits.astype(BF16), before, ((1,), (0,)))
        chosen = jnp.where(
            (rank[:, None, :] == slot) & (hits[:, None, :] > 0.5),
            jnp.ones((PLANE, CAP, ROWS), F32),
            jnp.zeros((PLANE, CAP, ROWS), F32),
        )
        combine_w[o] = (chosen * shares[:, None, :]).reshape(ROWS, ROWS)
        block = rows[...] if o == 0 else zall[o]
        packed = over(chosen.reshape(ROWS, ROWS).astype(BF16), block, ((1,), (0,)))
        send_rows[o] = packed.reshape(PLANE, CAP, D).astype(BF16)
        for _, _, index, peer in plane_peers:
            copy = pltpu.make_async_remote_copy(
                src_ref=send_rows.at[o, index],
                dst_ref=expert_rows.at[o, me],
                send_sem=ds_sem.at[o],
                recv_sem=dr_sem.at[o],
                device_id=peer,
                device_id_type=MESH,
            )
            copy.start()
        sends.append((send_rows.at[o], ds_sem.at[o]))
        expert_rows[o, me] = send_rows[o, me]

    def run_expert(blocks):
        for o in blocks:
            arrive(expert_rows.at[o, pl.ds(0, PLANE - 1)], dr_sem.at[o])
        inputs = jnp.concatenate(
            [expert_rows[o].astype(F32).reshape(ROWS, D) for o in blocks], axis=0
        ).astype(BF16)
        gate = over(inputs, rg[...], ((1,), (0,)))
        lifted = over(inputs, ru[...], ((1,), (0,)))
        hidden = (jax.nn.silu(gate) * lifted).astype(BF16)
        result = over(hidden, rd[...], ((1,), (0,)))
        for k, o in enumerate(blocks):
            expert_out[o] = (
                result[k * ROWS : (k + 1) * ROWS].reshape(PLANE, CAP, D).astype(BF16)
            )

    def give_back(o):
        for _, _, index, peer in plane_peers:
            copy = pltpu.make_async_remote_copy(
                src_ref=expert_out.at[o, index],
                dst_ref=back_rows.at[o, me],
                send_sem=bs_sem.at[o],
                recv_sem=br_sem.at[o],
                device_id=peer,
                device_id_type=MESH,
            )
            copy.start()
        sends.append((expert_out.at[o], bs_sem.at[o]))
        back_rows[o, me] = expert_out[o, me]

    def combined(o):
        arrive(back_rows.at[o, pl.ds(0, PLANE - 1)], br_sem.at[o])
        returned = back_rows[o].astype(F32).reshape(ROWS, D).astype(BF16)
        return over(combine_w[o].astype(BF16), returned, ((0,), (0,)))

    dispatch(0)
    for d in range(1, NZ):
        arrive(metas.at[NZ - d], mr_sem.at[NZ - d - 1])
    for half in range(2):
        for up in (True, False):
            ring_arrived(0, up, half)
            hop(1, up, half)
    dispatch(7)
    dispatch(1)
    for d in range(1, NX):
        send(rows, xall.at[x], xs_sem.at[d - 1], xr_sem.at[NX - d - 1], x_peers[d - 1])
    for k in range(5, 11):
        loads[k].wait()
    run_expert((0,))
    for half in range(2):
        for up in (True, False):
            ring_arrived(1, up, half)
            hop(2, up, half)
    dispatch(6)
    dispatch(2)
    run_expert((7, 1))
    ring_arrived(2, True, 0)
    hop(3, True, 0)
    ring_arrived(2, False, 1)
    hop(3, False, 1)
    ring_arrived(2, True, 1)
    ring_arrived(2, False, 0)
    dispatch(5)
    dispatch(3)
    run_expert((6, 2))

    for d in range(1, NX):
        arrive(xall.at[0], xr_sem.at[d - 1])
    xall[x] = rows[...]
    hidden_rows = xall[...].reshape(NX * ROWS, D)
    gate = over(hidden_rows, cg[...], ((1,), (0,)))
    lifted = over(hidden_rows, cu[...], ((1,), (0,)))
    hidden = (jax.nn.silu(gate) * lifted).astype(BF16)
    shared = over(hidden, cd[...], ((1,), (1,)))
    sh_send[...] = shared.reshape(NX, ROWS, D).astype(BF16)

    ring_arrived(3, True, 0)
    ring_arrived(3, False, 1)
    dispatch(4)
    for d in range(1, NX):
        send(
            sh_send.at[lax.rem(x + d, NX)],
            sh_recv.at[NX - d - 1],
            hs_sem.at[d - 1],
            hr_sem.at[NX - d - 1],
            x_peers[d - 1],
        )
    run_expert((5, 3))
    run_expert((4,))
    for o in (4, 3, 5, 2, 6, 1, 7, 0):
        give_back(o)

    def pass_on(step, up, half):
        k = 0 if up else 1
        lo = half * HALF
        send(
            rs_send.at[k, step, pl.ds(lo, HALF)],
            rs_recv.at[k, step, pl.ds(lo, HALF)],
            rss_sem.at[k, step, half],
            rsr_sem.at[k, step, half],
            device(z_at(1 if up else -1), y, c, x),
        )

    def sum_arrived(step, up, half):
        k = 0 if up else 1
        arrive(rs_recv.at[k, step, pl.ds(half * HALF, HALF)], rsr_sem.at[k, step, half])
        return rs_recv[k, step, pl.ds(half * HALF, HALF)].astype(F32)

    far = combined(4).astype(BF16)
    rs_send[0, 0, :HALF] = far[:HALF]
    pass_on(0, True, 0)
    rs_send[1, 0, HALF:] = far[HALF:]
    pass_on(0, False, 1)
    for step in range(1, 4):
        for k, up in enumerate((True, False)):
            part = combined(4 - step if up else 4 + step)
            for half in (k, 1 - k):
                piece = part[half * HALF : (half + 1) * HALF]
                if step > 1 or half == k:
                    piece = piece + sum_arrived(step - 1, up, half)
                rs_send[k, step, pl.ds(half * HALF, HALF)] = piece.astype(BF16)
                pass_on(step, up, half)
    total_rows = stream[...].astype(F32) + sh_send[x].astype(F32)
    for d in range(1, NX):
        arrive(sh_recv.at[d - 1], hr_sem.at[d - 1])
        total_rows = total_rows + sh_recv[d - 1].astype(F32)
    total_rows = total_rows + combined(0)
    for half in (1, 0):
        piece = total_rows[half * HALF : (half + 1) * HALF]
        for up in (True, False):
            piece = piece + sum_arrived(3, up, half)
        out[half * HALF : (half + 1) * HALF] = piece.astype(BF16)

    for copy in started:
        copy.wait_send()
    for ref, sem in sends:
        arrive(ref.at[pl.ds(0, PLANE - 1)], sem)


def layer(*arrays):
    vmem = pl.BlockSpec(memory_space=pltpu.VMEM)
    hbm = pl.BlockSpec(memory_space=pl.ANY)
    dma = pltpu.SemaphoreType.DMA
    return pl.pallas_call(
        layer_kernel,
        out_shape=jax.ShapeDtypeStruct((ROWS, D), BF16),
        in_specs=[vmem] + [hbm] * 4 + [vmem] * 8 + [hbm] + [vmem] * 3 + [hbm] * 6,
        out_specs=vmem,
        scratch_shapes=[
            pltpu.VMEM((LENGTH, INNER), BF16),
            pltpu.VMEM((LENGTH, INNER), BF16),
            pltpu.VMEM((LENGTH, NARROW), BF16),
            pltpu.VMEM((LENGTH, NARROW), BF16),
            pltpu.VMEM((INNER, D), BF16),
            pltpu.VMEM((RIM, INNER), BF16),
            pltpu.VMEM((RIM, NARROW), BF16),
            pltpu.VMEM((RIM, NARROW), BF16),
            pltpu.VMEM((LENGTH, WIDE), F32),
            pltpu.VMEM((8 + RIM, WIDE), F32),
            pltpu.VMEM((LENGTH, INNER), F32),
            pltpu.VMEM((LENGTH, INNER), BF16),
            pltpu.VMEM((LENGTH, NARROW), BF16),
            pltpu.VMEM((LENGTH, NARROW), BF16),
            pltpu.VMEM((LENGTH, INNER), F32),
            pltpu.VMEM((LENGTH, INNER), BF16),
            pltpu.VMEM((PAIRS, STATE, 128), BF16),
            pltpu.VMEM((PAIRS, STATE, 128), BF16),
            pltpu.VMEM((PAIRS, STATE, 128), F32),
            pltpu.VMEM((NZ, STATE, 128), BF16),
            pltpu.VMEM((PAIRS, STATE, 128), BF16),
            pltpu.VMEM((PAIRS, STATE, 128), BF16),
            pltpu.VMEM((PLANE, PAIRS, 128), F32),
            pltpu.VMEM((NZ, PAIRS, 128), F32),
            pltpu.VMEM((2 * PLANE + NZ, PAIRS, 128), F32),
            pltpu.VMEM((D // COLS, LENGTH, COLS), BF16),
            pltpu.VMEM((NX - 1, D // COLS, ROWS, COLS), BF16),
            pltpu.VMEM((ROWS, D), BF16),
            pltpu.VMEM((ROWS, D), BF16),
            pltpu.VMEM((8, 128), F32),
            pltpu.VMEM((NZ, ROWS, D), BF16),
            pltpu.VMEM((NZ, 8, 128), F32),
            pltpu.VMEM((NZ, ROWS, ROWS), F32),
            pltpu.VMEM((NZ, PLANE, CAP, D), BF16),
            pltpu.VMEM((NZ, PLANE, CAP, D), BF16),
            pltpu.VMEM((NZ, PLANE, CAP, D), BF16),
            pltpu.VMEM((NZ, PLANE, CAP, D), BF16),
            pltpu.VMEM((2, 4, ROWS, D), BF16),
            pltpu.VMEM((2, 4, ROWS, D), BF16),
            pltpu.VMEM((NX, ROWS, D), BF16),
            pltpu.VMEM((NX, ROWS, D), BF16),
            pltpu.VMEM((NX - 1, ROWS, D), BF16),
            pltpu.VMEM((D, FE), BF16),
            pltpu.VMEM((D, FE), BF16),
            pltpu.VMEM((FE, D), BF16),
            pltpu.VMEM((D, 128), BF16),
            pltpu.VMEM((D, 128), BF16),
            pltpu.VMEM((D, 128), BF16),
            dma((11,)),
            dma((3,)),
            dma((3,)),
            dma((PLANE - 1,)),
            dma((PLANE - 1,)),
            dma((PLANE - 1,)),
            dma((PLANE - 1,)),
            dma((NZ - 1,)),
            dma((NZ - 1,)),
            dma((NZ - 1,)),
            dma((NZ - 1,)),
            dma((PLANE - 1,)),
            dma((PLANE - 1,)),
            dma((NX - 1, D // COLS)),
            dma((NX - 1, D // COLS)),
            dma((2, 4, 2)),
            dma((2, 4, 2)),
            dma((NZ - 1,)),
            dma((NZ - 1,)),
            dma((NZ,)),
            dma((NZ,)),
            dma((NZ,)),
            dma((NZ,)),
            dma((2, 4, 2)),
            dma((2, 4, 2)),
            dma((NX - 1,)),
            dma((NX - 1,)),
            dma((NX - 1,)),
            dma((NX - 1,)),
        ],
        compiler_params=pltpu.CompilerParams(
            collective_id=1, has_side_effects=True, vmem_limit_bytes=60 * 1024 * 1024
        ),
    )(*arrays)


def shards(
    residual,
    output_gate_projected,
    value_projected_input,
    state_projected_input,
    readout_projected_input,
    step_preactivation,
    position_decay_extra,
    value_conv_kernel,
    state_conv_kernel,
    readout_conv_kernel,
    head_log_decay_rates,
    head_direct_weight,
    head_norm_gain,
    mixer_output_weight,
    expert_norm_gain,
    routed_expert_index,
    routed_expert_weight,
    routed_gate_weight,
    routed_up_weight,
    routed_down_weight,
    common_gate_weight,
    common_up_weight,
    common_down_weight,
):
    return layer(
        residual,
        output_gate_projected,
        value_projected_input,
        state_projected_input,
        readout_projected_input,
        step_preactivation.T,
        position_decay_extra.T,
        value_conv_kernel,
        state_conv_kernel,
        readout_conv_kernel,
        head_log_decay_rates[None, :],
        head_direct_weight[None, :],
        head_norm_gain[None, :],
        mixer_output_weight,
        expert_norm_gain[None, :],
        routed_expert_index.T,
        routed_expert_weight.T,
        routed_gate_weight[0],
        routed_up_weight[0],
        routed_down_weight[0],
        common_gate_weight,
        common_up_weight,
        common_down_weight,
    )


def solution(mesh):
    torus = Mesh(mesh.devices.reshape(8, 4, 2, mesh.shape["tp"]), ("sp_0", "sp_1", "sp_2", "tp"))
    return jax.shard_map(
        shards,
        mesh=torus,
        in_specs=(
            P(SP_TP, None),
            P(SP, "tp"),
            P(SP, "tp"),
            P(SP, "tp"),
            P(SP, "tp"),
            P(SP, "tp"),
            P(SP, "tp"),
            P(None, "tp"),
            P(None, "tp"),
            P(None, "tp"),
            P("tp"),
            P("tp"),
            P("tp"),
            P("tp", None),
            P(),
            P(SP_TP, None),
            P(SP_TP, None),
            P(SP, None, None),
            P(SP, None, None),
            P(SP, None, None),
            P(None, "tp"),
            P(None, "tp"),
            P(None, "tp"),
        ),
        out_specs=P(SP_TP, None),
        check_vma=False,
    )
```

```python
import jax
import jax.numpy as jnp
from jax import lax
from jax.experimental import pallas as pl
from jax.experimental.pallas import tpu as pltpu
from jax.sharding import Mesh
from jax.sharding import PartitionSpec as P

D = 2048
HEAD_DIM = 64
STATE = 128
CONV = 4
SP = ("sp_0", "sp_1", "sp_2")
SP_TP = ("sp_0", "sp_1", "sp_2", "tp")
EPSILON = 1e-06
MESH = pl.DeviceIdType.MESH
BF16 = jnp.bfloat16
F32 = jnp.float32
NZ, NY, NC, NX = 8, 4, 2, 4
PLANE = NY * NC
ROWS = 64
HALF = ROWS // 2
CAP = 8
FE = 256
FAR_Z = (4, 3, 5, 2, 6, 1, 7)
FAR_X = (2, 1, 3)
TOPK = 4
LENGTH = 256
HEADS_HERE = 16
GROUPS_HERE = 4
INNER = HEADS_HERE * HEAD_DIM
NARROW = GROUPS_HERE * STATE
WIDE = 256
PAIRS = 8
RIM = 16
COLS = 512
PIECES = D // COLS


def device(z, y, c, x):
    return {"sp_0": z, "sp_1": y, "sp_2": c, "tp": x}


def arrive(ref, sem):
    pltpu.make_async_copy(ref, ref, sem).wait()


def split_terms(value, count):
    terms = []
    for _ in range(count):
        term = value.astype(BF16)
        terms.append(term)
        value = value - term.astype(F32)
    return terms


def over(a, b, dims):
    return lax.dot_general(a, b, (dims, ((), ())), preferred_element_type=F32)


def layer_kernel(
    residual,
    gate_hbm,
    value_hbm,
    state_hbm,
    read_hbm,
    step_raw,
    extra_raw,
    value_taps,
    state_taps,
    read_taps,
    rates,
    direct,
    head_gain,
    w_hbm,
    expert_gain,
    index_raw,
    share_raw,
    rg_hbm,
    ru_hbm,
    rd_hbm,
    cg_hbm,
    cu_hbm,
    cd_hbm,
    out,
    gate_in,
    value_in,
    state_raw,
    read_raw,
    w_out,
    value_rim,
    state_rim,
    read_rim,
    ext,
    top,
    values,
    weighted,
    ending,
    first_sized,
    first_ended,
    state_in,
    readout,
    mixed,
    heads_out,
    own_send,
    gathered,
    before_me,
    planes,
    incoming_send,
    incoming,
    logs,
    plane_logs,
    factors,
    mix_send,
    mix_recv,
    stream,
    rows,
    meta,
    zall,
    scale_send,
    scales,
    slot_send,
    slot_scales,
    chosen_w,
    metas,
    combine_w,
    send_rows,
    expert_rows,
    expert_out,
    back_rows,
    rs_send,
    rs_recv,
    xall,
    sh_send,
    sh_recv,
    rg,
    ru,
    rd,
    cg,
    cu,
    cd,
    load_sem,
    rim_s,
    rim_r,
    log_s,
    log_r,
    own_s,
    own_r,
    plog_s,
    plog_r,
    slice_s,
    slice_r,
    in_s,
    in_r,
    mix_s,
    mix_r,
    zs_sem,
    zr_sem,
    sc_s,
    sc_r,
    sl_s,
    sl_r,
    ms_sem,
    mr_sem,
    ds_sem,
    dr_sem,
    bs_sem,
    br_sem,
    rss_sem,
    rsr_sem,
    xs_sem,
    xr_sem,
    hs_sem,
    hr_sem,
):
    z, y, c, x = tuple(lax.axis_index(name) for name in SP_TP)
    me = y * NC + c
    turn = 1 - 2 * c

    def z_at(steps):
        return lax.rem(z + turn * steps + NZ, NZ)

    x_peers = [device(z, y, c, lax.rem(x + d, NX)) for d in range(1, NX)]
    z_peers = [device(z_at(d), y, c, x) for d in range(1, NZ)]
    plane_peers = []
    for dy in (2, 1, 3, 0):
        for dc in range(NC):
            if dy or dc:
                yy, cc = lax.rem(y + dy, NY), lax.rem(c + dc, NC)
                plane_peers.append((yy * NC + cc, device(z, yy, cc, x)))

    def along(step):
        count = NZ * NY * NC
        flat = lax.rem((z * NY + y) * NC + c + step + count, count)
        return device(flat // (NY * NC), lax.rem(flat // NC, NY), lax.rem(flat, NC), x)

    loads = [
        pltpu.make_async_copy(far, near, load_sem.at[k])
        for k, (far, near) in enumerate(
            (
                (value_hbm, value_in),
                (state_hbm, state_raw),
                (read_hbm, read_raw),
                (gate_hbm, gate_in),
                (w_hbm, w_out),
                (rg_hbm, rg),
                (ru_hbm, ru),
                (rd_hbm, rd),
                (cg_hbm, cg),
                (cu_hbm, cu),
                (cd_hbm, cd),
            )
        )
    ]
    for load in loads:
        load.start()
    greeted = x_peers + z_peers + [peer for _, peer in plane_peers] + [along(1), along(-1)]
    barrier = pltpu.get_barrier_semaphore()
    for target in greeted:
        pl.semaphore_signal(barrier, inc=1, device_id=target, device_id_type=MESH)

    def send(src, dst, send_sem, recv_sem, target):
        copy = pltpu.make_async_remote_copy(
            src_ref=src,
            dst_ref=dst,
            send_sem=send_sem,
            recv_sem=recv_sem,
            device_id=target,
            device_id_type=MESH,
        )
        copy.start()

    meta[...] = jnp.zeros((8, 128), F32)
    meta[:TOPK, :ROWS] = index_raw[...].astype(F32)
    meta[TOPK:, :ROWS] = share_raw[...]
    sizes = jax.nn.softplus(step_raw[...])
    head_a = lax.broadcasted_iota(jnp.int32, (HEADS_HERE, HEADS_HERE), 0)
    head_b = lax.broadcasted_iota(jnp.int32, (HEADS_HERE, HEADS_HERE), 1)

    def as_column(row):
        square = jnp.broadcast_to(row, (HEADS_HERE, HEADS_HERE))
        return jnp.sum(jnp.where(head_a == head_b, square, 0.0), axis=1, keepdims=True)

    log_decay = sizes * as_column(-jnp.exp(rates[...])) + extra_raw[...]
    early = lax.broadcasted_iota(jnp.int32, (LENGTH, LENGTH), 0)
    late = lax.broadcasted_iota(jnp.int32, (LENGTH, LENGTH), 1)
    causal = early >= late
    lower = jnp.where(causal, 1.0, 0.0).astype(BF16)
    cumulative = jnp.zeros((LENGTH, HEADS_HERE), F32)
    by_head = jnp.zeros((HEADS_HERE, LENGTH), F32)
    for term in split_terms(log_decay, 3):
        cumulative = cumulative + over(lower, term, ((1,), (1,)))
        by_head = by_head + over(term, lower, ((1,), (1,)))
    head_row = lax.broadcasted_iota(jnp.int32, (HEADS_HERE, WIDE), 0)
    lane_head = lax.broadcasted_iota(jnp.int32, (HEADS_HERE, WIDE), 1) // HEAD_DIM
    spreads = [
        jnp.where(head_row == lane_head + 4 * g, 1.0, 0.0).astype(BF16) for g in range(GROUPS_HERE)
    ]

    def spread(value, g, count):
        wide = jnp.zeros((value.shape[1], WIDE), F32)
        for term in split_terms(value, count):
            wide = wide + over(term, spreads[g], ((0,), (0,)))
        return wide

    total = by_head[:, LENGTH - 1 :]
    total_wide = jnp.broadcast_to(total, (HEADS_HERE, 128))
    for g in range(GROUPS_HERE):
        wide = spread(total_wide, g, 3)
        for k in range(2):
            logs[me, pl.ds(2 * g + k, 1)] = wide[:1, k * 128 : (k + 1) * 128]

    for k in range(3):
        loads[k].wait()
    pl.semaphore_wait(barrier, len(greeted))
    convs = (
        (value_in, value_rim, value_taps),
        (state_raw, state_rim, state_taps),
        (read_raw, read_rim, read_taps),
    )
    for k, (near, rim, _) in enumerate(convs):
        send(near.at[pl.ds(LENGTH - RIM, RIM)], rim, rim_s.at[k], rim_r.at[k], along(1))
    for _, target in plane_peers:
        send(logs.at[me], logs.at[me], log_s, log_r, target)
    for d in FAR_Z:
        send(meta, metas.at[NZ - d], ms_sem, mr_sem, z_peers[d - 1])

    def late_rows(which, lo):
        near, _, taps = convs[which]
        ext[...] = near[:, lo : lo + WIDE].astype(F32)
        weights = taps[:, lo : lo + WIDE].astype(F32)
        sums = ext[RIM - 3 : LENGTH - 3] * weights[0:1]
        for k in range(1, CONV):
            sums = sums + ext[RIM - 3 + k : LENGTH - 3 + k] * weights[k : k + 1]
        return jax.nn.silu(sums)

    first = jnp.where(z + y + c == 0, 0.0, 1.0)

    def early_rows(which, lo):
        near, rim, taps = convs[which]
        top[:8] = rim[:, lo : lo + WIDE].astype(F32)[RIM - 8 :] * first
        top[8:] = near[:RIM, lo : lo + WIDE].astype(F32)
        weights = taps[:, lo : lo + WIDE].astype(F32)
        sums = top[5 : 5 + RIM] * weights[0:1]
        for k in range(1, CONV):
            sums = sums + top[5 + k : 5 + k + RIM] * weights[k : k + 1]
        return jax.nn.silu(sums)

    ends = jnp.exp(total - by_head) * sizes
    for lo in range(0, NARROW, WIDE):
        state_in[RIM:, lo : lo + WIDE] = late_rows(1, lo).astype(BF16)
    for g in range(GROUPS_HERE):
        at = slice(g * WIDE, (g + 1) * WIDE)
        value = late_rows(0, g * WIDE)
        values[RIM:, at] = value
        sized = spread(sizes, g, 2)
        ended = spread(ends, g, 2)
        weighted[RIM:, at] = (value * sized[RIM:]).astype(BF16)
        ending[RIM:, at] = (value * ended[RIM:]).astype(BF16)
        first_sized[:, at] = sized[:RIM]
        first_ended[:, at] = ended[:RIM]
    for lo in range(0, NARROW, WIDE):
        readout[RIM:, lo : lo + WIDE] = late_rows(2, lo).astype(BF16)
    arrive(state_rim, rim_r.at[1])
    for lo in range(0, NARROW, WIDE):
        state_in[:RIM, lo : lo + WIDE] = early_rows(1, lo).astype(BF16)
    arrive(value_rim, rim_r.at[0])
    for g in range(GROUPS_HERE):
        at = slice(g * WIDE, (g + 1) * WIDE)
        value = early_rows(0, g * WIDE)
        values[:RIM, at] = value
        ending[:RIM, at] = (value * first_ended[:, at]).astype(BF16)
        fresh = over(state_in[:, g * STATE : (g + 1) * STATE], ending[:, at], ((0,), (0,)))
        for k in range(2):
            own_send[2 * g + k] = fresh[:, k * 128 : (k + 1) * 128].astype(BF16)
    for index, target in plane_peers:
        send(own_send.at[index], gathered.at[me], own_s, own_r, target)
    gathered[me] = own_send[me]

    arrive(logs.at[pl.ds(0, PLANE - 1)], log_r)
    reach = jnp.zeros((PAIRS, 128), F32)
    for k in range(PLANE):
        factors[k] = jnp.exp(logs[k])
        factors[PLANE + k] = jnp.exp(reach)
        reach = reach + logs[k]
    plane_logs[z] = reach
    for d in FAR_Z:
        send(plane_logs.at[z], plane_logs.at[z], plog_s, plog_r, z_peers[d - 1])

    arrive(read_rim, rim_r.at[2])
    for lo in range(0, NARROW, WIDE):
        readout[:RIM, lo : lo + WIDE] = early_rows(2, lo).astype(BF16)
    weighted[:RIM] = (values[:RIM] * first_sized[...]).astype(BF16)

    def within(g):
        scores = over(
            readout[:, g * STATE : (g + 1) * STATE],
            state_in[:, g * STATE : (g + 1) * STATE],
            ((1,), (1,)),
        )
        scores = jnp.where(causal, scores, 0.0)
        group_values = weighted[:, g * WIDE : (g + 1) * WIDE]
        lane = lax.broadcasted_iota(jnp.int32, (LENGTH, WIDE), 1) // HEAD_DIM
        result = jnp.zeros((LENGTH, WIDE), F32)
        for r in range(4):
            h = 4 * g + r
            span = cumulative[:, h : h + 1] - by_head[h : h + 1, :]
            decay = jnp.exp(jnp.where(causal, span, -jnp.inf))
            chosen = jnp.where(lane == r, group_values, jnp.zeros_like(group_values))
            result = result + over((scores * decay).astype(BF16), chosen, ((1,), (0,)))
        mixed[:, g * WIDE : (g + 1) * WIDE] = result

    within(0)

    arrive(gathered.at[pl.ds(0, PLANE - 1)], own_r)
    carried = jnp.zeros((STATE, 128), F32)
    for k in range(PLANE):
        before_me[k] = carried
        carried = carried * factors[k, pl.ds(me, 1)] + gathered[k].astype(F32)
    planes[z] = carried.astype(BF16)
    for d in FAR_Z:
        send(planes.at[z], planes.at[z], slice_s, slice_r, z_peers[d - 1])

    within(1)
    within(2)
    within(3)
    loads[3].wait()
    from_start = jnp.exp(by_head)
    direct_wide = jnp.broadcast_to(as_column(direct[...]), (HEADS_HERE, 128))
    for g in range(GROUPS_HERE):
        at = slice(g * WIDE, (g + 1) * WIDE)
        gate = jax.nn.silu(gate_in[:, at].astype(F32))
        mixed[:, at] = (mixed[:, at] + values[:, at] * spread(direct_wide, g, 3)[:1]) * gate
        values[:, at] = spread(from_start, g, 2) * gate
    lane_a = lax.broadcasted_iota(jnp.int32, (WIDE, WIDE), 0) // HEAD_DIM
    lane_b = lax.broadcasted_iota(jnp.int32, (WIDE, WIDE), 1) // HEAD_DIM
    same_head = jnp.where(lane_a == lane_b, 1.0, 0.0).astype(BF16)

    token = lax.broadcasted_iota(jnp.int32, (ROWS, ROWS), 0)
    later = lax.broadcasted_iota(jnp.int32, (ROWS, ROWS), 1)
    before = jnp.where(token < later, 1.0, 0.0).astype(BF16)
    expert_row = lax.broadcasted_iota(jnp.int32, (PLANE, ROWS), 0) + z * PLANE
    expert_row = expert_row.astype(F32)
    slot = lax.broadcasted_iota(jnp.int32, (PLANE, CAP, ROWS), 1).astype(F32)
    arrive(metas.at[pl.ds(0, NZ - 1)], mr_sem)
    for o in range(NZ):
        table = meta[...] if o == 0 else metas[o]
        hits = jnp.zeros((PLANE, ROWS), F32)
        shares = jnp.zeros((PLANE, ROWS), F32)
        for k in range(TOPK):
            hit = jnp.where(expert_row == table[k : k + 1, :ROWS], 1.0, 0.0)
            hits = hits + hit
            shares = shares + hit * table[TOPK + k : TOPK + k + 1, :ROWS]
        rank = over(hits.astype(BF16), before, ((1,), (0,)))
        chosen = jnp.where(
            (rank[:, None, :] == slot) & (hits[:, None, :] > 0.5),
            jnp.ones((PLANE, CAP, ROWS), F32),
            jnp.zeros((PLANE, CAP, ROWS), F32),
        )
        chosen_w[o] = chosen.reshape(ROWS, ROWS)
        combine_w[o] = (chosen * shares[:, None, :]).reshape(ROWS, ROWS)

    arrive(plane_logs.at[pl.ds(0, NZ - 1)], plog_r)
    for k in range(NZ - 1):
        factors[2 * PLANE + k] = jnp.exp(plane_logs[k])
    arrive(planes.at[pl.ds(0, NZ - 1)], slice_r)
    carried = jnp.zeros((STATE, 128), F32)
    for k in range(NZ - 1):
        joined = carried * factors[2 * PLANE + k, pl.ds(me, 1)] + planes[k].astype(F32)
        carried = jnp.where(k < z, joined, carried)
    for k in range(PLANE):
        incoming_send[k] = (carried * factors[PLANE + k, pl.ds(me, 1)] + before_me[k]).astype(BF16)
    for index, target in plane_peers:
        send(incoming_send.at[index], incoming.at[me], in_s, in_r, target)
    incoming[me] = incoming_send[me]
    loads[4].wait()
    arrive(incoming.at[pl.ds(0, PLANE - 1)], in_r)
    for g in range(GROUPS_HERE):
        at = slice(g * WIDE, (g + 1) * WIDE)
        state = jnp.concatenate([incoming[2 * g], incoming[2 * g + 1]], axis=1)
        carried_out = over(readout[:, g * STATE : (g + 1) * STATE], state, ((1,), (0,)))
        gated = mixed[:, at] + carried_out * values[:, at]
        squares = jnp.zeros((LENGTH, WIDE), F32)
        for term in split_terms(gated * gated, 2):
            squares = squares + over(term, same_head, ((1,), (0,)))
        normed = gated * lax.rsqrt(squares * (1.0 / HEAD_DIM) + EPSILON) * head_gain[:, at]
        heads_out[:, at] = normed.astype(BF16)

    for n in range(PIECES):
        partial = over(heads_out[...], w_out[:, n * COLS : (n + 1) * COLS], ((1,), (0,)))
        mix_send[n] = partial.astype(BF16)
        for d in FAR_X:
            xx = lax.rem(x + d, NX)
            send(
                mix_send.at[n, pl.ds(pl.multiple_of(xx * ROWS, ROWS), ROWS)],
                mix_recv.at[n, NX - d - 1],
                mix_s,
                mix_r.at[n],
                x_peers[d - 1],
            )
    def hop(step, up, n):
        here = ((NZ - step) % NZ) if up else step
        there = ((NZ - step - 1) % NZ) if up else step + 1
        k = 0 if up else 1
        send(
            stream.at[n] if step == 0 else zall.at[here, n],
            zall.at[there, n],
            zs_sem,
            zr_sem.at[k, step, n],
            device(z_at(1 if up else -1), y, c, x),
        )

    def ring_arrived(step, up, n):
        there = ((NZ - step - 1) % NZ) if up else step + 1
        arrive(zall.at[there, n], zr_sem.at[0 if up else 1, step, n])

    def relay(step, n):
        for up in (True, False):
            if step < 2:
                ring_arrived(step, up, n)
                hop(step + 1, up, n)
            elif step == 2:
                ring_arrived(step, up, n)
                if (n < 2) == up:
                    hop(3, up, n)
            elif (n < 2) == up:
                ring_arrived(3, up, n)

    def dispatch(o, m):
        for n in range(2):
            block = stream[2 * m + n] if o == 0 else zall[o, 2 * m + n]
            packed = over(chosen_w[o].astype(BF16), block, ((1,), (0,)))
            send_rows[o, m, :, :, n * COLS : (n + 1) * COLS] = packed.reshape(
                PLANE, CAP, COLS
            ).astype(BF16)
        for index, peer in plane_peers:
            copy = pltpu.make_async_remote_copy(
                src_ref=send_rows.at[o, m, index],
                dst_ref=expert_rows.at[o, m * PLANE + me],
                send_sem=ds_sem,
                recv_sem=dr_sem.at[o],
                device_id=peer,
                device_id_type=MESH,
            )
            copy.start()
        expert_rows[o, m * PLANE + me] = send_rows[o, m, me]

    def run_expert(blocks):
        halves = []
        for m in range(2):
            parts = []
            gain = expert_gain[:, m * (D // 2) : (m + 1) * (D // 2)]
            for o in blocks:
                if m == 0:
                    arrive(expert_rows.at[o, pl.ds(0, 2 * PLANE - 2)], dr_sem.at[o])
                wide = expert_rows[o, m * PLANE : (m + 1) * PLANE].astype(F32) * slot_scales[:, :, o : o + 1]
                parts.append(wide.reshape(ROWS, D // 2))
            halves.append((jnp.concatenate(parts, axis=0) * gain).astype(BF16))
        gate = over(halves[0], rg[: D // 2], ((1,), (0,))) + over(halves[1], rg[D // 2 :], ((1,), (0,)))
        lifted = over(halves[0], ru[: D // 2], ((1,), (0,))) + over(halves[1], ru[D // 2 :], ((1,), (0,)))
        hidden = (jax.nn.silu(gate) * lifted).astype(BF16)
        for m in range(2):
            result = over(hidden, rd[:, m * (D // 2) : (m + 1) * (D // 2)], ((1,), (0,)))
            for k, o in enumerate(blocks):
                expert_out[o, m] = (
                    result[k * ROWS : (k + 1) * ROWS].reshape(PLANE, CAP, D // 2).astype(BF16)
                )

    def give_back(o, m):
        for index, peer in plane_peers:
            copy = pltpu.make_async_remote_copy(
                src_ref=expert_out.at[o, m, index],
                dst_ref=back_rows.at[o, m, me],
                send_sem=bs_sem,
                recv_sem=br_sem.at[o, m],
                device_id=peer,
                device_id_type=MESH,
            )
            copy.start()
        back_rows[o, m, me] = expert_out[o, m, me]

    def combined(o, m):
        arrive(back_rows.at[o, m, pl.ds(0, PLANE - 1)], br_sem.at[o, m])
        returned = back_rows[o, m].astype(F32).reshape(ROWS, D // 2).astype(BF16)
        return over(combine_w[o].astype(BF16), returned, ((0,), (0,)))

    square_sums = []

    def take_piece(n):
        at = slice(n * COLS, (n + 1) * COLS)
        summed = mix_send[n, pl.ds(pl.multiple_of(x * ROWS, ROWS), ROWS)].astype(F32)
        arrive(mix_recv.at[n], mix_r.at[n])
        for d in range(1, NX):
            summed = summed + mix_recv[n, d - 1].astype(F32)
        joined = (residual[:, at].astype(F32) + summed).astype(BF16)
        stream[n] = joined
        hop(0, True, n)
        hop(0, False, n)
        wide = joined.astype(F32)
        square_sums.append(jnp.sum(wide * wide, axis=-1, keepdims=True))

    take_piece(0)
    take_piece(1)
    dispatch(0, 0)
    relay(0, 0)
    take_piece(2)
    relay(0, 1)
    dispatch(7, 0)
    dispatch(1, 0)
    relay(1, 0)
    take_piece(3)
    squares = square_sums[0] + square_sums[1] + square_sums[2] + square_sums[3]
    scale = lax.rsqrt(squares * (1.0 / D) + EPSILON)
    scale_row = jnp.sum(jnp.where(token == later, scale, 0.0), axis=0, keepdims=True)
    scale_send[...] = jnp.zeros((8, 128), F32)
    scale_send[:1, :ROWS] = scale_row
    for d in FAR_Z:
        send(scale_send, scales.at[NZ - d], sc_s, sc_r, z_peers[d - 1])
    dispatch(0, 1)
    for n in range(PIECES):
        at = slice(n * COLS, (n + 1) * COLS)
        rows[:, at] = (stream[n].astype(F32) * scale * expert_gain[:, at]).astype(BF16)
    for d in FAR_X:
        send(rows, xall.at[x], xs_sem, xr_sem, x_peers[d - 1])
    relay(0, 2)
    relay(1, 1)
    dispatch(6, 0)
    dispatch(2, 0)
    relay(2, 0)
    relay(0, 3)
    dispatch(7, 1)
    dispatch(1, 1)
    lane = lax.broadcasted_iota(jnp.int32, (PLANE, CAP, 128), 2)
    by_slot = jnp.zeros((PLANE, CAP, 128), F32)
    arrive(scales.at[pl.ds(0, NZ - 1)], sc_r)
    for o in range(NZ):
        known = scale_row if o == 0 else scales[o, :1, :ROWS]
        found = jnp.sum(chosen_w[o] * known, axis=1, keepdims=True).reshape(PLANE, CAP, 1)
        by_slot = jnp.where(lane == o, found, by_slot)
    slot_send[...] = by_slot
    for index, target in plane_peers:
        send(slot_send.at[index], slot_scales.at[me], sl_s, sl_r, target)
    slot_scales[me] = slot_send[me]
    relay(1, 2)
    relay(2, 1)
    dispatch(5, 0)
    dispatch(3, 0)
    relay(3, 0)
    relay(1, 3)
    dispatch(6, 1)
    dispatch(2, 1)
    for k in range(5, 11):
        loads[k].wait()
    arrive(slot_scales.at[pl.ds(0, PLANE - 1)], sl_r)
    run_expert((0,))
    relay(2, 2)
    relay(3, 1)
    dispatch(4, 0)
    relay(2, 3)
    dispatch(5, 1)
    dispatch(3, 1)
    run_expert((7, 1))
    relay(3, 2)
    relay(3, 3)
    dispatch(4, 1)
    arrive(xall.at[pl.ds(0, NX - 1)], xr_sem)
    xall[x] = rows[...]
    hidden_rows = xall[...].reshape(NX * ROWS, D)
    gate = over(hidden_rows, cg[...], ((1,), (0,)))
    lifted = over(hidden_rows, cu[...], ((1,), (0,)))
    hidden = (jax.nn.silu(gate) * lifted).astype(BF16)
    shared = over(hidden, cd[...], ((1,), (1,)))
    sh_send[...] = shared.reshape(NX, ROWS, D).astype(BF16)
    for d in FAR_X:
        send(
            sh_send.at[lax.rem(x + d, NX)],
            sh_recv.at[NX - d - 1],
            hs_sem,
            hr_sem,
            x_peers[d - 1],
        )
    run_expert((6, 2))
    run_expert((5, 3))
    run_expert((4,))
    for o in (4, 3, 5, 2, 6, 1, 7, 0):
        for m in range(2):
            give_back(o, m)

    def cell(step, up, m):
        if step == 0:
            return 12 + m
        return (step - 1) * 4 + (0 if up else 2) + m

    def pass_on(step, up, m):
        k = cell(step, up, m)
        send(
            rs_send.at[k],
            rs_recv.at[k],
            rss_sem,
            rsr_sem.at[k],
            device(z_at(1 if up else -1), y, c, x),
        )

    def sum_arrived(step, up, m):
        k = cell(step, up, m)
        arrive(rs_recv.at[k], rsr_sem.at[k])
        return rs_recv[k].astype(F32)

    for m, up in ((0, True), (1, False)):
        rs_send[cell(0, up, m)] = combined(4, m).astype(BF16)
        pass_on(0, up, m)
    for step in range(1, 4):
        for k, up in enumerate((True, False)):
            for m in (k, 1 - k):
                piece = combined(4 - step if up else 4 + step, m)
                if step > 1 or m == k:
                    piece = piece + sum_arrived(step - 1, up, m)
                rs_send[cell(step, up, m)] = piece.astype(BF16)
                pass_on(step, up, m)
    arrive(sh_recv, hr_sem)
    for m in range(2):
        at = slice(m * (D // 2), (m + 1) * (D // 2))
        piece = jnp.concatenate([stream[2 * m], stream[2 * m + 1]], axis=1).astype(F32)
        piece = piece + sh_send[x, :, at].astype(F32)
        for d in range(1, NX):
            piece = piece + sh_recv[d - 1, :, at].astype(F32)
        piece = piece + combined(0, m)
        for up in (True, False):
            piece = piece + sum_arrived(3, up, m)
        out[:, at] = piece.astype(BF16)

    for k, (near, _, _) in enumerate(convs):
        arrive(near.at[pl.ds(0, RIM)], rim_s.at[k])
    for ref, sem in (
        (logs.at[pl.ds(0, PLANE - 1)], log_s),
        (metas.at[pl.ds(0, NZ - 1)], ms_sem),
        (own_send.at[pl.ds(0, PLANE - 1)], own_s),
        (plane_logs.at[pl.ds(0, NZ - 1)], plog_s),
        (planes.at[pl.ds(0, NZ - 1)], slice_s),
        (incoming_send.at[pl.ds(0, PLANE - 1)], in_s),
        (mix_recv, mix_s),
        (scales.at[pl.ds(0, NZ - 1)], sc_s),
        (slot_send.at[pl.ds(0, PLANE - 1)], sl_s),
        (xall.at[pl.ds(0, NX - 1)], xs_sem),
        (sh_recv, hs_sem),
        (zall.at[pl.ds(0, NZ - 1)], zs_sem),
        (send_rows.at[pl.ds(0, NZ - 1)], ds_sem),
        (expert_out.at[pl.ds(0, NZ - 1)], bs_sem),
        (rs_send, rss_sem),
    ):
        arrive(ref, sem)


def layer(*arrays):
    vmem = pl.BlockSpec(memory_space=pltpu.VMEM)
    hbm = pl.BlockSpec(memory_space=pl.ANY)
    dma = pltpu.SemaphoreType.DMA
    return pl.pallas_call(
        layer_kernel,
        out_shape=jax.ShapeDtypeStruct((ROWS, D), BF16),
        in_specs=[vmem] + [hbm] * 4 + [vmem] * 8 + [hbm] + [vmem] * 3 + [hbm] * 6,
        out_specs=vmem,
        scratch_shapes=[
            pltpu.VMEM((LENGTH, INNER), BF16),
            pltpu.VMEM((LENGTH, INNER), BF16),
            pltpu.VMEM((LENGTH, NARROW), BF16),
            pltpu.VMEM((LENGTH, NARROW), BF16),
            pltpu.VMEM((INNER, D), BF16),
            pltpu.VMEM((RIM, INNER), BF16),
            pltpu.VMEM((RIM, NARROW), BF16),
            pltpu.VMEM((RIM, NARROW), BF16),
            pltpu.VMEM((LENGTH, WIDE), F32),
            pltpu.VMEM((8 + RIM, WIDE), F32),
            pltpu.VMEM((LENGTH, INNER), F32),
            pltpu.VMEM((LENGTH, INNER), BF16),
            pltpu.VMEM((LENGTH, INNER), BF16),
            pltpu.VMEM((RIM, INNER), F32),
            pltpu.VMEM((RIM, INNER), F32),
            pltpu.VMEM((LENGTH, NARROW), BF16),
            pltpu.VMEM((LENGTH, NARROW), BF16),
            pltpu.VMEM((LENGTH, INNER), F32),
            pltpu.VMEM((LENGTH, INNER), BF16),
            pltpu.VMEM((PAIRS, STATE, 128), BF16),
            pltpu.VMEM((PAIRS, STATE, 128), BF16),
            pltpu.VMEM((PAIRS, STATE, 128), F32),
            pltpu.VMEM((NZ, STATE, 128), BF16),
            pltpu.VMEM((PAIRS, STATE, 128), BF16),
            pltpu.VMEM((PAIRS, STATE, 128), BF16),
            pltpu.VMEM((PLANE, PAIRS, 128), F32),
            pltpu.VMEM((NZ, PAIRS, 128), F32),
            pltpu.VMEM((2 * PLANE + NZ, PAIRS, 128), F32),
            pltpu.VMEM((PIECES, LENGTH, COLS), BF16),
            pltpu.VMEM((PIECES, NX - 1, ROWS, COLS), BF16),
            pltpu.VMEM((PIECES, ROWS, COLS), BF16),
            pltpu.VMEM((ROWS, D), BF16),
            pltpu.VMEM((8, 128), F32),
            pltpu.VMEM((NZ, PIECES, ROWS, COLS), BF16),
            pltpu.VMEM((8, 128), F32),
            pltpu.VMEM((NZ, 8, 128), F32),
            pltpu.VMEM((PLANE, CAP, 128), F32),
            pltpu.VMEM((PLANE, CAP, 128), F32),
            pltpu.VMEM((NZ, ROWS, ROWS), F32),
            pltpu.VMEM((NZ, 8, 128), F32),
            pltpu.VMEM((NZ, ROWS, ROWS), F32),
            pltpu.VMEM((NZ, 2, PLANE, CAP, D // 2), BF16),
            pltpu.VMEM((NZ, 2 * PLANE, CAP, D // 2), BF16),
            pltpu.VMEM((NZ, 2, PLANE, CAP, D // 2), BF16),
            pltpu.VMEM((NZ, 2, PLANE, CAP, D // 2), BF16),
            pltpu.VMEM((14, ROWS, D // 2), BF16),
            pltpu.VMEM((14, ROWS, D // 2), BF16),
            pltpu.VMEM((NX, ROWS, D), BF16),
            pltpu.VMEM((NX, ROWS, D), BF16),
            pltpu.VMEM((NX - 1, ROWS, D), BF16),
            pltpu.VMEM((D, FE), BF16),
            pltpu.VMEM((D, FE), BF16),
            pltpu.VMEM((FE, D), BF16),
            pltpu.VMEM((D, 128), BF16),
            pltpu.VMEM((D, 128), BF16),
            pltpu.VMEM((D, 128), BF16),
            dma((11,)),
            dma((3,)),
            dma((3,)),
            dma,
            dma,
            dma,
            dma,
            dma,
            dma,
            dma,
            dma,
            dma,
            dma,
            dma,
            dma((PIECES,)),
            dma,
            dma((2, 4, PIECES)),
            dma,
            dma,
            dma,
            dma,
            dma,
            dma,
            dma,
            dma((NZ,)),
            dma,
            dma((NZ, 2)),
            dma,
            dma((14,)),
            dma,
            dma,
            dma,
            dma,
        ],
        compiler_params=pltpu.CompilerParams(
            collective_id=1, has_side_effects=True, vmem_limit_bytes=60 * 1024 * 1024
        ),
    )(*arrays)


def shards(
    residual,
    output_gate_projected,
    value_projected_input,
    state_projected_input,
    readout_projected_input,
    step_preactivation,
    position_decay_extra,
    value_conv_kernel,
    state_conv_kernel,
    readout_conv_kernel,
    head_log_decay_rates,
    head_direct_weight,
    head_norm_gain,
    mixer_output_weight,
    expert_norm_gain,
    routed_expert_index,
    routed_expert_weight,
    routed_gate_weight,
    routed_up_weight,
    routed_down_weight,
    common_gate_weight,
    common_up_weight,
    common_down_weight,
):
    return layer(
        residual,
        output_gate_projected,
        value_projected_input,
        state_projected_input,
        readout_projected_input,
        step_preactivation.T,
        position_decay_extra.T,
        value_conv_kernel,
        state_conv_kernel,
        readout_conv_kernel,
        head_log_decay_rates[None, :],
        head_direct_weight[None, :],
        head_norm_gain[None, :],
        mixer_output_weight,
        expert_norm_gain[None, :],
        routed_expert_index.T,
        routed_expert_weight.T,
        routed_gate_weight[0],
        routed_up_weight[0],
        routed_down_weight[0],
        common_gate_weight,
        common_up_weight,
        common_down_weight,
    )


def solution(mesh):
    torus = Mesh(mesh.devices.reshape(8, 4, 2, mesh.shape["tp"]), ("sp_0", "sp_1", "sp_2", "tp"))
    return jax.shard_map(
        shards,
        mesh=torus,
        in_specs=(
            P(SP_TP, None),
            P(SP, "tp"),
            P(SP, "tp"),
            P(SP, "tp"),
            P(SP, "tp"),
            P(SP, "tp"),
            P(SP, "tp"),
            P(None, "tp"),
            P(None, "tp"),
            P(None, "tp"),
            P("tp"),
            P("tp"),
            P("tp"),
            P("tp", None),
            P(),
            P(SP_TP, None),
            P(SP_TP, None),
            P(SP, None, None),
            P(SP, None, None),
            P(SP, None, None),
            P(None, "tp"),
            P(None, "tp"),
            P(None, "tp"),
        ),
        out_specs=P(SP_TP, None),
        check_vma=False,
    )
```

```python
import jax
import jax.numpy as jnp
from jax import lax
from jax.experimental import pallas as pl
from jax.experimental.pallas import tpu as pltpu
from jax.sharding import Mesh
from jax.sharding import PartitionSpec as P

D = 2048
HEAD_DIM = 64
STATE = 128
CONV = 4
SP = ("sp_0", "sp_1", "sp_2")
SP_TP = ("sp_0", "sp_1", "sp_2", "tp")
EPSILON = 1e-06
MESH = pl.DeviceIdType.MESH
BF16 = jnp.bfloat16
F32 = jnp.float32
NZ, NY, NC, NX = 8, 4, 2, 4
PLANE = NY * NC
ROWS = 64
HALF = ROWS // 2
CAP = 8
FE = 256
FAR_Z = (4, 3, 5, 2, 6, 1, 7)
FAR_X = (2, 1, 3)
TOPK = 4
LENGTH = 256
HEADS_HERE = 16
GROUPS_HERE = 4
INNER = HEADS_HERE * HEAD_DIM
NARROW = GROUPS_HERE * STATE
WIDE = 256
PAIRS = 8
RIM = 16
COLS = 512
PIECES = D // COLS


def device(z, y, c, x):
    return {"sp_0": z, "sp_1": y, "sp_2": c, "tp": x}


def arrive(ref, sem):
    pltpu.make_async_copy(ref, ref, sem).wait()


def split_terms(value, count):
    terms = []
    for _ in range(count):
        term = value.astype(BF16)
        terms.append(term)
        value = value - term.astype(F32)
    return terms


def over(a, b, dims):
    return lax.dot_general(a, b, (dims, ((), ())), preferred_element_type=F32)


def layer_kernel(
    residual_hbm,
    gate_hbm,
    value_hbm,
    state_hbm,
    read_hbm,
    step_hbm,
    extra_hbm,
    value_taps_hbm,
    state_taps_hbm,
    read_taps_hbm,
    rates_hbm,
    direct_hbm,
    head_gain_hbm,
    w_hbm,
    expert_gain_hbm,
    index_hbm,
    share_hbm,
    rg_hbm,
    ru_hbm,
    rd_hbm,
    cg_hbm,
    cu_hbm,
    cd_hbm,
    out,
    residual,
    step_raw,
    extra_raw,
    value_taps,
    state_taps,
    read_taps,
    rates,
    direct,
    head_gain,
    expert_gain,
    index_raw,
    share_raw,
    gate_in,
    value_in,
    state_raw,
    read_raw,
    w_out,
    value_rim,
    state_rim,
    read_rim,
    ext,
    top,
    values,
    weighted,
    ending,
    first_sized,
    first_ended,
    state_in,
    readout,
    mixed,
    heads_out,
    own_send,
    gathered,
    before_me,
    planes,
    incoming_send,
    incoming,
    logs,
    plane_logs,
    factors,
    mix_send,
    mix_recv,
    stream,
    rows,
    meta,
    zall,
    scale_send,
    scales,
    slot_send,
    slot_scales,
    chosen_w,
    metas,
    combine_w,
    send_rows,
    expert_rows,
    expert_out,
    back_rows,
    rs_send,
    rs_recv,
    xall,
    sh_send,
    sh_recv,
    rg,
    ru,
    rd,
    cg,
    cu,
    cd,
    load_sem,
    rim_s,
    rim_r,
    log_s,
    log_r,
    own_s,
    own_r,
    plog_s,
    plog_r,
    slice_s,
    slice_r,
    in_s,
    in_r,
    mix_s,
    mix_r,
    zs_sem,
    zr_sem,
    sc_s,
    sc_r,
    sl_s,
    sl_r,
    ms_sem,
    mr_sem,
    ds_sem,
    dr_sem,
    bs_sem,
    br_sem,
    rss_sem,
    rsr_sem,
    xs_sem,
    xr_sem,
    hs_sem,
    hr_sem,
):
    z, y, c, x = tuple(lax.axis_index(name) for name in SP_TP)
    me = y * NC + c
    turn = 1 - 2 * c

    def z_at(steps):
        return lax.rem(z + turn * steps + NZ, NZ)

    x_peers = [device(z, y, c, lax.rem(x + d, NX)) for d in range(1, NX)]
    z_peers = [device(z_at(d), y, c, x) for d in range(1, NZ)]
    plane_peers = []
    for dy in (2, 1, 3, 0):
        for dc in range(NC):
            if dy or dc:
                yy, cc = lax.rem(y + dy, NY), lax.rem(c + dc, NC)
                plane_peers.append((yy * NC + cc, device(z, yy, cc, x)))

    def along(step):
        count = NZ * NY * NC
        flat = lax.rem((z * NY + y) * NC + c + step + count, count)
        return device(flat // (NY * NC), lax.rem(flat // NC, NY), lax.rem(flat, NC), x)

    greeted = x_peers + z_peers + [peer for _, peer in plane_peers] + [along(1), along(-1)]
    barrier = pltpu.get_barrier_semaphore()
    for target in greeted:
        pl.semaphore_signal(barrier, inc=1, device_id=target, device_id_type=MESH)
    loads = {}
    for k, (name, far, near) in enumerate(
        (
            ("step", step_hbm, step_raw),
            ("extra", extra_hbm, extra_raw),
            ("rates", rates_hbm, rates),
            ("value", value_hbm, value_in),
            ("state", state_hbm, state_raw),
            ("read", read_hbm, read_raw),
            ("value_taps", value_taps_hbm, value_taps),
            ("state_taps", state_taps_hbm, state_taps),
            ("read_taps", read_taps_hbm, read_taps),
            ("index", index_hbm, index_raw),
            ("share", share_hbm, share_raw),
            ("direct", direct_hbm, direct),
            ("gate", gate_hbm, gate_in),
            ("head_gain", head_gain_hbm, head_gain),
            ("w", w_hbm, w_out),
            ("residual", residual_hbm, residual),
            ("expert_gain", expert_gain_hbm, expert_gain),
            ("rg", rg_hbm, rg),
            ("ru", ru_hbm, ru),
            ("rd", rd_hbm, rd),
            ("cg", cg_hbm, cg),
            ("cu", cu_hbm, cu),
            ("cd", cd_hbm, cd),
        )
    ):
        loads[name] = pltpu.make_async_copy(far, near, load_sem.at[k])
        loads[name].start()

    def loaded(*wanted):
        for name in wanted:
            loads[name].wait()

    def send(src, dst, send_sem, recv_sem, target):
        copy = pltpu.make_async_remote_copy(
            src_ref=src,
            dst_ref=dst,
            send_sem=send_sem,
            recv_sem=recv_sem,
            device_id=target,
            device_id_type=MESH,
        )
        copy.start()

    loaded("step", "extra", "rates")
    sizes = jax.nn.softplus(step_raw[...])
    head_a = lax.broadcasted_iota(jnp.int32, (HEADS_HERE, HEADS_HERE), 0)
    head_b = lax.broadcasted_iota(jnp.int32, (HEADS_HERE, HEADS_HERE), 1)

    def as_column(row):
        square = jnp.broadcast_to(row, (HEADS_HERE, HEADS_HERE))
        return jnp.sum(jnp.where(head_a == head_b, square, 0.0), axis=1, keepdims=True)

    log_decay = sizes * as_column(-jnp.exp(rates[...])) + extra_raw[...]
    early = lax.broadcasted_iota(jnp.int32, (LENGTH, LENGTH), 0)
    late = lax.broadcasted_iota(jnp.int32, (LENGTH, LENGTH), 1)
    causal = early >= late
    lower = jnp.where(causal, 1.0, 0.0).astype(BF16)
    cumulative = jnp.zeros((LENGTH, HEADS_HERE), F32)
    by_head = jnp.zeros((HEADS_HERE, LENGTH), F32)
    for term in split_terms(log_decay, 3):
        cumulative = cumulative + over(lower, term, ((1,), (1,)))
        by_head = by_head + over(term, lower, ((1,), (1,)))
    head_row = lax.broadcasted_iota(jnp.int32, (HEADS_HERE, WIDE), 0)
    lane_head = lax.broadcasted_iota(jnp.int32, (HEADS_HERE, WIDE), 1) // HEAD_DIM
    spreads = [
        jnp.where(head_row == lane_head + 4 * g, 1.0, 0.0).astype(BF16) for g in range(GROUPS_HERE)
    ]

    def spread(value, g, count):
        wide = jnp.zeros((value.shape[1], WIDE), F32)
        for term in split_terms(value, count):
            wide = wide + over(term, spreads[g], ((0,), (0,)))
        return wide

    total = by_head[:, LENGTH - 1 :]
    total_wide = jnp.broadcast_to(total, (HEADS_HERE, 128))
    for g in range(GROUPS_HERE):
        wide = spread(total_wide, g, 3)
        for k in range(2):
            logs[me, pl.ds(2 * g + k, 1)] = wide[:1, k * 128 : (k + 1) * 128]

    loaded("index", "share")
    meta[...] = jnp.zeros((8, 128), F32)
    meta[:TOPK, :ROWS] = index_raw[...].astype(F32)
    meta[TOPK:, :ROWS] = share_raw[...]
    loaded("value", "state", "read", "value_taps", "state_taps", "read_taps")
    pl.semaphore_wait(barrier, len(greeted))
    convs = (
        (value_in, value_rim, value_taps),
        (state_raw, state_rim, state_taps),
        (read_raw, read_rim, read_taps),
    )
    for k, (near, rim, _) in enumerate(convs):
        send(near.at[pl.ds(LENGTH - RIM, RIM)], rim, rim_s.at[k], rim_r.at[k], along(1))
    for _, target in plane_peers:
        send(logs.at[me], logs.at[me], log_s, log_r, target)
    for d in FAR_Z:
        send(meta, metas.at[NZ - d], ms_sem, mr_sem, z_peers[d - 1])

    def late_rows(which, lo):
        near, _, taps = convs[which]
        ext[...] = near[:, lo : lo + WIDE].astype(F32)
        weights = taps[:, lo : lo + WIDE].astype(F32)
        sums = ext[RIM - 3 : LENGTH - 3] * weights[0:1]
        for k in range(1, CONV):
            sums = sums + ext[RIM - 3 + k : LENGTH - 3 + k] * weights[k : k + 1]
        return jax.nn.silu(sums)

    first = jnp.where(z + y + c == 0, 0.0, 1.0)

    def early_rows(which, lo):
        near, rim, taps = convs[which]
        top[:8] = rim[:, lo : lo + WIDE].astype(F32)[RIM - 8 :] * first
        top[8:] = near[:RIM, lo : lo + WIDE].astype(F32)
        weights = taps[:, lo : lo + WIDE].astype(F32)
        sums = top[5 : 5 + RIM] * weights[0:1]
        for k in range(1, CONV):
            sums = sums + top[5 + k : 5 + k + RIM] * weights[k : k + 1]
        return jax.nn.silu(sums)

    ends = jnp.exp(total - by_head) * sizes
    for lo in range(0, NARROW, WIDE):
        state_in[RIM:, lo : lo + WIDE] = late_rows(1, lo).astype(BF16)
    for g in range(GROUPS_HERE):
        at = slice(g * WIDE, (g + 1) * WIDE)
        value = late_rows(0, g * WIDE)
        values[RIM:, at] = value
        sized = spread(sizes, g, 2)
        ended = spread(ends, g, 2)
        weighted[RIM:, at] = (value * sized[RIM:]).astype(BF16)
        ending[RIM:, at] = (value * ended[RIM:]).astype(BF16)
        first_sized[:, at] = sized[:RIM]
        first_ended[:, at] = ended[:RIM]
    for lo in range(0, NARROW, WIDE):
        readout[RIM:, lo : lo + WIDE] = late_rows(2, lo).astype(BF16)
    arrive(state_rim, rim_r.at[1])
    for lo in range(0, NARROW, WIDE):
        state_in[:RIM, lo : lo + WIDE] = early_rows(1, lo).astype(BF16)
    arrive(value_rim, rim_r.at[0])
    for g in range(GROUPS_HERE):
        at = slice(g * WIDE, (g + 1) * WIDE)
        value = early_rows(0, g * WIDE)
        values[:RIM, at] = value
        ending[:RIM, at] = (value * first_ended[:, at]).astype(BF16)
        fresh = over(state_in[:, g * STATE : (g + 1) * STATE], ending[:, at], ((0,), (0,)))
        for k in range(2):
            own_send[2 * g + k] = fresh[:, k * 128 : (k + 1) * 128].astype(BF16)
    parts = [pl.ds(k * (STATE // 2), STATE // 2) for k in range(2)]
    for k, part in enumerate(parts):
        for index, target in plane_peers:
            send(own_send.at[index, part], gathered.at[me, part], own_s, own_r.at[k], target)
    gathered[me] = own_send[me]

    arrive(logs.at[pl.ds(0, PLANE - 1)], log_r)
    reach = jnp.zeros((PAIRS, 128), F32)
    for k in range(PLANE):
        factors[k] = jnp.exp(logs[k])
        factors[PLANE + k] = jnp.exp(reach)
        reach = reach + logs[k]
    plane_logs[z] = reach
    for d in FAR_Z:
        send(plane_logs.at[z], plane_logs.at[z], plog_s, plog_r, z_peers[d - 1])

    arrive(read_rim, rim_r.at[2])
    for lo in range(0, NARROW, WIDE):
        readout[:RIM, lo : lo + WIDE] = early_rows(2, lo).astype(BF16)
    weighted[:RIM] = (values[:RIM] * first_sized[...]).astype(BF16)

    def within(g):
        scores = over(
            readout[:, g * STATE : (g + 1) * STATE],
            state_in[:, g * STATE : (g + 1) * STATE],
            ((1,), (1,)),
        )
        scores = jnp.where(causal, scores, 0.0)
        group_values = weighted[:, g * WIDE : (g + 1) * WIDE]
        lane = lax.broadcasted_iota(jnp.int32, (LENGTH, WIDE), 1) // HEAD_DIM
        result = jnp.zeros((LENGTH, WIDE), F32)
        for r in range(4):
            h = 4 * g + r
            span = cumulative[:, h : h + 1] - by_head[h : h + 1, :]
            decay = jnp.exp(jnp.where(causal, span, -jnp.inf))
            chosen = jnp.where(lane == r, group_values, jnp.zeros_like(group_values))
            result = result + over((scores * decay).astype(BF16), chosen, ((1,), (0,)))
        mixed[:, g * WIDE : (g + 1) * WIDE] = result

    within(0)

    for h, part in enumerate(parts):
        arrive(gathered.at[pl.ds(0, PLANE - 1), part], own_r.at[h])
        carried = jnp.zeros((STATE // 2, 128), F32)
        for k in range(PLANE):
            before_me[k, part] = carried
            carried = carried * factors[k, pl.ds(me, 1)] + gathered[k, part].astype(F32)
        planes[z, part] = carried.astype(BF16)
        for d in FAR_Z:
            send(planes.at[z, part], planes.at[z, part], slice_s, slice_r.at[h], z_peers[d - 1])

    within(1)
    within(2)
    within(3)
    loaded("direct", "gate")
    from_start = jnp.exp(by_head)
    direct_wide = jnp.broadcast_to(as_column(direct[...]), (HEADS_HERE, 128))
    for g in range(GROUPS_HERE):
        at = slice(g * WIDE, (g + 1) * WIDE)
        gate = jax.nn.silu(gate_in[:, at].astype(F32))
        mixed[:, at] = (mixed[:, at] + values[:, at] * spread(direct_wide, g, 3)[:1]) * gate
        values[:, at] = spread(from_start, g, 2) * gate
    lane_a = lax.broadcasted_iota(jnp.int32, (WIDE, WIDE), 0) // HEAD_DIM
    lane_b = lax.broadcasted_iota(jnp.int32, (WIDE, WIDE), 1) // HEAD_DIM
    same_head = jnp.where(lane_a == lane_b, 1.0, 0.0).astype(BF16)

    token = lax.broadcasted_iota(jnp.int32, (ROWS, ROWS), 0)
    later = lax.broadcasted_iota(jnp.int32, (ROWS, ROWS), 1)
    before = jnp.where(token < later, 1.0, 0.0).astype(BF16)
    expert_row = lax.broadcasted_iota(jnp.int32, (PLANE, ROWS), 0) + z * PLANE
    expert_row = expert_row.astype(F32)
    slot = lax.broadcasted_iota(jnp.int32, (PLANE, CAP, ROWS), 1).astype(F32)
    arrive(metas.at[pl.ds(0, NZ - 1)], mr_sem)
    for o in range(NZ):
        table = meta[...] if o == 0 else metas[o]
        hits = jnp.zeros((PLANE, ROWS), F32)
        shares = jnp.zeros((PLANE, ROWS), F32)
        for k in range(TOPK):
            hit = jnp.where(expert_row == table[k : k + 1, :ROWS], 1.0, 0.0)
            hits = hits + hit
            shares = shares + hit * table[TOPK + k : TOPK + k + 1, :ROWS]
        rank = over(hits.astype(BF16), before, ((1,), (0,)))
        chosen = jnp.where(
            (rank[:, None, :] == slot) & (hits[:, None, :] > 0.5),
            jnp.ones((PLANE, CAP, ROWS), F32),
            jnp.zeros((PLANE, CAP, ROWS), F32),
        )
        chosen_w[o] = chosen.reshape(ROWS, ROWS)
        combine_w[o] = (chosen * shares[:, None, :]).reshape(ROWS, ROWS)

    arrive(plane_logs.at[pl.ds(0, NZ - 1)], plog_r)
    for k in range(NZ - 1):
        factors[2 * PLANE + k] = jnp.exp(plane_logs[k])
    for h, part in enumerate(parts):
        arrive(planes.at[pl.ds(0, NZ - 1), part], slice_r.at[h])
        carried = jnp.zeros((STATE // 2, 128), F32)
        for k in range(NZ - 1):
            joined = carried * factors[2 * PLANE + k, pl.ds(me, 1)] + planes[k, part].astype(F32)
            carried = jnp.where(k < z, joined, carried)
        for k in range(PLANE):
            incoming_send[k, part] = (
                carried * factors[PLANE + k, pl.ds(me, 1)] + before_me[k, part]
            ).astype(BF16)
        for index, target in plane_peers:
            send(incoming_send.at[index, part], incoming.at[me, part], in_s, in_r.at[h], target)
    incoming[me] = incoming_send[me]
    loaded("head_gain", "w", "residual", "expert_gain")
    for h, part in enumerate(parts):
        arrive(incoming.at[pl.ds(0, PLANE - 1), part], in_r.at[h])
    for g in range(GROUPS_HERE):
        at = slice(g * WIDE, (g + 1) * WIDE)
        state = jnp.concatenate([incoming[2 * g], incoming[2 * g + 1]], axis=1)
        carried_out = over(readout[:, g * STATE : (g + 1) * STATE], state, ((1,), (0,)))
        gated = mixed[:, at] + carried_out * values[:, at]
        squares = jnp.zeros((LENGTH, WIDE), F32)
        for term in split_terms(gated * gated, 2):
            squares = squares + over(term, same_head, ((1,), (0,)))
        normed = gated * lax.rsqrt(squares * (1.0 / HEAD_DIM) + EPSILON) * head_gain[:, at]
        heads_out[:, at] = normed.astype(BF16)

    for n in range(PIECES):
        partial = over(heads_out[...], w_out[:, n * COLS : (n + 1) * COLS], ((1,), (0,)))
        mix_send[n] = partial.astype(BF16)
        for d in FAR_X:
            xx = lax.rem(x + d, NX)
            send(
                mix_send.at[n, pl.ds(pl.multiple_of(xx * ROWS, ROWS), ROWS)],
                mix_recv.at[n, NX - d - 1],
                mix_s,
                mix_r.at[n],
                x_peers[d - 1],
            )
    def hop(step, up, n):
        here = ((NZ - step) % NZ) if up else step
        there = ((NZ - step - 1) % NZ) if up else step + 1
        k = 0 if up else 1
        send(
            stream.at[n] if step == 0 else zall.at[here, n],
            zall.at[there, n],
            zs_sem,
            zr_sem.at[k, step, n],
            device(z_at(1 if up else -1), y, c, x),
        )

    def ring_arrived(step, up, n):
        there = ((NZ - step - 1) % NZ) if up else step + 1
        arrive(zall.at[there, n], zr_sem.at[0 if up else 1, step, n])

    def relay(step, n):
        for up in (True, False):
            if step < 2:
                ring_arrived(step, up, n)
                hop(step + 1, up, n)
            elif step == 2:
                ring_arrived(step, up, n)
                if (n < 2) == up:
                    hop(3, up, n)
            elif (n < 2) == up:
                ring_arrived(3, up, n)

    def dispatch(o, n):
        block = stream[n] if o == 0 else zall[o, n]
        packed = over(chosen_w[o].astype(BF16), block, ((1,), (0,)))
        send_rows[o, n] = packed.reshape(PLANE, CAP, COLS).astype(BF16)
        for index, peer in plane_peers:
            send(
                send_rows.at[o, n, index],
                expert_rows.at[o, n * PLANE + me],
                ds_sem,
                dr_sem.at[o],
                peer,
            )
        expert_rows[o, n * PLANE + me] = send_rows[o, n, me]

    def run_expert(blocks):
        gate = lifted = None
        for o in blocks:
            arrive(expert_rows.at[o, pl.ds(0, PIECES * (PLANE - 1))], dr_sem.at[o])
        for n in range(PIECES):
            at = slice(n * COLS, (n + 1) * COLS)
            parts = []
            for o in blocks:
                wide = expert_rows[o, n * PLANE : (n + 1) * PLANE].astype(F32)
                parts.append((wide * slot_scales[:, :, o : o + 1]).reshape(ROWS, COLS))
            piece = (jnp.concatenate(parts, axis=0) * expert_gain[:, at]).astype(BF16)
            g, u = over(piece, rg[at], ((1,), (0,))), over(piece, ru[at], ((1,), (0,)))
            gate, lifted = (g, u) if n == 0 else (gate + g, lifted + u)
        hidden = (jax.nn.silu(gate) * lifted).astype(BF16)
        for n in range(PIECES):
            result = over(hidden, rd[:, n * COLS : (n + 1) * COLS], ((1,), (0,)))
            for k, o in enumerate(blocks):
                expert_out[o, n] = (
                    result[k * ROWS : (k + 1) * ROWS].reshape(PLANE, CAP, COLS).astype(BF16)
                )

    def give_back(o):
        for n in ((0, 2, 1, 3) if o == 4 else (2, 3, 0, 1) if o > 4 else range(PIECES)):
            for index, peer in plane_peers:
                send(
                    expert_out.at[o, n, index], back_rows.at[o, n, me], bs_sem, br_sem.at[o, n], peer
                )
            back_rows[o, n, me] = expert_out[o, n, me]

    def combined(o, n):
        arrive(back_rows.at[o, n, pl.ds(0, PLANE - 1)], br_sem.at[o, n])
        returned = back_rows[o, n].astype(F32).reshape(ROWS, COLS).astype(BF16)
        return over(combine_w[o].astype(BF16), returned, ((0,), (0,)))

    square_sums = []

    def take_piece(n):
        at = slice(n * COLS, (n + 1) * COLS)
        summed = mix_send[n, pl.ds(pl.multiple_of(x * ROWS, ROWS), ROWS)].astype(F32)
        arrive(mix_recv.at[n], mix_r.at[n])
        for d in range(1, NX):
            summed = summed + mix_recv[n, d - 1].astype(F32)
        joined = (residual[:, at].astype(F32) + summed).astype(BF16)
        stream[n] = joined
        hop(0, True, n)
        hop(0, False, n)
        wide = joined.astype(F32)
        square_sums.append(jnp.sum(wide * wide, axis=-1, keepdims=True))

    take_piece(0)
    dispatch(0, 0)
    take_piece(1)
    relay(0, 0)
    dispatch(7, 0)
    dispatch(1, 0)
    dispatch(0, 1)
    take_piece(2)
    relay(0, 1)
    dispatch(7, 1)
    dispatch(1, 1)
    relay(1, 0)
    dispatch(6, 0)
    dispatch(2, 0)
    dispatch(0, 2)
    take_piece(3)
    squares = square_sums[0] + square_sums[1] + square_sums[2] + square_sums[3]
    scale = lax.rsqrt(squares * (1.0 / D) + EPSILON)
    scale_row = jnp.sum(jnp.where(token == later, scale, 0.0), axis=0, keepdims=True)
    scale_send[...] = jnp.zeros((8, 128), F32)
    scale_send[:1, :ROWS] = scale_row
    for d in FAR_Z:
        send(scale_send, scales.at[NZ - d], sc_s, sc_r, z_peers[d - 1])
    relay(0, 2)
    dispatch(7, 2)
    dispatch(1, 2)
    relay(1, 1)
    dispatch(6, 1)
    dispatch(2, 1)
    dispatch(0, 3)
    for n in range(PIECES):
        at = slice(n * COLS, (n + 1) * COLS)
        rows[:, at] = (stream[n].astype(F32) * scale * expert_gain[:, at]).astype(BF16)
    for d in FAR_X:
        send(rows, xall.at[x], xs_sem, xr_sem, x_peers[d - 1])
    relay(2, 0)
    dispatch(5, 0)
    dispatch(3, 0)
    relay(0, 3)
    dispatch(7, 3)
    dispatch(1, 3)
    lane = lax.broadcasted_iota(jnp.int32, (PLANE, CAP, 128), 2)
    by_slot = jnp.zeros((PLANE, CAP, 128), F32)
    arrive(scales.at[pl.ds(0, NZ - 1)], sc_r)
    for o in range(NZ):
        known = scale_row if o == 0 else scales[o, :1, :ROWS]
        found = jnp.sum(chosen_w[o] * known, axis=1, keepdims=True).reshape(PLANE, CAP, 1)
        by_slot = jnp.where(lane == o, found, by_slot)
    slot_send[...] = by_slot
    for index, target in plane_peers:
        send(slot_send.at[index], slot_scales.at[me], sl_s, sl_r, target)
    slot_scales[me] = slot_send[me]
    relay(1, 2)
    dispatch(6, 2)
    dispatch(2, 2)
    relay(2, 1)
    dispatch(5, 1)
    dispatch(3, 1)
    relay(3, 0)
    dispatch(4, 0)
    relay(1, 3)
    dispatch(6, 3)
    dispatch(2, 3)
    loaded("rg", "ru", "rd", "cg", "cu", "cd")
    arrive(slot_scales.at[pl.ds(0, PLANE - 1)], sl_r)
    run_expert((0,))
    relay(2, 2)
    dispatch(5, 2)
    dispatch(3, 2)
    relay(3, 1)
    dispatch(4, 1)
    relay(2, 3)
    dispatch(5, 3)
    run_expert((7, 1))
    relay(3, 2)
    dispatch(4, 2)
    relay(3, 3)
    dispatch(4, 3)
    dispatch(3, 3)
    arrive(xall.at[pl.ds(0, NX - 1)], xr_sem)
    xall[x] = rows[...]
    hidden_rows = xall[...].reshape(NX * ROWS, D)
    gate = over(hidden_rows, cg[...], ((1,), (0,)))
    lifted = over(hidden_rows, cu[...], ((1,), (0,)))
    hidden = (jax.nn.silu(gate) * lifted).astype(BF16)
    shared = over(hidden, cd[...], ((1,), (1,)))
    sh_send[...] = shared.reshape(NX, ROWS, D).astype(BF16)
    for d in FAR_X:
        send(
            sh_send.at[lax.rem(x + d, NX)],
            sh_recv.at[NX - d - 1],
            hs_sem,
            hr_sem,
            x_peers[d - 1],
        )
    run_expert((6, 2))
    run_expert((4,))
    give_back(4)
    run_expert((5, 3))
    for o in (3, 5, 2, 6, 1, 7, 0):
        give_back(o)

    def cell(step, up, n):
        if step == 0:
            return 24 + n
        return (step - 1) * 8 + (0 if up else 4) + n

    def pass_on(step, up, n, piece):
        k = cell(step, up, n)
        rs_send[k] = piece.astype(BF16)
        send(
            rs_send.at[k],
            rs_recv.at[k],
            rss_sem,
            rsr_sem.at[k],
            device(z_at(1 if up else -1), y, c, x),
        )

    def sum_arrived(step, up, n):
        k = cell(step, up, n)
        arrive(rs_recv.at[k], rsr_sem.at[k])
        return rs_recv[k].astype(F32)

    for n in (0, 2, 1, 3):
        pass_on(0, n < 2, n, combined(4, n))
    for step in range(1, 4):
        for up, order in ((True, (0, 1, 2, 3)), (False, (2, 3, 0, 1))):
            for n in order:
                piece = combined(4 - step if up else 4 + step, n)
                if step > 1 or (n < 2) == up:
                    piece = piece + sum_arrived(step - 1, up, n)
                pass_on(step, up, n, piece)
    arrive(sh_recv, hr_sem)
    for n in (2, 3, 0, 1):
        at = slice(n * COLS, (n + 1) * COLS)
        piece = stream[n].astype(F32) + sh_send[x, :, at].astype(F32)
        for d in range(1, NX):
            piece = piece + sh_recv[d - 1, :, at].astype(F32)
        piece = piece + combined(0, n)
        for up in (True, False):
            piece = piece + sum_arrived(3, up, n)
        out[:, at] = piece.astype(BF16)

    for k, (near, _, _) in enumerate(convs):
        arrive(near.at[pl.ds(0, RIM)], rim_s.at[k])
    for ref, sem in (
        (logs.at[pl.ds(0, PLANE - 1)], log_s),
        (metas.at[pl.ds(0, NZ - 1)], ms_sem),
        (own_send.at[pl.ds(0, PLANE - 1)], own_s),
        (plane_logs.at[pl.ds(0, NZ - 1)], plog_s),
        (planes.at[pl.ds(0, NZ - 1)], slice_s),
        (incoming_send.at[pl.ds(0, PLANE - 1)], in_s),
        (mix_recv, mix_s),
        (scales.at[pl.ds(0, NZ - 1)], sc_s),
        (slot_send.at[pl.ds(0, PLANE - 1)], sl_s),
        (xall.at[pl.ds(0, NX - 1)], xs_sem),
        (sh_recv, hs_sem),
        (zall.at[pl.ds(0, NZ - 1)], zs_sem),
        (send_rows.at[pl.ds(0, NZ - 1)], ds_sem),
        (expert_out.at[pl.ds(0, NZ - 1)], bs_sem),
        (rs_send, rss_sem),
    ):
        arrive(ref, sem)


def layer(*arrays):
    vmem = pl.BlockSpec(memory_space=pltpu.VMEM)
    hbm = pl.BlockSpec(memory_space=pl.ANY)
    dma = pltpu.SemaphoreType.DMA
    return pl.pallas_call(
        layer_kernel,
        out_shape=jax.ShapeDtypeStruct((ROWS, D), BF16),
        in_specs=[hbm] * 23,
        out_specs=vmem,
        scratch_shapes=[
            pltpu.VMEM((ROWS, D), BF16),
            pltpu.VMEM((HEADS_HERE, LENGTH), F32),
            pltpu.VMEM((HEADS_HERE, LENGTH), F32),
            pltpu.VMEM((CONV, INNER), BF16),
            pltpu.VMEM((CONV, NARROW), BF16),
            pltpu.VMEM((CONV, NARROW), BF16),
            pltpu.VMEM((1, HEADS_HERE), F32),
            pltpu.VMEM((1, HEADS_HERE), F32),
            pltpu.VMEM((1, INNER), F32),
            pltpu.VMEM((1, D), F32),
            pltpu.VMEM((TOPK, ROWS), jnp.int32),
            pltpu.VMEM((TOPK, ROWS), F32),
            pltpu.VMEM((LENGTH, INNER), BF16),
            pltpu.VMEM((LENGTH, INNER), BF16),
            pltpu.VMEM((LENGTH, NARROW), BF16),
            pltpu.VMEM((LENGTH, NARROW), BF16),
            pltpu.VMEM((INNER, D), BF16),
            pltpu.VMEM((RIM, INNER), BF16),
            pltpu.VMEM((RIM, NARROW), BF16),
            pltpu.VMEM((RIM, NARROW), BF16),
            pltpu.VMEM((LENGTH, WIDE), F32),
            pltpu.VMEM((8 + RIM, WIDE), F32),
            pltpu.VMEM((LENGTH, INNER), F32),
            pltpu.VMEM((LENGTH, INNER), BF16),
            pltpu.VMEM((LENGTH, INNER), BF16),
            pltpu.VMEM((RIM, INNER), F32),
            pltpu.VMEM((RIM, INNER), F32),
            pltpu.VMEM((LENGTH, NARROW), BF16),
            pltpu.VMEM((LENGTH, NARROW), BF16),
            pltpu.VMEM((LENGTH, INNER), F32),
            pltpu.VMEM((LENGTH, INNER), BF16),
            pltpu.VMEM((PAIRS, STATE, 128), BF16),
            pltpu.VMEM((PAIRS, STATE, 128), BF16),
            pltpu.VMEM((PAIRS, STATE, 128), F32),
            pltpu.VMEM((NZ, STATE, 128), BF16),
            pltpu.VMEM((PAIRS, STATE, 128), BF16),
            pltpu.VMEM((PAIRS, STATE, 128), BF16),
            pltpu.VMEM((PLANE, PAIRS, 128), F32),
            pltpu.VMEM((NZ, PAIRS, 128), F32),
            pltpu.VMEM((2 * PLANE + NZ, PAIRS, 128), F32),
            pltpu.VMEM((PIECES, LENGTH, COLS), BF16),
            pltpu.VMEM((PIECES, NX - 1, ROWS, COLS), BF16),
            pltpu.VMEM((PIECES, ROWS, COLS), BF16),
            pltpu.VMEM((ROWS, D), BF16),
            pltpu.VMEM((8, 128), F32),
            pltpu.VMEM((NZ, PIECES, ROWS, COLS), BF16),
            pltpu.VMEM((8, 128), F32),
            pltpu.VMEM((NZ, 8, 128), F32),
            pltpu.VMEM((PLANE, CAP, 128), F32),
            pltpu.VMEM((PLANE, CAP, 128), F32),
            pltpu.VMEM((NZ, ROWS, ROWS), F32),
            pltpu.VMEM((NZ, 8, 128), F32),
            pltpu.VMEM((NZ, ROWS, ROWS), F32),
            pltpu.VMEM((NZ, PIECES, PLANE, CAP, COLS), BF16),
            pltpu.VMEM((NZ, PIECES * PLANE, CAP, COLS), BF16),
            pltpu.VMEM((NZ, PIECES, PLANE, CAP, COLS), BF16),
            pltpu.VMEM((NZ, PIECES, PLANE, CAP, COLS), BF16),
            pltpu.VMEM((28, ROWS, COLS), BF16),
            pltpu.VMEM((28, ROWS, COLS), BF16),
            pltpu.VMEM((NX, ROWS, D), BF16),
            pltpu.VMEM((NX, ROWS, D), BF16),
            pltpu.VMEM((NX - 1, ROWS, D), BF16),
            pltpu.VMEM((D, FE), BF16),
            pltpu.VMEM((D, FE), BF16),
            pltpu.VMEM((FE, D), BF16),
            pltpu.VMEM((D, 128), BF16),
            pltpu.VMEM((D, 128), BF16),
            pltpu.VMEM((D, 128), BF16),
            dma((23,)),
            dma((3,)),
            dma((3,)),
            dma,
            dma,
            dma,
            dma((2,)),
            dma,
            dma,
            dma,
            dma((2,)),
            dma,
            dma((2,)),
            dma,
            dma((PIECES,)),
            dma,
            dma((2, 4, PIECES)),
            dma,
            dma,
            dma,
            dma,
            dma,
            dma,
            dma,
            dma((NZ,)),
            dma,
            dma((NZ, PIECES)),
            dma,
            dma((28,)),
            dma,
            dma,
            dma,
            dma,
        ],
        compiler_params=pltpu.CompilerParams(
            collective_id=1, has_side_effects=True, vmem_limit_bytes=60 * 1024 * 1024
        ),
    )(*arrays)


def shards(
    residual,
    output_gate_projected,
    value_projected_input,
    state_projected_input,
    readout_projected_input,
    step_preactivation,
    position_decay_extra,
    value_conv_kernel,
    state_conv_kernel,
    readout_conv_kernel,
    head_log_decay_rates,
    head_direct_weight,
    head_norm_gain,
    mixer_output_weight,
    expert_norm_gain,
    routed_expert_index,
    routed_expert_weight,
    routed_gate_weight,
    routed_up_weight,
    routed_down_weight,
    common_gate_weight,
    common_up_weight,
    common_down_weight,
):
    return layer(
        residual,
        output_gate_projected,
        value_projected_input,
        state_projected_input,
        readout_projected_input,
        step_preactivation.T,
        position_decay_extra.T,
        value_conv_kernel,
        state_conv_kernel,
        readout_conv_kernel,
        head_log_decay_rates[None, :],
        head_direct_weight[None, :],
        head_norm_gain[None, :],
        mixer_output_weight,
        expert_norm_gain[None, :],
        routed_expert_index.T,
        routed_expert_weight.T,
        routed_gate_weight[0],
        routed_up_weight[0],
        routed_down_weight[0],
        common_gate_weight,
        common_up_weight,
        common_down_weight,
    )


def solution(mesh):
    torus = Mesh(mesh.devices.reshape(8, 4, 2, mesh.shape["tp"]), ("sp_0", "sp_1", "sp_2", "tp"))
    return jax.shard_map(
        shards,
        mesh=torus,
        in_specs=(
            P(SP_TP, None),
            P(SP, "tp"),
            P(SP, "tp"),
            P(SP, "tp"),
            P(SP, "tp"),
            P(SP, "tp"),
            P(SP, "tp"),
            P(None, "tp"),
            P(None, "tp"),
            P(None, "tp"),
            P("tp"),
            P("tp"),
            P("tp"),
            P("tp", None),
            P(),
            P(SP_TP, None),
            P(SP_TP, None),
            P(SP, None, None),
            P(SP, None, None),
            P(SP, None, None),
            P(None, "tp"),
            P(None, "tp"),
            P(None, "tp"),
        ),
        out_specs=P(SP_TP, None),
        check_vma=False,
    )
```

```python
import jax
import jax.numpy as jnp
from jax import lax
from jax.experimental import pallas as pl
from jax.experimental.pallas import tpu as pltpu
from jax.sharding import Mesh
from jax.sharding import PartitionSpec as P

D = 2048
HEAD_DIM = 64
STATE = 128
CONV = 4
SP = ("sp_0", "sp_1", "sp_2")
SP_TP = ("sp_0", "sp_1", "sp_2", "tp")
EPSILON = 1e-06
MESH = pl.DeviceIdType.MESH
BF16 = jnp.bfloat16
F32 = jnp.float32
NZ, NY, NC, NX = 8, 4, 2, 4
PLANE = NY * NC
ROWS = 64
HALF = ROWS // 2
CAP = 8
FE = 256
FAR_Z = (4, 3, 5, 2, 6, 1, 7)
FAR_X = (2, 1, 3)
TOPK = 4
LENGTH = 256
HEADS_HERE = 16
GROUPS_HERE = 4
INNER = HEADS_HERE * HEAD_DIM
NARROW = GROUPS_HERE * STATE
WIDE = 256
PAIRS = 8
RIM = 16
COLS = 512
PIECES = D // COLS
FINE = 256
PARTS = D // FINE


def device(z, y, c, x):
    return {"sp_0": z, "sp_1": y, "sp_2": c, "tp": x}


def arrive(ref, sem):
    pltpu.make_async_copy(ref, ref, sem).wait()


def split_terms(value, count):
    terms = []
    for _ in range(count):
        term = value.astype(BF16)
        terms.append(term)
        value = value - term.astype(F32)
    return terms


def over(a, b, dims):
    return lax.dot_general(a, b, (dims, ((), ())), preferred_element_type=F32)


def layer_kernel(
    residual_hbm,
    gate_hbm,
    value_hbm,
    state_hbm,
    read_hbm,
    step_hbm,
    extra_hbm,
    value_taps_hbm,
    state_taps_hbm,
    read_taps_hbm,
    rates_hbm,
    direct_hbm,
    head_gain_hbm,
    w_hbm,
    expert_gain_hbm,
    index_hbm,
    share_hbm,
    rg_hbm,
    ru_hbm,
    rd_hbm,
    cg_hbm,
    cu_hbm,
    cd_hbm,
    out,
    residual,
    step_raw,
    extra_raw,
    value_taps,
    state_taps,
    read_taps,
    rates,
    direct,
    head_gain,
    expert_gain,
    index_raw,
    share_raw,
    gate_in,
    value_in,
    state_raw,
    read_raw,
    w_out,
    value_rim,
    state_rim,
    read_rim,
    ext,
    top,
    values,
    weighted,
    ending,
    first_sized,
    first_ended,
    state_in,
    readout,
    mixed,
    heads_out,
    own_send,
    gathered,
    edge_send,
    edges,
    before_me,
    planes,
    incoming_send,
    incoming,
    logs,
    plane_logs,
    factors,
    mix_send,
    mix_recv,
    staged,
    stream,
    rows,
    meta,
    zall,
    scale_send,
    scales,
    slot_send,
    slot_scales,
    chosen_w,
    metas,
    combine_w,
    send_rows,
    expert_rows,
    expert_out,
    back_rows,
    rs_send,
    rs_recv,
    xall,
    sh_send,
    sh_recv,
    rg,
    ru,
    rd,
    cg,
    cu,
    cd,
    out_sem,
    load_sem,
    rim_s,
    rim_r,
    log_s,
    log_r,
    edge_s,
    edge_r,
    own_s,
    own_r,
    plog_s,
    plog_r,
    slice_s,
    slice_r,
    in_s,
    in_r,
    mix_s,
    mix_r,
    zs_sem,
    zr_sem,
    sc_s,
    sc_r,
    sl_s,
    sl_r,
    ms_sem,
    mr_sem,
    ds_sem,
    dr_sem,
    last_r,
    bs_sem,
    br_sem,
    rss_sem,
    rsr_sem,
    xs_sem,
    xr_sem,
    hs_sem,
    hr_sem,
):
    z, y, c, x = tuple(lax.axis_index(name) for name in SP_TP)
    me = y * NC + c
    turn = 1 - 2 * c

    def z_at(steps):
        return lax.rem(z + turn * steps + NZ, NZ)

    x_peers = [device(z, y, c, lax.rem(x + d, NX)) for d in range(1, NX)]
    z_peers = [device(z_at(d), y, c, x) for d in range(1, NZ)]
    plane_peers = []
    for dy in (2, 1, 3, 0):
        for dc in range(NC):
            if dy or dc:
                yy, cc = lax.rem(y + dy, NY), lax.rem(c + dc, NC)
                plane_peers.append((yy * NC + cc, device(z, yy, cc, x)))

    def along(step):
        count = NZ * NY * NC
        flat = lax.rem((z * NY + y) * NC + c + step + count, count)
        return device(flat // (NY * NC), lax.rem(flat // NC, NY), lax.rem(flat, NC), x)

    greeted = x_peers + z_peers + [peer for _, peer in plane_peers] + [along(1), along(-1)]
    barrier = pltpu.get_barrier_semaphore()
    for target in greeted:
        pl.semaphore_signal(barrier, inc=1, device_id=target, device_id_type=MESH)
    loads = {}
    for k, (name, far, near) in enumerate(
        (
            ("step", step_hbm, step_raw),
            ("extra", extra_hbm, extra_raw),
            ("rates", rates_hbm, rates),
            ("value", value_hbm, value_in),
            ("state", state_hbm, state_raw),
            ("read", read_hbm, read_raw),
            ("value_taps", value_taps_hbm, value_taps),
            ("state_taps", state_taps_hbm, state_taps),
            ("read_taps", read_taps_hbm, read_taps),
            ("index", index_hbm, index_raw),
            ("share", share_hbm, share_raw),
            ("direct", direct_hbm, direct),
            ("gate", gate_hbm, gate_in),
            ("head_gain", head_gain_hbm, head_gain),
            ("w", w_hbm, w_out),
            ("residual", residual_hbm, residual),
            ("expert_gain", expert_gain_hbm, expert_gain),
            ("rg", rg_hbm, rg),
            ("ru", ru_hbm, ru),
            ("rd", rd_hbm, rd),
            ("cg", cg_hbm, cg),
            ("cu", cu_hbm, cu),
            ("cd", cd_hbm, cd),
        )
    ):
        loads[name] = pltpu.make_async_copy(far, near, load_sem.at[k])
        loads[name].start()

    def loaded(*wanted):
        for name in wanted:
            loads[name].wait()

    def send(src, dst, send_sem, recv_sem, target):
        copy = pltpu.make_async_remote_copy(
            src_ref=src,
            dst_ref=dst,
            send_sem=send_sem,
            recv_sem=recv_sem,
            device_id=target,
            device_id_type=MESH,
        )
        copy.start()

    loaded("step", "extra", "rates")
    sizes = jax.nn.softplus(step_raw[...])
    head_a = lax.broadcasted_iota(jnp.int32, (HEADS_HERE, HEADS_HERE), 0)
    head_b = lax.broadcasted_iota(jnp.int32, (HEADS_HERE, HEADS_HERE), 1)

    def as_column(row):
        square = jnp.broadcast_to(row, (HEADS_HERE, HEADS_HERE))
        return jnp.sum(jnp.where(head_a == head_b, square, 0.0), axis=1, keepdims=True)

    log_decay = sizes * as_column(-jnp.exp(rates[...])) + extra_raw[...]
    early = lax.broadcasted_iota(jnp.int32, (LENGTH, LENGTH), 0)
    late = lax.broadcasted_iota(jnp.int32, (LENGTH, LENGTH), 1)
    causal = early >= late
    lower = jnp.where(causal, 1.0, 0.0).astype(BF16)
    cumulative = jnp.zeros((LENGTH, HEADS_HERE), F32)
    by_head = jnp.zeros((HEADS_HERE, LENGTH), F32)
    for term in split_terms(log_decay, 3):
        cumulative = cumulative + over(lower, term, ((1,), (1,)))
        by_head = by_head + over(term, lower, ((1,), (1,)))
    head_row = lax.broadcasted_iota(jnp.int32, (HEADS_HERE, WIDE), 0)
    lane_head = lax.broadcasted_iota(jnp.int32, (HEADS_HERE, WIDE), 1) // HEAD_DIM
    spreads = [
        jnp.where(head_row == lane_head + 4 * g, 1.0, 0.0).astype(BF16) for g in range(GROUPS_HERE)
    ]

    def spread(value, g, count):
        wide = jnp.zeros((value.shape[1], WIDE), F32)
        for term in split_terms(value, count):
            wide = wide + over(term, spreads[g], ((0,), (0,)))
        return wide

    total = by_head[:, LENGTH - 1 :]
    total_wide = jnp.broadcast_to(total, (HEADS_HERE, 128))
    for g in range(GROUPS_HERE):
        wide = spread(total_wide, g, 3)
        for k in range(2):
            logs[me, pl.ds(2 * g + k, 1)] = wide[:1, k * 128 : (k + 1) * 128]

    loaded("index", "share")
    meta[...] = jnp.zeros((8, 128), F32)
    meta[:TOPK, :ROWS] = index_raw[...].astype(F32)
    meta[TOPK:, :ROWS] = share_raw[...]
    loaded("value", "state", "read", "value_taps", "state_taps", "read_taps")
    pl.semaphore_wait(barrier, len(greeted))
    convs = (
        (value_in, value_rim, value_taps),
        (state_raw, state_rim, state_taps),
        (read_raw, read_rim, read_taps),
    )
    for k, (near, rim, _) in enumerate(convs):
        send(near.at[pl.ds(LENGTH - RIM, RIM)], rim, rim_s.at[k], rim_r.at[k], along(1))
    for _, target in plane_peers:
        send(logs.at[me], logs.at[me], log_s, log_r, target)
    for d in FAR_Z:
        send(meta, metas.at[NZ - d], ms_sem, mr_sem, z_peers[d - 1])

    def late_rows(which, lo):
        near, _, taps = convs[which]
        ext[...] = near[:, lo : lo + WIDE].astype(F32)
        weights = taps[:, lo : lo + WIDE].astype(F32)
        sums = ext[RIM - 3 : LENGTH - 3] * weights[0:1]
        for k in range(1, CONV):
            sums = sums + ext[RIM - 3 + k : LENGTH - 3 + k] * weights[k : k + 1]
        return jax.nn.silu(sums)

    first = jnp.where(z + y + c == 0, 0.0, 1.0)

    def early_rows(which, lo):
        near, rim, taps = convs[which]
        top[:8] = rim[:, lo : lo + WIDE].astype(F32)[RIM - 8 :] * first
        top[8:] = near[:RIM, lo : lo + WIDE].astype(F32)
        weights = taps[:, lo : lo + WIDE].astype(F32)
        sums = top[5 : 5 + RIM] * weights[0:1]
        for k in range(1, CONV):
            sums = sums + top[5 + k : 5 + k + RIM] * weights[k : k + 1]
        return jax.nn.silu(sums)

    ends = jnp.exp(total - by_head) * sizes
    for lo in range(0, NARROW, WIDE):
        state_in[RIM:, lo : lo + WIDE] = late_rows(1, lo).astype(BF16)
    for g in range(GROUPS_HERE):
        at = slice(g * WIDE, (g + 1) * WIDE)
        value = late_rows(0, g * WIDE)
        values[RIM:, at] = value
        sized = spread(sizes, g, 2)
        ended = spread(ends, g, 2)
        weighted[RIM:, at] = (value * sized[RIM:]).astype(BF16)
        ending[RIM:, at] = (value * ended[RIM:]).astype(BF16)
        first_sized[:, at] = sized[:RIM]
        first_ended[:, at] = ended[:RIM]
        fresh = over(state_in[RIM:, g * STATE : (g + 1) * STATE], ending[RIM:, at], ((0,), (0,)))
        for k in range(2):
            own_send[2 * g + k] = fresh[:, k * 128 : (k + 1) * 128].astype(BF16)
    parts = [pl.ds(k * (STATE // 2), STATE // 2) for k in range(2)]
    for k, part in enumerate(parts):
        for index, target in plane_peers:
            send(own_send.at[index, part], gathered.at[me, part], own_s, own_r.at[k], target)
    gathered[me] = own_send[me]
    arrive(state_rim, rim_r.at[1])
    for lo in range(0, NARROW, WIDE):
        state_in[:RIM, lo : lo + WIDE] = early_rows(1, lo).astype(BF16)
    arrive(value_rim, rim_r.at[0])
    for g in range(GROUPS_HERE):
        at = slice(g * WIDE, (g + 1) * WIDE)
        value = early_rows(0, g * WIDE)
        values[:RIM, at] = value
        edge = (value * first_ended[:, at]).astype(BF16)
        for k in range(2):
            edge_send[2 * g + k, 0] = state_in[:RIM, g * STATE : (g + 1) * STATE]
            edge_send[2 * g + k, 1] = edge[:, k * 128 : (k + 1) * 128]
    for index, target in plane_peers:
        send(edge_send.at[index], edges.at[me], edge_s, edge_r, target)
    edges[me] = edge_send[me]
    for lo in range(0, NARROW, WIDE):
        readout[RIM:, lo : lo + WIDE] = late_rows(2, lo).astype(BF16)

    arrive(logs.at[pl.ds(0, PLANE - 1)], log_r)
    reach = jnp.zeros((PAIRS, 128), F32)
    for k in range(PLANE):
        factors[k] = jnp.exp(logs[k])
        factors[PLANE + k] = jnp.exp(reach)
        reach = reach + logs[k]
    plane_logs[z] = reach
    for d in FAR_Z:
        send(plane_logs.at[z], plane_logs.at[z], plog_s, plog_r, z_peers[d - 1])

    arrive(read_rim, rim_r.at[2])
    for lo in range(0, NARROW, WIDE):
        readout[:RIM, lo : lo + WIDE] = early_rows(2, lo).astype(BF16)
    weighted[:RIM] = (values[:RIM] * first_sized[...]).astype(BF16)

    def within(g):
        scores = over(
            readout[:, g * STATE : (g + 1) * STATE],
            state_in[:, g * STATE : (g + 1) * STATE],
            ((1,), (1,)),
        )
        scores = jnp.where(causal, scores, 0.0)
        group_values = weighted[:, g * WIDE : (g + 1) * WIDE]
        lane = lax.broadcasted_iota(jnp.int32, (LENGTH, WIDE), 1) // HEAD_DIM
        result = jnp.zeros((LENGTH, WIDE), F32)
        for r in range(4):
            h = 4 * g + r
            span = cumulative[:, h : h + 1] - by_head[h : h + 1, :]
            decay = jnp.exp(jnp.where(causal, span, -jnp.inf))
            chosen = jnp.where(lane == r, group_values, jnp.zeros_like(group_values))
            result = result + over((scores * decay).astype(BF16), chosen, ((1,), (0,)))
        mixed[:, g * WIDE : (g + 1) * WIDE] = result

    within(0)

    arrive(edges.at[pl.ds(0, PLANE - 1)], edge_r)
    for k in range(PLANE):
        before_me[k] = over(edges[k, 0], edges[k, 1], ((0,), (0,)))
    for h, part in enumerate(parts):
        arrive(gathered.at[pl.ds(0, PLANE - 1), part], own_r.at[h])
        carried = jnp.zeros((STATE // 2, 128), F32)
        for k in range(PLANE):
            fresh = gathered[k, part].astype(F32) + before_me[k, part]
            before_me[k, part] = carried
            carried = carried * factors[k, pl.ds(me, 1)] + fresh
        planes[z, part] = carried.astype(BF16)
        for d in FAR_Z:
            send(planes.at[z, part], planes.at[z, part], slice_s, slice_r.at[h], z_peers[d - 1])

    within(1)
    within(2)
    within(3)
    loaded("direct", "gate")
    from_start = jnp.exp(by_head)
    direct_wide = jnp.broadcast_to(as_column(direct[...]), (HEADS_HERE, 128))
    for g in range(GROUPS_HERE):
        at = slice(g * WIDE, (g + 1) * WIDE)
        gate = jax.nn.silu(gate_in[:, at].astype(F32))
        mixed[:, at] = (mixed[:, at] + values[:, at] * spread(direct_wide, g, 3)[:1]) * gate
        values[:, at] = spread(from_start, g, 2) * gate
    lane_a = lax.broadcasted_iota(jnp.int32, (WIDE, WIDE), 0) // HEAD_DIM
    lane_b = lax.broadcasted_iota(jnp.int32, (WIDE, WIDE), 1) // HEAD_DIM
    same_head = jnp.where(lane_a == lane_b, 1.0, 0.0).astype(BF16)

    token = lax.broadcasted_iota(jnp.int32, (ROWS, ROWS), 0)
    later = lax.broadcasted_iota(jnp.int32, (ROWS, ROWS), 1)
    before = jnp.where(token < later, 1.0, 0.0).astype(BF16)
    expert_row = lax.broadcasted_iota(jnp.int32, (PLANE, ROWS), 0) + z * PLANE
    expert_row = expert_row.astype(F32)
    slot = lax.broadcasted_iota(jnp.int32, (PLANE, CAP, ROWS), 1).astype(F32)
    arrive(metas.at[pl.ds(0, NZ - 1)], mr_sem)
    for o in range(NZ):
        table = meta[...] if o == 0 else metas[o]
        hits = jnp.zeros((PLANE, ROWS), F32)
        shares = jnp.zeros((PLANE, ROWS), F32)
        for k in range(TOPK):
            hit = jnp.where(expert_row == table[k : k + 1, :ROWS], 1.0, 0.0)
            hits = hits + hit
            shares = shares + hit * table[TOPK + k : TOPK + k + 1, :ROWS]
        rank = over(hits.astype(BF16), before, ((1,), (0,)))
        chosen = jnp.where(
            (rank[:, None, :] == slot) & (hits[:, None, :] > 0.5),
            jnp.ones((PLANE, CAP, ROWS), F32),
            jnp.zeros((PLANE, CAP, ROWS), F32),
        )
        chosen_w[o] = chosen.reshape(ROWS, ROWS)
        combine_w[o] = (chosen * shares[:, None, :]).reshape(ROWS, ROWS)

    arrive(plane_logs.at[pl.ds(0, NZ - 1)], plog_r)
    for k in range(NZ - 1):
        factors[2 * PLANE + k] = jnp.exp(plane_logs[k])
    for h, part in enumerate(parts):
        arrive(planes.at[pl.ds(0, NZ - 1), part], slice_r.at[h])
        carried = jnp.zeros((STATE // 2, 128), F32)
        for k in range(NZ - 1):
            joined = carried * factors[2 * PLANE + k, pl.ds(me, 1)] + planes[k, part].astype(F32)
            carried = jnp.where(k < z, joined, carried)
        for k in range(PLANE):
            incoming_send[k, part] = (
                carried * factors[PLANE + k, pl.ds(me, 1)] + before_me[k, part]
            ).astype(BF16)
        for index, target in plane_peers:
            send(incoming_send.at[index, part], incoming.at[me, part], in_s, in_r.at[h], target)
    incoming[me] = incoming_send[me]
    loaded("head_gain", "w", "residual", "expert_gain")
    blank = jnp.zeros((STATE // 2, WIDE), BF16)

    def carried_part(g, h):
        half = jnp.concatenate([incoming[2 * g, parts[h]], incoming[2 * g + 1, parts[h]]], axis=1)
        state = jnp.concatenate([half, blank] if h == 0 else [blank, half], axis=0)
        at = slice(g * WIDE, (g + 1) * WIDE)
        return over(readout[:, g * STATE : (g + 1) * STATE], state, ((1,), (0,))) * values[:, at]

    arrive(incoming.at[pl.ds(0, PLANE - 1), parts[0]], in_r.at[0])
    for g in range(GROUPS_HERE):
        at = slice(g * WIDE, (g + 1) * WIDE)
        mixed[:, at] = mixed[:, at] + carried_part(g, 0)
    arrive(incoming.at[pl.ds(0, PLANE - 1), parts[1]], in_r.at[1])
    for g in range(GROUPS_HERE):
        at = slice(g * WIDE, (g + 1) * WIDE)
        gated = mixed[:, at] + carried_part(g, 1)
        squares = over((gated * gated).astype(BF16), same_head, ((1,), (0,)))
        normed = gated * lax.rsqrt(squares * (1.0 / HEAD_DIM) + EPSILON) * head_gain[:, at]
        heads_out[:, at] = normed.astype(BF16)

    for m in range(PIECES):
        partial = over(heads_out[...], w_out[:, m * COLS : (m + 1) * COLS], ((1,), (0,)))
        for n in (2 * m, 2 * m + 1):
            lo = (n - 2 * m) * FINE
            mix_send[n] = partial[:, lo : lo + FINE].astype(BF16)
            for d in FAR_X:
                xx = lax.rem(x + d, NX)
                send(
                    mix_send.at[n, pl.ds(pl.multiple_of(xx * ROWS, ROWS), ROWS)],
                    mix_recv.at[n, NX - d - 1],
                    mix_s,
                    mix_r.at[n],
                    x_peers[d - 1],
                )
    def hop(step, up, n):
        here = ((NZ - step) % NZ) if up else step
        there = ((NZ - step - 1) % NZ) if up else step + 1
        k = 0 if up else 1
        send(
            stream.at[n] if step == 0 else zall.at[here, n],
            zall.at[there, n],
            zs_sem,
            zr_sem.at[k, step, n],
            device(z_at(1 if up else -1), y, c, x),
        )

    def ring_arrived(step, up, n):
        there = ((NZ - step - 1) % NZ) if up else step + 1
        arrive(zall.at[there, n], zr_sem.at[0 if up else 1, step, n])

    def relay(step, n):
        for up in (True, False):
            if step < 2:
                ring_arrived(step, up, n)
                hop(step + 1, up, n)
            elif step == 2:
                ring_arrived(step, up, n)
                if (n < PARTS // 2) == up:
                    hop(3, up, n)
            elif (n < PARTS // 2) == up:
                ring_arrived(3, up, n)

    def dispatch(o, n):
        for k in range(2):
            block = stream[2 * n + k] if o == 0 else zall[o, 2 * n + k]
            packed = over(chosen_w[o].astype(BF16), block, ((1,), (0,)))
            send_rows[o, n, :, :, k * FINE : (k + 1) * FINE] = packed.reshape(
                PLANE, CAP, FINE
            ).astype(BF16)
        for index, peer in plane_peers:
            send(
                send_rows.at[o, n, index],
                expert_rows.at[o, n * PLANE + me],
                ds_sem,
                last_r.at[n] if o == 4 else dr_sem.at[o],
                peer,
            )
        expert_rows[o, n * PLANE + me] = send_rows[o, n, me]

    def run_expert(blocks):
        gate = lifted = None
        for o in blocks:
            if o != 4:
                arrive(expert_rows.at[o, pl.ds(0, PIECES * (PLANE - 1))], dr_sem.at[o])
        for n in range(PIECES):
            if blocks == (4,):
                arrive(expert_rows.at[4, pl.ds(n * PLANE, PLANE - 1)], last_r.at[n])
            at = slice(n * COLS, (n + 1) * COLS)
            parts = []
            for o in blocks:
                wide = expert_rows[o, n * PLANE : (n + 1) * PLANE].astype(F32)
                parts.append((wide * slot_scales[:, :, o : o + 1]).reshape(ROWS, COLS))
            piece = (jnp.concatenate(parts, axis=0) * expert_gain[:, at]).astype(BF16)
            g, u = over(piece, rg[at], ((1,), (0,))), over(piece, ru[at], ((1,), (0,)))
            gate, lifted = (g, u) if n == 0 else (gate + g, lifted + u)
        hidden = (jax.nn.silu(gate) * lifted).astype(BF16)
        for n in (0, 2, 1, 3):
            result = over(hidden, rd[:, n * COLS : (n + 1) * COLS], ((1,), (0,)))
            for k, o in enumerate(blocks):
                expert_out[o, n] = (
                    result[k * ROWS : (k + 1) * ROWS].reshape(PLANE, CAP, COLS).astype(BF16)
                )
            if blocks == (4,):
                give_piece(4, n)

    def give_piece(o, n):
        for index, peer in plane_peers:
            send(expert_out.at[o, n, index], back_rows.at[o, n, me], bs_sem, br_sem.at[o, n], peer)
        back_rows[o, n, me] = expert_out[o, n, me]

    def give_back(o):
        for n in (2, 3, 0, 1) if o > 4 else range(PIECES):
            give_piece(o, n)

    def combined(o, n):
        arrive(back_rows.at[o, n, pl.ds(0, PLANE - 1)], br_sem.at[o, n])
        returned = back_rows[o, n].astype(F32).reshape(ROWS, COLS).astype(BF16)
        return over(combine_w[o].astype(BF16), returned, ((0,), (0,)))

    square_sums = []

    def take_piece(n):
        at = slice(n * FINE, (n + 1) * FINE)
        summed = mix_send[n, pl.ds(pl.multiple_of(x * ROWS, ROWS), ROWS)].astype(F32)
        arrive(mix_recv.at[n], mix_r.at[n])
        for d in range(1, NX):
            summed = summed + mix_recv[n, d - 1].astype(F32)
        joined = (residual[:, at].astype(F32) + summed).astype(BF16)
        stream[n] = joined
        hop(0, True, n)
        hop(0, False, n)
        wide = joined.astype(F32)
        square_sums.append(jnp.sum(wide * wide, axis=-1, keepdims=True))

    take_piece(0)
    take_piece(1)
    dispatch(0, 0)
    take_piece(2)
    relay(0, 0)
    take_piece(3)
    dispatch(0, 1)
    relay(0, 1)
    dispatch(7, 0)
    dispatch(1, 0)
    take_piece(4)
    relay(0, 2)
    relay(1, 0)
    take_piece(5)
    dispatch(0, 2)
    relay(0, 3)
    dispatch(7, 1)
    dispatch(1, 1)
    relay(1, 1)
    dispatch(6, 0)
    dispatch(2, 0)
    take_piece(6)
    relay(0, 4)
    relay(1, 2)
    take_piece(7)
    dispatch(0, 3)
    squares = sum(square_sums)
    scale = lax.rsqrt(squares * (1.0 / D) + EPSILON)
    scale_row = jnp.sum(jnp.where(token == later, scale, 0.0), axis=0, keepdims=True)
    scale_send[...] = jnp.zeros((8, 128), F32)
    scale_send[:1, :ROWS] = scale_row
    for d in FAR_Z:
        send(scale_send, scales.at[NZ - d], sc_s, sc_r, z_peers[d - 1])
    relay(2, 0)
    for n in range(PARTS):
        at = slice(n * FINE, (n + 1) * FINE)
        rows[:, at] = (stream[n].astype(F32) * scale * expert_gain[:, at]).astype(BF16)
    for d in FAR_X:
        send(rows, xall.at[x], xs_sem, xr_sem, x_peers[d - 1])
    relay(0, 5)
    dispatch(7, 2)
    dispatch(1, 2)
    relay(1, 3)
    dispatch(6, 1)
    dispatch(2, 1)
    relay(2, 1)
    dispatch(5, 0)
    dispatch(3, 0)
    relay(0, 6)
    relay(1, 4)
    relay(2, 2)
    relay(0, 7)
    dispatch(7, 3)
    dispatch(1, 3)
    lane = lax.broadcasted_iota(jnp.int32, (PLANE, CAP, 128), 2)
    by_slot = jnp.zeros((PLANE, CAP, 128), F32)
    arrive(scales.at[pl.ds(0, NZ - 1)], sc_r)
    for o in range(NZ):
        known = scale_row if o == 0 else scales[o, :1, :ROWS]
        found = jnp.sum(chosen_w[o] * known, axis=1, keepdims=True).reshape(PLANE, CAP, 1)
        by_slot = jnp.where(lane == o, found, by_slot)
    slot_send[...] = by_slot
    for index, target in plane_peers:
        send(slot_send.at[index], slot_scales.at[me], sl_s, sl_r, target)
    slot_scales[me] = slot_send[me]
    relay(3, 0)
    relay(1, 5)
    dispatch(6, 2)
    dispatch(2, 2)
    relay(2, 3)
    dispatch(5, 1)
    dispatch(3, 1)
    relay(3, 1)
    dispatch(4, 0)
    relay(1, 6)
    relay(2, 4)
    relay(3, 2)
    relay(1, 7)
    dispatch(6, 3)
    dispatch(2, 3)
    loaded("rg", "ru", "rd", "cg", "cu", "cd")
    arrive(slot_scales.at[pl.ds(0, PLANE - 1)], sl_r)
    run_expert((0,))
    relay(2, 5)
    dispatch(5, 2)
    dispatch(3, 2)
    relay(3, 3)
    dispatch(4, 1)
    relay(3, 4)
    relay(2, 6)
    relay(2, 7)
    dispatch(5, 3)
    run_expert((7, 1))
    relay(3, 5)
    dispatch(4, 2)
    relay(3, 6)
    relay(3, 7)
    dispatch(4, 3)
    dispatch(3, 3)
    give_back(1)
    arrive(xall.at[pl.ds(0, NX - 1)], xr_sem)
    xall[x] = rows[...]
    hidden_rows = xall[...].reshape(NX * ROWS, D)
    gate = over(hidden_rows, cg[...], ((1,), (0,)))
    lifted = over(hidden_rows, cu[...], ((1,), (0,)))
    hidden = (jax.nn.silu(gate) * lifted).astype(BF16)
    shared = over(hidden, cd[...], ((1,), (1,)))
    sh_send[...] = shared.reshape(NX, ROWS, D).astype(BF16)
    for d in FAR_X:
        send(
            sh_send.at[lax.rem(x + d, NX)],
            sh_recv.at[NX - d - 1],
            hs_sem,
            hr_sem,
            x_peers[d - 1],
        )
    run_expert((6, 2))
    run_expert((4,))
    run_expert((5, 3))
    for o in (3, 5, 2, 6, 7, 0):
        give_back(o)

    def cell(step, up, n):
        if step == 0:
            return 24 + n
        return (step - 1) * 8 + (0 if up else 4) + n

    def pass_on(step, up, n, piece):
        k = cell(step, up, n)
        rs_send[k] = piece.astype(BF16)
        send(
            rs_send.at[k],
            rs_recv.at[k],
            rss_sem,
            rsr_sem.at[k],
            device(z_at(1 if up else -1), y, c, x),
        )

    def sum_arrived(step, up, n):
        k = cell(step, up, n)
        arrive(rs_recv.at[k], rsr_sem.at[k])
        return rs_recv[k].astype(F32)

    for n in (0, 2, 1, 3):
        pass_on(0, n < 2, n, combined(4, n))
    for step in range(1, 4):
        for up, order in ((True, (0, 1, 2, 3)), (False, (2, 3, 0, 1))):
            for n in order:
                piece = combined(4 - step if up else 4 + step, n)
                if step > 1 or (n < 2) == up:
                    piece = piece + sum_arrived(step - 1, up, n)
                pass_on(step, up, n, piece)
    arrive(sh_recv, hr_sem)
    for n in (2, 3, 0, 1):
        at = slice(n * COLS, (n + 1) * COLS)
        piece = jnp.concatenate([stream[2 * n], stream[2 * n + 1]], axis=1).astype(F32)
        piece = piece + sh_send[x, :, at].astype(F32)
        for d in range(1, NX):
            piece = piece + sh_recv[d - 1, :, at].astype(F32)
        piece = piece + combined(0, n)
        for up in (True, False):
            piece = piece + sum_arrived(3, up, n)
        staged[:, at] = piece.astype(BF16)
        pltpu.make_async_copy(staged.at[:, at], out.at[:, at], out_sem).start()

    for k, (near, _, _) in enumerate(convs):
        arrive(near.at[pl.ds(0, RIM)], rim_s.at[k])
    for ref, sem in (
        (logs.at[pl.ds(0, PLANE - 1)], log_s),
        (metas.at[pl.ds(0, NZ - 1)], ms_sem),
        (own_send.at[pl.ds(0, PLANE - 1)], own_s),
        (edge_send.at[pl.ds(0, PLANE - 1)], edge_s),
        (plane_logs.at[pl.ds(0, NZ - 1)], plog_s),
        (planes.at[pl.ds(0, NZ - 1)], slice_s),
        (incoming_send.at[pl.ds(0, PLANE - 1)], in_s),
        (mix_recv, mix_s),
        (scales.at[pl.ds(0, NZ - 1)], sc_s),
        (slot_send.at[pl.ds(0, PLANE - 1)], sl_s),
        (xall.at[pl.ds(0, NX - 1)], xs_sem),
        (sh_recv, hs_sem),
        (zall.at[pl.ds(0, NZ - 1)], zs_sem),
        (send_rows.at[pl.ds(0, NZ - 1)], ds_sem),
        (expert_out.at[pl.ds(0, NZ - 1)], bs_sem),
        (rs_send, rss_sem),
    ):
        arrive(ref, sem)
    pltpu.make_async_copy(staged, out, out_sem).wait()


def layer(*arrays):
    hbm = pl.BlockSpec(memory_space=pl.ANY)
    dma = pltpu.SemaphoreType.DMA
    return pl.pallas_call(
        layer_kernel,
        out_shape=jax.ShapeDtypeStruct((ROWS, D), BF16),
        in_specs=[hbm] * 23,
        out_specs=hbm,
        scratch_shapes=[
            pltpu.VMEM((ROWS, D), BF16),
            pltpu.VMEM((HEADS_HERE, LENGTH), F32),
            pltpu.VMEM((HEADS_HERE, LENGTH), F32),
            pltpu.VMEM((CONV, INNER), BF16),
            pltpu.VMEM((CONV, NARROW), BF16),
            pltpu.VMEM((CONV, NARROW), BF16),
            pltpu.VMEM((1, HEADS_HERE), F32),
            pltpu.VMEM((1, HEADS_HERE), F32),
            pltpu.VMEM((1, INNER), F32),
            pltpu.VMEM((1, D), F32),
            pltpu.VMEM((TOPK, ROWS), jnp.int32),
            pltpu.VMEM((TOPK, ROWS), F32),
            pltpu.VMEM((LENGTH, INNER), BF16),
            pltpu.VMEM((LENGTH, INNER), BF16),
            pltpu.VMEM((LENGTH, NARROW), BF16),
            pltpu.VMEM((LENGTH, NARROW), BF16),
            pltpu.VMEM((INNER, D), BF16),
            pltpu.VMEM((RIM, INNER), BF16),
            pltpu.VMEM((RIM, NARROW), BF16),
            pltpu.VMEM((RIM, NARROW), BF16),
            pltpu.VMEM((LENGTH, WIDE), F32),
            pltpu.VMEM((8 + RIM, WIDE), F32),
            pltpu.VMEM((LENGTH, INNER), F32),
            pltpu.VMEM((LENGTH, INNER), BF16),
            pltpu.VMEM((LENGTH, INNER), BF16),
            pltpu.VMEM((RIM, INNER), F32),
            pltpu.VMEM((RIM, INNER), F32),
            pltpu.VMEM((LENGTH, NARROW), BF16),
            pltpu.VMEM((LENGTH, NARROW), BF16),
            pltpu.VMEM((LENGTH, INNER), F32),
            pltpu.VMEM((LENGTH, INNER), BF16),
            pltpu.VMEM((PAIRS, STATE, 128), BF16),
            pltpu.VMEM((PAIRS, STATE, 128), BF16),
            pltpu.VMEM((PAIRS, 2, RIM, 128), BF16),
            pltpu.VMEM((PLANE, 2, RIM, 128), BF16),
            pltpu.VMEM((PAIRS, STATE, 128), F32),
            pltpu.VMEM((NZ, STATE, 128), BF16),
            pltpu.VMEM((PAIRS, STATE, 128), BF16),
            pltpu.VMEM((PAIRS, STATE, 128), BF16),
            pltpu.VMEM((PLANE, PAIRS, 128), F32),
            pltpu.VMEM((NZ, PAIRS, 128), F32),
            pltpu.VMEM((2 * PLANE + NZ, PAIRS, 128), F32),
            pltpu.VMEM((PARTS, LENGTH, FINE), BF16),
            pltpu.VMEM((PARTS, NX - 1, ROWS, FINE), BF16),
            pltpu.VMEM((ROWS, D), BF16),
            pltpu.VMEM((PARTS, ROWS, FINE), BF16),
            pltpu.VMEM((ROWS, D), BF16),
            pltpu.VMEM((8, 128), F32),
            pltpu.VMEM((NZ, PARTS, ROWS, FINE), BF16),
            pltpu.VMEM((8, 128), F32),
            pltpu.VMEM((NZ, 8, 128), F32),
            pltpu.VMEM((PLANE, CAP, 128), F32),
            pltpu.VMEM((PLANE, CAP, 128), F32),
            pltpu.VMEM((NZ, ROWS, ROWS), F32),
            pltpu.VMEM((NZ, 8, 128), F32),
            pltpu.VMEM((NZ, ROWS, ROWS), F32),
            pltpu.VMEM((NZ, PIECES, PLANE, CAP, COLS), BF16),
            pltpu.VMEM((NZ, PIECES * PLANE, CAP, COLS), BF16),
            pltpu.VMEM((NZ, PIECES, PLANE, CAP, COLS), BF16),
            pltpu.VMEM((NZ, PIECES, PLANE, CAP, COLS), BF16),
            pltpu.VMEM((28, ROWS, COLS), BF16),
            pltpu.VMEM((28, ROWS, COLS), BF16),
            pltpu.VMEM((NX, ROWS, D), BF16),
            pltpu.VMEM((NX, ROWS, D), BF16),
            pltpu.VMEM((NX - 1, ROWS, D), BF16),
            pltpu.VMEM((D, FE), BF16),
            pltpu.VMEM((D, FE), BF16),
            pltpu.VMEM((FE, D), BF16),
            pltpu.VMEM((D, 128), BF16),
            pltpu.VMEM((D, 128), BF16),
            pltpu.VMEM((D, 128), BF16),
            dma,
            dma((23,)),
            dma((3,)),
            dma((3,)),
            dma,
            dma,
            dma,
            dma,
            dma,
            dma((2,)),
            dma,
            dma,
            dma,
            dma((2,)),
            dma,
            dma((2,)),
            dma,
            dma((PARTS,)),
            dma,
            dma((2, 4, PARTS)),
            dma,
            dma,
            dma,
            dma,
            dma,
            dma,
            dma,
            dma((NZ,)),
            dma((PIECES,)),
            dma,
            dma((NZ, PIECES)),
            dma,
            dma((28,)),
            dma,
            dma,
            dma,
            dma,
        ],
        compiler_params=pltpu.CompilerParams(
            collective_id=1, has_side_effects=True, vmem_limit_bytes=60 * 1024 * 1024
        ),
    )(*arrays)


def shards(
    residual,
    output_gate_projected,
    value_projected_input,
    state_projected_input,
    readout_projected_input,
    step_preactivation,
    position_decay_extra,
    value_conv_kernel,
    state_conv_kernel,
    readout_conv_kernel,
    head_log_decay_rates,
    head_direct_weight,
    head_norm_gain,
    mixer_output_weight,
    expert_norm_gain,
    routed_expert_index,
    routed_expert_weight,
    routed_gate_weight,
    routed_up_weight,
    routed_down_weight,
    common_gate_weight,
    common_up_weight,
    common_down_weight,
):
    return layer(
        residual,
        output_gate_projected,
        value_projected_input,
        state_projected_input,
        readout_projected_input,
        step_preactivation.T,
        position_decay_extra.T,
        value_conv_kernel,
        state_conv_kernel,
        readout_conv_kernel,
        head_log_decay_rates[None, :],
        head_direct_weight[None, :],
        head_norm_gain[None, :],
        mixer_output_weight,
        expert_norm_gain[None, :],
        routed_expert_index.T,
        routed_expert_weight.T,
        routed_gate_weight[0],
        routed_up_weight[0],
        routed_down_weight[0],
        common_gate_weight,
        common_up_weight,
        common_down_weight,
    )


def solution(mesh):
    torus = Mesh(mesh.devices.reshape(8, 4, 2, mesh.shape["tp"]), ("sp_0", "sp_1", "sp_2", "tp"))
    return jax.shard_map(
        shards,
        mesh=torus,
        in_specs=(
            P(SP_TP, None),
            P(SP, "tp"),
            P(SP, "tp"),
            P(SP, "tp"),
            P(SP, "tp"),
            P(SP, "tp"),
            P(SP, "tp"),
            P(None, "tp"),
            P(None, "tp"),
            P(None, "tp"),
            P("tp"),
            P("tp"),
            P("tp"),
            P("tp", None),
            P(),
            P(SP_TP, None),
            P(SP_TP, None),
            P(SP, None, None),
            P(SP, None, None),
            P(SP, None, None),
            P(None, "tp"),
            P(None, "tp"),
            P(None, "tp"),
        ),
        out_specs=P(SP_TP, None),
        check_vma=False,
    )
```
